32 devices in a mesh: sp: 16 (over z, y, x), tp: 2 (over core).
Axes of the slice: x: 2, y: 2, z: 4, core: 2. Of those that a mesh axis runs over, the one named last changes fastest.
Arguments:
- stream: bfloat16 [4096, 2048], P(('sp', 'tp')), may hold values from -6 to 6
- head_input_signal: bfloat16 [4096, 2048], P('sp', 'tp'), may hold values from -6 to 6
- write_input_vectors: bfloat16 [4096, 512], P('sp', 'tp'), may hold values from -6 to 6
- read_input_vectors: bfloat16 [4096, 512], P('sp', 'tp'), may hold values from -6 to 6
- output_gate_input: bfloat16 [4096, 2048], P('sp', 'tp'), may hold values from -6 to 6
- step_size_input: bfloat16 [4096, 32], P('sp', 'tp'), may hold values from -5 to 5.5
- position_log_decay: float32 [4096, 32], P('sp', 'tp'), may hold values from -0.7 to 0
- signal_filter_taps: bfloat16 [4, 2048], P(None, 'tp'), may hold values from -3 to 3
- write_filter_taps: bfloat16 [4, 512], P(None, 'tp'), may hold values from -3 to 3
- read_filter_taps: bfloat16 [4, 512], P(None, 'tp'), may hold values from -3 to 3
- step_size_bias: float32 [32], P('tp'), may hold values from -1 to 1
- head_decay_rate: float32 [32], P('tp'), may hold values from 2.4414063e-06 to 0.03
- head_direct_term: float32 [32], P('tp'), may hold values from 0.5 to 2
- grouped_norm_gain: float32 [2048], P('tp'), may hold values from 0.1 to 1.9
- mixer_output_weight: bfloat16 [2048, 2048], P('tp'), may hold values from -0.125 to 0.125
- expert_norm_gain: float32 [2048], replicated, may hold values from 0.1 to 1.9
- chosen_expert_index: int32 [4096, 4], P(('sp', 'tp')), may hold values from 0 to 31, all different within a row; in each aligned block of 128 rows (0 to 127, 128 to 255, ...) at most 24 rows name the same one
- chosen_expert_weight: float32 [4096, 4], P(('sp', 'tp')), may hold values from 0.1 to 1
- routed_gate_weight: bfloat16 [32, 2048, 512], P(('sp', 'tp')), may hold values from -0.125 to 0.125
- routed_up_weight: bfloat16 [32, 2048, 512], P(('sp', 'tp')), may hold values from -0.125 to 0.125
- routed_down_weight: bfloat16 [32, 512, 2048], P(('sp', 'tp')), may hold values from -0.25 to 0.25
- common_gate_weight: bfloat16 [2048, 512], replicated, may hold values from -0.125 to 0.125
- common_up_weight: bfloat16 [2048, 512], replicated, may hold values from -0.125 to 0.125
- common_down_weight: bfloat16 [512, 2048], replicated, may hold values from -0.25 to 0.25
Outputs:
- layer_out: bfloat16 [4096, 2048], P(('sp', 'tp'))
The draws below stay inside these ranges and needn't reach their ends.
Inputs may be any that keep to these rules, and one draw needn't show every extreme that they name: `chosen_expert_index`: each row names 4 different experts. Among the 128 rows of one device (aligned blocks of 128 rows) no expert is named more than 24 times; in some block one expert is named exactly 24 times.
All inputs are finite; a program needn't handle non-finite values.
Results may differ from the reference program's by a relative error of at most 0.015.
Values may be sent and summed in bfloat16 or wider, within the bound.
A program may use at most 128 MiB of HBM per device.

```python
import math
import jax
import jax.numpy as jnp
import numpy as np
from jax import lax

D = 2048
HEADS = 32
HEAD_DIM = 64
GROUPS = 4
STATE = 128
CONV_K = 4
BLK = 128
EFF = 512
SFF = 512
TOP = 4
TOK_DEV = 256
SSM_WIDTH = 2048
TOKENS = 4096
ROWS = 128
EXPERTS = 32
CAP = 24
N_SP = 16
N_TP = 2


def draw_step_size_input(key, part):
    first_key, second_key = jax.random.split(jax.random.fold_in(key, 11))
    base = jnp.clip(jax.random.normal(first_key, (TOKENS, HEADS), jnp.float32), -4.0, 4.0)
    shifts = jax.random.uniform(second_key, (TOKENS // TOK_DEV, 1, 1), jnp.float32, -1.0, 1.5)
    shifts = jnp.broadcast_to(shifts, (TOKENS // TOK_DEV, TOK_DEV, HEADS)).reshape(TOKENS, HEADS)
    return (base + shifts).astype(jnp.bfloat16)


def draw_position_log_decay(key, part):
    first_key, second_key = jax.random.split(jax.random.fold_in(key, 23))
    spots = jax.random.randint(first_key, (8,), 0, TOKENS)
    struck = jnp.any(jnp.arange(TOKENS)[:, None] == spots[None, :], axis=1)
    values = jax.random.uniform(second_key, (TOKENS, HEADS), jnp.float32, -0.69, -0.22)
    return jnp.where(struck[:, None], values, 0.0).astype(jnp.float32)


def draw_head_decay_rate(key, part):
    lowest = math.log(0.01 / TOKENS)
    highest = math.log(0.03)
    logs = jax.random.uniform(jax.random.fold_in(key, 37), (HEADS,), jnp.float32, lowest, highest)
    return jnp.exp(logs).astype(jnp.float32)


def block_scale(key, dims, shards, smallest, top_value):
    factor_of, own = 1.0, jax.random.fold_in(key, 6)
    for axis_at, blocks in shards:
        heights = jnp.exp(jax.random.uniform(jax.random.fold_in(own, axis_at), (blocks,), jnp.float32, smallest / len(shards), top_value / len(shards)))
        factor_of = factor_of * jnp.repeat(heights, dims[axis_at] // blocks).reshape([-1 if axis == axis_at else 1 for axis in range(len(dims))])
    return factor_of


def routed_block(stream_key, own, number, rows, number_of, top, bound, lean):
    order = jax.random.permutation(stream_key, number_of)
    packed, ordinary = shares(number_of, rows * top, bound, lean, True), shares(number_of, rows * top, bound, lean, False)
    places = jnp.arange(number_of)

    def named(tallies, turn):
        used = int((tallies > 0).sum())
        fixed = max(1, used // 4)
        shifted = fixed + (places - fixed + turn * (used - fixed)) % max(1, number_of - fixed)
        return jnp.zeros((number_of,), jnp.int32).at[order[jnp.where(places < fixed, places, shifted)]].set(jnp.asarray(tallies, jnp.int32))

    tallies = jnp.where(number % 4 == 0, named(packed, number // 4), named(ordinary, number - number // 4 - 1))
    mixed = jax.random.permutation(jax.random.fold_in(own, 3), number_of)
    giver, sink = mixed[0:number_of // 2 * 2:2], mixed[1:number_of // 2 * 2:2]
    room = jnp.minimum(tallies[giver] - 1, bound - tallies[sink]) // 2
    room = jnp.where((giver == order[0]) | (sink == order[0]) | (tallies[sink] == 0), 0, jnp.maximum(room, 0))
    shifted = jax.random.randint(jax.random.fold_in(own, 4), (number_of // 2,), 0, 1 << 20) % (room + 1)
    tallies = tallies.at[giver].add(-shifted).at[sink].add(shifted)
    members = jnp.searchsorted(jnp.cumsum(tallies), jnp.arange(rows * top), side="right").astype(jnp.int32)
    table = members.reshape(top, rows).T
    table = table[jax.random.permutation(jax.random.fold_in(own, 1), rows)]
    turn = jax.random.randint(jax.random.fold_in(own, 2), (rows, 1), 0, top)
    return jnp.take_along_axis(table, (jnp.arange(top)[None, :] + turn) % top, axis=1)


def shares(amount, total, limit, slope, full):
    loads = [(1 << 20) // math.isqrt(standing ** slope) + 1 for standing in range(1, amount + 1)]
    largest = limit if full else min(limit, max(-(-total // amount), total * loads[0] // sum(loads)))
    least = 1 if total - largest >= amount - 1 else 0
    given, rest = [largest] + [least] * (amount - 1), total - largest - least * (amount - 1)
    while rest > 0:
        free = [i for i in range(1, amount) if given[i] < largest] or [i for i in range(1, amount) if given[i] < limit]
        pool, budget = sum([loads[i] for i in free]), rest
        for i in free:
            more = min(limit - given[i], max(1, budget * loads[i] // pool), rest)
            given[i] = given[i] + more
            rest = rest - more
    return np.array(given)


def scatter_about(stream_key, extent, deviation, reach, cuts=(), kind=jnp.bfloat16):
    loudness = block_scale(stream_key, extent, cuts, -0.22, 0.18) if cuts else 1.0
    drawn = jax.random.normal(stream_key, extent, jnp.float32) * deviation * loudness
    return jnp.minimum(jnp.maximum(drawn, -reach), reach).astype(kind)


def setup_inputs(seed: int = 0) -> dict:
    arg_keys = jax.random.split(jax.random.key(seed), 25)
    stream = scatter_about(arg_keys[0], (TOKENS, D), 1.0, 6.0, ((0, 32),))
    head_input_signal = scatter_about(arg_keys[1], (TOKENS, SSM_WIDTH), 1.0, 6.0, ((0, 16), (1, 2)))
    write_input_vectors = scatter_about(arg_keys[2], (TOKENS, GROUPS * STATE), 1.0, 6.0, ((0, 16), (1, 2)))
    read_input_vectors = scatter_about(arg_keys[3], (TOKENS, GROUPS * STATE), 1.0, 6.0, ((0, 16), (1, 2)))
    output_gate_input = scatter_about(arg_keys[4], (TOKENS, SSM_WIDTH), 1.0, 6.0, ((0, 16), (1, 2)))
    step_size_input = draw_step_size_input(jax.random.fold_in(arg_keys[24], 71), 0)
    position_log_decay = draw_position_log_decay(jax.random.fold_in(arg_keys[24], 71), 0)
    signal_filter_taps = scatter_about(arg_keys[7], (CONV_K, SSM_WIDTH), CONV_K ** -0.5, 3.0, ((1, 2),))
    write_filter_taps = scatter_about(arg_keys[8], (CONV_K, GROUPS * STATE), CONV_K ** -0.5, 3.0, ((1, 2),))
    read_filter_taps = scatter_about(arg_keys[9], (CONV_K, GROUPS * STATE), CONV_K ** -0.5, 3.0, ((1, 2),))
    step_size_bias = jnp.clip(jax.random.uniform(arg_keys[10], (HEADS,), jnp.float32, -1.0, 1.0) * block_scale(arg_keys[10], (HEADS,), ((0, 2),), -0.4, 0.0), -1.0, 1.0)
    head_decay_rate = draw_head_decay_rate(jax.random.fold_in(arg_keys[24], 71), 0)
    head_direct_term = jnp.clip(0.5 + 1.5 * jax.random.uniform(arg_keys[12], (HEADS,), jnp.float32) ** block_scale(arg_keys[12], (HEADS,), ((0, 2),), -0.2, 0.2), 0.5, 2.0)
    grouped_norm_gain = jnp.clip(1.0 + 0.18 * jax.random.normal(arg_keys[13], (SSM_WIDTH,), jnp.float32), 0.1, 1.9)
    mixer_output_weight = scatter_about(arg_keys[14], (SSM_WIDTH, D), SSM_WIDTH ** -0.5, 0.125, ((0, 2),))
    expert_norm_gain = jnp.clip(1.0 + 0.18 * jax.random.normal(arg_keys[15], (D,), jnp.float32), 0.1, 1.9)
    chosen_expert_index_keys = jax.random.split(jax.random.fold_in(arg_keys[16], 1), TOKENS // ROWS)
    chosen_expert_index_turns = jax.random.permutation(jax.random.fold_in(arg_keys[16], 3), TOKENS // ROWS)
    chosen_expert_index = jax.vmap(lambda own, number: routed_block(jax.random.fold_in(arg_keys[16], 2), own, number, ROWS, EXPERTS, TOP, CAP, 1))(chosen_expert_index_keys, chosen_expert_index_turns).reshape((TOKENS, TOP))
    chosen_expert_weight = jnp.clip(0.1 + 0.9 * jax.random.uniform(arg_keys[17], (TOKENS, TOP), jnp.float32) ** block_scale(arg_keys[17], (TOKENS, TOP), ((0, 32),), -0.2, 0.2), 0.1, 1.0)
    routed_gate_weight = scatter_about(arg_keys[18], (EXPERTS, D, EFF), D ** -0.5, 0.125, ((0, 32),))
    routed_up_weight = scatter_about(arg_keys[19], (EXPERTS, D, EFF), D ** -0.5, 0.125, ((0, 32),))
    routed_down_weight = scatter_about(arg_keys[20], (EXPERTS, EFF, D), EFF ** -0.5, 0.25, ((0, 32),))
    common_gate_weight = scatter_about(arg_keys[21], (D, SFF), D ** -0.5, 0.125)
    common_up_weight = scatter_about(arg_keys[22], (D, SFF), D ** -0.5, 0.125)
    common_down_weight = scatter_about(arg_keys[23], (SFF, D), SFF ** -0.5, 0.25)
    return {"stream": stream, "head_input_signal": head_input_signal, "write_input_vectors": write_input_vectors, "read_input_vectors": read_input_vectors, "output_gate_input": output_gate_input, "step_size_input": step_size_input, "position_log_decay": position_log_decay, "signal_filter_taps": signal_filter_taps, "write_filter_taps": write_filter_taps, "read_filter_taps": read_filter_taps, "step_size_bias": step_size_bias, "head_decay_rate": head_decay_rate, "head_direct_term": head_direct_term, "grouped_norm_gain": grouped_norm_gain, "mixer_output_weight": mixer_output_weight, "expert_norm_gain": expert_norm_gain, "chosen_expert_index": chosen_expert_index, "chosen_expert_weight": chosen_expert_weight, "routed_gate_weight": routed_gate_weight, "routed_up_weight": routed_up_weight, "routed_down_weight": routed_down_weight, "common_gate_weight": common_gate_weight, "common_up_weight": common_up_weight, "common_down_weight": common_down_weight}


precise = lax.Precision.HIGHEST

def causal_conv(previous, current, weight):
    stacked = jnp.concatenate([previous, current], axis=0).astype(jnp.float32)
    weight = weight.astype(jnp.float32)
    kernel_len = weight.shape[0]
    length = current.shape[0]
    summed_taps = weight[0] * stacked[0:length]
    for offset in range(1, kernel_len):
        summed_taps = summed_taps + weight[offset] * stacked[offset:offset + length]
    return jax.nn.silu(summed_taps)

def reference(stream, head_input_signal, write_input_vectors, read_input_vectors, output_gate_input, step_size_input, position_log_decay, signal_filter_taps, write_filter_taps, read_filter_taps, step_size_bias, head_decay_rate, head_direct_term, grouped_norm_gain, mixer_output_weight, expert_norm_gain, chosen_expert_index, chosen_expert_weight, routed_gate_weight, routed_up_weight, routed_down_weight, common_gate_weight, common_up_weight, common_down_weight):
    margin = CONV_K - 1
    signal = causal_conv(jnp.zeros((margin, SSM_WIDTH), jnp.bfloat16), head_input_signal, signal_filter_taps)
    write_vec = causal_conv(jnp.zeros((margin, GROUPS * STATE), jnp.bfloat16), write_input_vectors, write_filter_taps)
    read_vec = causal_conv(jnp.zeros((margin, GROUPS * STATE), jnp.bfloat16), read_input_vectors, read_filter_taps)
    time_position = jax.nn.softplus(step_size_input.astype(jnp.float32) + step_size_bias)
    decay_logarithm = position_log_decay - head_decay_rate * time_position
    per_group = HEADS // GROUPS
    blocks = TOKENS // BLK
    signal_heads = signal.reshape(TOKENS, GROUPS, per_group, HEAD_DIM)
    scaled_in = signal_heads * time_position.reshape(TOKENS, GROUPS, per_group)[..., None]
    causal = jnp.arange(BLK)[:, None] >= jnp.arange(BLK)[None, :]
    skip_heads = head_direct_term.reshape(GROUPS, per_group)[:, :, None]

    def advance(carry_state, inputs):
        scaled_blk, write_blk, read_blk, decay_blk, signal_blk = inputs
        within_cum = jnp.cumsum(decay_blk, axis=0)
        cum_heads = jnp.transpose(within_cum, (1, 2, 0))
        decay_matrix = jnp.exp(jnp.where(causal, cum_heads[..., :, None] - cum_heads[..., None, :], -jnp.inf))
        intersection = jnp.einsum('tgn,sgn->gts', read_blk, write_blk, precision=precise)
        intra = jnp.einsum('gts,gets,sgep->tgep', intersection, decay_matrix, scaled_blk, precision=precise)
        carried = jnp.einsum('tgn,gepn,tge->tgep', read_blk, carry_state, jnp.exp(within_cum), precision=precise)
        tail_decay = jnp.exp(within_cum[-1][None] - within_cum)
        fresh = jnp.einsum('sgn,sge,sgep->gepn', write_blk, tail_decay, scaled_blk, precision=precise)
        next_state = carry_state * jnp.exp(within_cum[-1])[..., None, None] + fresh
        return (next_state, intra + carried + skip_heads * signal_blk)
    sequence = (scaled_in.reshape(blocks, BLK, GROUPS, per_group, HEAD_DIM), write_vec.reshape(blocks, BLK, GROUPS, STATE), read_vec.reshape(blocks, BLK, GROUPS, STATE), decay_logarithm.reshape(blocks, BLK, GROUPS, per_group), signal_heads.reshape(blocks, BLK, GROUPS, per_group, HEAD_DIM))
    initial = jnp.zeros((GROUPS, per_group, HEAD_DIM, STATE), jnp.float32)
    ssd_out = lax.scan(advance, initial, sequence)[1]
    gated = ssd_out.reshape(TOKENS, GROUPS, per_group * HEAD_DIM) * jax.nn.silu(output_gate_input.astype(jnp.float32)).reshape(TOKENS, GROUPS, per_group * HEAD_DIM)
    norm_scale = lax.rsqrt(lax.optimization_barrier(jnp.mean(gated * gated, axis=-1, keepdims=True)) + 1e-06)
    mixer_out = ((gated * norm_scale).reshape(TOKENS, SSM_WIDTH) * grouped_norm_gain).astype(jnp.bfloat16)
    residual = (stream.astype(jnp.float32) + jnp.dot(mixer_out, mixer_output_weight, preferred_element_type=jnp.float32)).astype(jnp.bfloat16)
    widened = residual.astype(jnp.float32)
    normed = (widened * lax.rsqrt(lax.optimization_barrier(jnp.mean(widened * widened, axis=-1, keepdims=True)) + 1e-06) * expert_norm_gain).astype(jnp.bfloat16)
    shared_hidden = (jax.nn.silu(jnp.dot(normed, common_gate_weight, preferred_element_type=jnp.float32)) * jnp.dot(normed, common_up_weight, preferred_element_type=jnp.float32)).astype(jnp.bfloat16)
    shared = jnp.dot(shared_hidden, common_down_weight, preferred_element_type=jnp.float32)
    row_total = TOKENS * TOP
    chosen = chosen_expert_index.reshape(-1).astype(jnp.int32)
    one_hot = (chosen[:, None] == jnp.arange(EXPERTS, dtype=jnp.int32)[None, :]).astype(jnp.int32)
    slot_index = lax.optimization_barrier(jnp.sum((jnp.cumsum(one_hot, axis=0) - one_hot) * one_hot, axis=1)).astype(jnp.int32)
    slot_limit = N_SP * N_TP * CAP
    source_row = (jnp.arange(row_total, dtype=jnp.int32) // TOP).astype(jnp.int32)
    slot_table = jnp.full((EXPERTS, slot_limit), TOKENS, jnp.int32).at[chosen, slot_index].set(source_row)
    weight_table = jnp.zeros((EXPERTS, slot_limit), jnp.float32).at[chosen, slot_index].set(chosen_expert_weight.reshape(-1))
    padded = jnp.concatenate([normed, jnp.zeros((1, D), normed.dtype)], axis=0)

    def serve_expert(summed, inputs):
        gate_w, up_w, down_w, indices, weights = inputs
        picked = padded[indices]
        hidden = (jax.nn.silu(jnp.dot(picked, gate_w, preferred_element_type=jnp.float32)) * jnp.dot(picked, up_w, preferred_element_type=jnp.float32)).astype(jnp.bfloat16)
        result = jnp.dot(hidden, down_w, preferred_element_type=jnp.float32).astype(jnp.bfloat16)
        return (summed.at[indices].add(weights[:, None] * result.astype(jnp.float32), mode='drop'), None)
    routed = lax.scan(serve_expert, jnp.zeros((TOKENS, D), jnp.float32), (routed_gate_weight, routed_up_weight, routed_down_weight, slot_table, weight_table))[0]
    return (widened + shared + routed).astype(jnp.bfloat16)
```

```python
import functools

import jax
import jax.numpy as jnp
from jax import lax
from jax.experimental import pallas as pl
from jax.experimental.pallas import tpu as pltpu
from jax.sharding import PartitionSpec as P

HEAD_DIM = 64
STATE = 128
BLK = 128


def from_behind(block, axis, distance):
    devices = range(lax.axis_size(axis))
    route = [(i - distance, i) for i in devices if i - distance in devices]
    return lax.ppermute(block, axis, route)


def swap(block, axis, step, upward_only):
    devices = range(lax.axis_size(axis))
    route = [(i, i ^ step) for i in devices if not (upward_only and i & step)]
    return lax.ppermute(block, axis, route)


def carried_in(log_total, state, axis):
    count, mine = lax.axis_size(axis), lax.axis_index(axis)
    heads, width = log_total.size, state.shape[-1]
    flat = state.reshape(heads, -1, width)
    decay = jnp.exp(log_total).reshape(heads)
    total, before, before_decay = flat, jnp.zeros_like(flat), jnp.ones_like(decay)
    step = 1
    while step < count:
        coarse = lax.reduce_precision(decay, 8, 7)
        lane = jnp.arange(width)[None, :]
        tail = jnp.where(lane == 0, coarse[:, None], jnp.where(lane == 1, (decay - coarse)[:, None], 0.0))
        sent = jnp.concatenate([total.reshape(-1, width), tail], axis=0).astype(jnp.bfloat16)
        got = swap(sent, axis, step, 2 * step >= count).astype(jnp.float32)
        other = got[: got.shape[0] - heads].reshape(flat.shape)
        other_decay = got[got.shape[0] - heads :, 0] + got[got.shape[0] - heads :, 1]
        upper = (mine & step) != 0
        before = before + jnp.where(upper, before_decay, 0.0)[:, None, None] * other
        if 2 * step < count:
            before_decay = before_decay * jnp.where(upper, other_decay, 1.0)
            total = jnp.where(
                upper, other * decay[:, None, None] + total, total * other_decay[:, None, None] + other
            )
            decay = decay * other_decay
        step *= 2
    return before.reshape(state.shape)


def causal_conv(previous, current, weight):
    stacked = jnp.concatenate([previous, current], axis=0).astype(jnp.float32)
    weight = weight.astype(jnp.float32)
    kernel_len = weight.shape[0]
    length = current.shape[0]
    summed_taps = weight[0] * stacked[0:length]
    for offset in range(1, kernel_len):
        summed_taps = summed_taps + weight[offset] * stacked[offset : offset + length]
    return jax.nn.silu(summed_taps)


def product(spec, *operands):
    return jnp.einsum(
        spec, *[part.astype(jnp.bfloat16) for part in operands], preferred_element_type=jnp.float32
    )


MESH = pl.DeviceIdType.MESH
PLANES = 4
COLS = 512


def column_chunks(width):
    step = min(COLS, width)
    return [(at, step) for at in range(0, width, step)]


def pick(values, place, which, index):
    chosen = jnp.int32(0)
    for spot, row in enumerate(values):
        chosen = chosen + (place == spot).astype(jnp.int32) * pick_one(row, which)
    return chosen


def pick_one(row, which):
    chosen = jnp.int32(0)
    for spot, value in enumerate(row):
        chosen = chosen + (which == spot).astype(jnp.int32) * value
    return chosen


def tail_kernel(
    planes,
    ring,
    tp_count,
    capacity,
    fanout,
    mixed_ref,
    stream_ref,
    gain_ref,
    table_ref,
    out_weight_hbm,
    gate_hbm,
    up_hbm,
    down_hbm,
    common_gate_hbm,
    common_up_hbm,
    common_down_hbm,
    out_ref,
    out_weight,
    gate,
    up,
    down,
    common_gate,
    common_up,
    common_down,
    tables,
    total,
    residual,
    part_out,
    part_in,
    rows,
    sent,
    arrived,
    flat,
    hidden,
    answer,
    returned,
    sums_out,
    sums_in,
    weight_sem,
    part_send,
    part_recv,
    table_send,
    table_recv,
    rows_up,
    rows_down,
    rows_recv,
    go_send,
    go_recv,
    back_send,
    back_recv,
    sums_send,
    sums_recv,
):
    chip = lax.axis_index("sp")
    core = lax.axis_index("tp")
    chips = ring // tp_count
    plane = chip // chips
    mine = (chip % chips) * tp_count + core
    count, width = rows.shape[1], rows.shape[2]
    order = [sorted(range(planes), key=lambda s: (abs(s - z), s)) for z in range(planes)]

    def in_plane(spot):
        return (plane * chips + spot // tp_count, spot % tp_count)

    def in_line(spot):
        return (spot * chips + chip % chips, core)

    loads = [
        pltpu.make_async_copy(source, target, weight_sem.at[number])
        for number, (source, target) in enumerate(
            [
                (out_weight_hbm, out_weight),
                (common_gate_hbm, common_gate),
                (common_up_hbm, common_up),
                (common_down_hbm, common_down),
                (gate_hbm.at[0], gate),
                (up_hbm.at[0], up),
                (down_hbm.at[0], down),
            ]
        )
    ]
    for load in loads:
        load.start()

    barrier = pltpu.get_barrier_semaphore()
    for ahead in range(1, ring):
        pl.semaphore_signal(
            barrier, inc=1, device_id=in_plane((mine + ahead) % ring), device_id_type=MESH
        )
    for ahead in range(1, planes):
        pl.semaphore_signal(
            barrier, inc=1, device_id=in_line((plane + ahead) % planes), device_id_type=MESH
        )
    pl.semaphore_wait(barrier, ring + planes - 2)

    def table_copy(ahead, owner):
        return pltpu.make_async_remote_copy(
            src_ref=table_ref,
            dst_ref=tables.at[owner],
            send_sem=table_send.at[ahead],
            recv_sem=table_recv.at[owner],
            device_id=in_line((plane + ahead) % planes),
            device_id_type=MESH,
        )

    for ahead in range(1, planes):
        table_copy(ahead, plane).start()
    tables[plane] = table_ref[...]

    def part_copy(ahead):
        return pltpu.make_async_remote_copy(
            src_ref=part_out.at[ahead - 1],
            dst_ref=part_in.at[ahead - 1],
            send_sem=part_send.at[ahead - 1],
            recv_sem=part_recv.at[ahead - 1],
            device_id=(chip, (core + ahead) % tp_count),
            device_id_type=MESH,
        )

    loads[0].wait()
    for ahead in range(1, tp_count):
        owner = (core + ahead) % tp_count
        held = mixed_ref[pl.ds(pl.multiple_of(owner * count, count), count), :]
        for at, step in column_chunks(width):
            part_out[ahead - 1, :, at : at + step] = jnp.dot(
                held, out_weight[:, at : at + step], preferred_element_type=jnp.float32
            ).astype(jnp.bfloat16)
        part_copy(ahead).start()
    held = mixed_ref[pl.ds(pl.multiple_of(core * count, count), count), :]
    for at, step in column_chunks(width):
        total[:, at : at + step] = stream_ref[:, at : at + step].astype(jnp.float32) + jnp.dot(
            held, out_weight[:, at : at + step], preferred_element_type=jnp.float32
        )
    for ahead in range(1, tp_count):
        part_copy(ahead).wait_recv()
    band = 16

    def norm_band(number, carry):
        spot = pl.ds(pl.multiple_of(number * band, band), band)
        summed = total[spot, :]
        for ahead in range(1, tp_count):
            summed = summed + part_in[ahead - 1, spot, :].astype(jnp.float32)
        rounded = summed.astype(jnp.bfloat16)
        wide = rounded.astype(jnp.float32)
        total[spot, :] = wide
        scale = lax.rsqrt(jnp.mean(wide * wide, axis=-1, keepdims=True) + 1e-06)
        rows[plane, spot, :] = (wide * scale * gain_ref[...]).astype(jnp.bfloat16)
        return carry

    lax.fori_loop(0, count // band, norm_band, 0)

    def rows_copy(owner, target, sem):
        return pltpu.make_async_remote_copy(
            src_ref=rows.at[owner],
            dst_ref=rows.at[owner],
            send_sem=sem.at[owner],
            recv_sem=rows_recv.at[owner],
            device_id=in_line(target),
            device_id_type=MESH,
        )

    def go_copy(owner, ahead):
        spot = (mine + ahead) % ring
        return pltpu.make_async_remote_copy(
            src_ref=sent.at[owner, spot],
            dst_ref=arrived.at[owner, mine],
            send_sem=go_send.at[owner, spot],
            recv_sem=go_recv.at[owner, mine],
            device_id=in_plane(spot),
            device_id_type=MESH,
        )

    def go_wait(owner, ahead):
        spot = (mine + ahead) % ring
        return pltpu.make_async_remote_copy(
            src_ref=sent.at[owner, spot],
            dst_ref=arrived.at[owner, spot],
            send_sem=go_send.at[owner, spot],
            recv_sem=go_recv.at[owner, spot],
            device_id=in_plane(spot),
            device_id_type=MESH,
        )

    def back_copy(owner, ahead):
        spot = (mine + ahead) % ring
        return pltpu.make_async_remote_copy(
            src_ref=answer.at[owner, spot],
            dst_ref=returned.at[owner, mine],
            send_sem=back_send.at[owner, spot],
            recv_sem=back_recv.at[owner, mine],
            device_id=in_plane(spot),
            device_id_type=MESH,
        )

    def back_wait(owner, ahead):
        spot = (mine + ahead) % ring
        return pltpu.make_async_remote_copy(
            src_ref=answer.at[owner, spot],
            dst_ref=returned.at[owner, spot],
            send_sem=back_send.at[owner, spot],
            recv_sem=back_recv.at[owner, spot],
            device_id=in_plane(spot),
            device_id_type=MESH,
        )

    def sums_copy(owner):
        return pltpu.make_async_remote_copy(
            src_ref=sums_out.at[owner],
            dst_ref=sums_in.at[plane],
            send_sem=sums_send.at[owner],
            recv_sem=sums_recv.at[plane],
            device_id=in_line(owner),
            device_id_type=MESH,
        )

    def sums_wait(owner):
        return pltpu.make_async_remote_copy(
            src_ref=sums_out.at[owner],
            dst_ref=sums_in.at[owner],
            send_sem=sums_send.at[owner],
            recv_sem=sums_recv.at[owner],
            device_id=in_line(owner),
            device_id_type=MESH,
        )

    def slots_of(owner):
        table = tables[owner]
        first = (plane * ring).astype(jnp.float32)
        names = lax.broadcasted_iota(jnp.int32, (ring, count), 0).astype(jnp.float32) + first
        hits = jnp.zeros((ring, count), jnp.float32)
        share = jnp.zeros((ring, count), jnp.float32)
        for turn in range(fanout):
            named = table[turn : turn + 1, :] == names
            hits = hits + jnp.where(named, 1.0, 0.0)
            share = share + jnp.where(named, table[fanout + turn : fanout + turn + 1, :], 0.0)
        before = lax.broadcasted_iota(jnp.int32, (count, count), 0)
        after = lax.broadcasted_iota(jnp.int32, (count, count), 1)
        earlier = jnp.where(before < after, 1.0, 0.0).astype(jnp.bfloat16)
        slot = jnp.dot(hits.astype(jnp.bfloat16), earlier, preferred_element_type=jnp.float32)
        return jnp.where(hits > 0.5, slot, -1.0), share

    places = lax.broadcasted_iota(jnp.int32, (capacity, count), 0).astype(jnp.float32)

    def wait_table(owner):
        ahead = (owner + planes - plane) % planes
        table_copy(ahead, owner).wait_recv()

    def dispatch(owner):
        @pl.when(owner != plane)
        def _():
            rows_copy(owner, owner, rows_up).wait_recv()
            wait_table(owner)

        @pl.when((owner <= plane) & (plane < planes - 1))
        def _():
            rows_copy(owner, plane + 1, rows_up).start()

        @pl.when((owner >= plane) & (plane > 0))
        def _():
            rows_copy(owner, plane - 1, rows_down).start()

        slot, _ = slots_of(owner)
        chosen = jnp.concatenate(
            [
                jnp.where(slot[spot : spot + 1, :] == places, 1.0, 0.0)
                for spot in range(ring)
            ],
            axis=0,
        ).astype(jnp.bfloat16)
        for at, step in column_chunks(width):
            picked = jnp.dot(
                chosen, rows[owner, :, at : at + step], preferred_element_type=jnp.float32
            )
            for spot in range(ring):
                sent[owner, spot, :, at : at + step] = picked[
                    spot * capacity : (spot + 1) * capacity
                ].astype(jnp.bfloat16)
        for ahead in range(1, ring):
            go_copy(owner, ahead).start()
        arrived[owner, mine] = sent[owner, mine]

    def ffn(x_ref, gate_ref, up_ref, down_ref, hidden_ref, put):
        for at, step in column_chunks(gate_ref.shape[1]):
            half = step // 2
            for lane in (at, at + half):
                g = jnp.dot(
                    x_ref[...], gate_ref[:, lane : lane + half], preferred_element_type=jnp.float32
                )
                u = jnp.dot(
                    x_ref[...], up_ref[:, lane : lane + half], preferred_element_type=jnp.float32
                )
                hidden_ref[:, lane : lane + half] = (jax.nn.silu(g) * u).astype(jnp.bfloat16)
        for at, step in column_chunks(width):
            put(
                at,
                step,
                jnp.dot(
                    hidden_ref[...],
                    down_ref[:, at : at + step],
                    preferred_element_type=jnp.float32,
                ),
            )

    def serve(owner):
        for ahead in range(1, ring):
            go_wait(owner, ahead).wait_recv()
        for at, step in column_chunks(width):
            flat[:, at : at + step] = jnp.concatenate(
                [
                    arrived[owner, spot, :, at : at + step].astype(jnp.float32)
                    for spot in range(ring)
                ],
                axis=0,
            ).astype(jnp.bfloat16)

        def put(at, step, value):
            for spot in range(ring):
                answer[owner, spot, :, at : at + step] = value[
                    spot * capacity : (spot + 1) * capacity
                ].astype(jnp.bfloat16)

        ffn(flat, gate, up, down, hidden, put)
        for ahead in range(1, ring):
            back_copy(owner, ahead).start()
        returned[owner, mine] = answer[owner, mine]

    def collect(owner):
        for ahead in range(1, ring):
            back_wait(owner, ahead).wait_recv()
        slot, share = slots_of(owner)
        spread = jnp.concatenate(
            [
                jnp.where(slot[spot : spot + 1, :] == places, share[spot : spot + 1, :], 0.0)
                for spot in range(ring)
            ],
            axis=0,
        )
        coarse = spread.astype(jnp.bfloat16)
        fine = (spread - coarse.astype(jnp.float32)).astype(jnp.bfloat16)
        contract = (((0,), (0,)), ((), ()))
        for at, step in column_chunks(width):
            back = jnp.concatenate(
                [
                    returned[owner, spot, :, at : at + step].astype(jnp.float32)
                    for spot in range(ring)
                ],
                axis=0,
            ).astype(jnp.bfloat16)
            value = lax.dot_general(coarse, back, contract, preferred_element_type=jnp.float32)
            value = value + lax.dot_general(
                fine, back, contract, preferred_element_type=jnp.float32
            )

            @pl.when(owner == plane)
            def _():
                total[:, at : at + step] += value

            @pl.when(owner != plane)
            def _():
                sums_out[owner, :, at : at + step] = value.astype(jnp.bfloat16)

        @pl.when(owner != plane)
        def _():
            sums_copy(owner).start()

    def source(turn):
        return pick(order, plane, turn, 0)

    def step(turn, carry):
        @pl.when(turn < planes)
        def _():
            dispatch(source(turn))

        @pl.when(turn == 0)
        def _():
            for load in loads[1:]:
                load.wait()

            def put(at, step, value):
                total[:, at : at + step] += value

            ffn(rows.at[plane], common_gate, common_up, common_down, residual, put)

        @pl.when((turn >= 1) & (turn <= planes))
        def _():
            serve(source(turn - 1))

        @pl.when(turn >= 2)
        def _():
            collect(source(turn - 2))

        return carry

    lax.fori_loop(0, planes + 2, step, 0)

    for ahead in range(1, planes):
        sums_wait((plane + ahead) % planes).wait_recv()

    def last_band(number, carry):
        spot = pl.ds(pl.multiple_of(number * band, band), band)
        summed = total[spot, :]
        for ahead in range(1, planes):
            summed = summed + sums_in[(plane + ahead) % planes, spot, :].astype(jnp.float32)
        out_ref[spot, :] = summed.astype(jnp.bfloat16)
        return carry

    lax.fori_loop(0, count // band, last_band, 0)

    for ahead in range(1, tp_count):
        part_copy(ahead).wait_send()
    for ahead in range(1, planes):
        table_copy(ahead, plane).wait_send()
        sums_copy((plane + ahead) % planes).wait_send()
    for owner in range(planes):

        @pl.when((owner <= plane) & (plane < planes - 1))
        def _():
            rows_copy(owner, plane + 1, rows_up).wait_send()

        @pl.when((owner >= plane) & (plane > 0))
        def _():
            rows_copy(owner, plane - 1, rows_down).wait_send()

    def drain(owner, carry):
        for ahead in range(1, ring):
            go_copy(owner, ahead).wait_send()
            back_copy(owner, ahead).wait_send()
        return carry

    lax.fori_loop(0, planes, drain, 0)


def tail(
    mixed,
    stream,
    gain,
    index,
    weight,
    out_weight,
    gate,
    up,
    down,
    common_gate,
    common_up,
    common_down,
):
    sp_count, tp_count = lax.axis_size("sp"), lax.axis_size("tp")
    planes = PLANES if sp_count % PLANES == 0 else 1
    ring = sp_count // planes * tp_count
    count, width = stream.shape
    fanout = index.shape[1]
    experts = sp_count * tp_count
    capacity = max(2, (3 * count * fanout + 2 * experts - 1) // (2 * experts))
    capacity = (capacity + 7) // 8 * 8
    table = jnp.concatenate([index.astype(jnp.float32).T, weight.T], axis=0)
    bf16 = jnp.bfloat16
    vmem, anywhere = pl.BlockSpec(memory_space=pltpu.VMEM), pl.BlockSpec(memory_space=pl.ANY)
    slots = (planes, ring, capacity, width)
    dma = pltpu.SemaphoreType.DMA
    return pl.pallas_call(
        functools.partial(tail_kernel, planes, ring, tp_count, capacity, fanout),
        out_shape=jax.ShapeDtypeStruct((count, width), bf16),
        in_specs=[vmem] * 4 + [anywhere] * 7,
        out_specs=vmem,
        scratch_shapes=[
            pltpu.VMEM(out_weight.shape, bf16),
            pltpu.VMEM(gate.shape[1:], bf16),
            pltpu.VMEM(up.shape[1:], bf16),
            pltpu.VMEM(down.shape[1:], bf16),
            pltpu.VMEM(common_gate.shape, bf16),
            pltpu.VMEM(common_up.shape, bf16),
            pltpu.VMEM(common_down.shape, bf16),
            pltpu.VMEM((planes, 2 * fanout, count), jnp.float32),
            pltpu.VMEM((count, width), jnp.float32),
            pltpu.VMEM((count, common_gate.shape[1]), bf16),
            pltpu.VMEM((tp_count - 1, count, width), bf16),
            pltpu.VMEM((tp_count - 1, count, width), bf16),
            pltpu.VMEM((planes, count, width), bf16),
            pltpu.VMEM(slots, bf16),
            pltpu.VMEM(slots, bf16),
            pltpu.VMEM((ring * capacity, width), bf16),
            pltpu.VMEM((ring * capacity, gate.shape[2]), bf16),
            pltpu.VMEM(slots, bf16),
            pltpu.VMEM(slots, bf16),
            pltpu.VMEM((planes, count, width), bf16),
            pltpu.VMEM((planes, count, width), bf16),
            dma((7,)),
            dma((tp_count - 1,)),
            dma((tp_count - 1,)),
            dma((planes,)),
            dma((planes,)),
            dma((planes,)),
            dma((planes,)),
            dma((planes,)),
            dma((planes, ring)),
            dma((planes, ring)),
            dma((planes, ring)),
            dma((planes, ring)),
            dma((planes,)),
            dma((planes,)),
        ],
        compiler_params=pltpu.CompilerParams(
            collective_id=0, has_side_effects=True, vmem_limit_bytes=60 * 2**20
        ),
    )(
        mixed,
        stream,
        gain.reshape(1, -1),
        table,
        out_weight,
        gate,
        up,
        down,
        common_gate,
        common_up,
        common_down,
    )


def on_device(
    stream,
    head_input_signal,
    write_input_vectors,
    read_input_vectors,
    output_gate_input,
    step_size_input,
    position_log_decay,
    signal_filter_taps,
    write_filter_taps,
    read_filter_taps,
    step_size_bias,
    head_decay_rate,
    head_direct_term,
    grouped_norm_gain,
    mixer_output_weight,
    expert_norm_gain,
    chosen_expert_index,
    chosen_expert_weight,
    routed_gate_weight,
    routed_up_weight,
    routed_down_weight,
    common_gate_weight,
    common_up_weight,
    common_down_weight,
):
    length = head_input_signal.shape[0]
    margin = signal_filter_taps.shape[0] - 1
    head_count = step_size_input.shape[1]
    groups = write_input_vectors.shape[1] // STATE
    per_group = head_count // groups
    blocks = length // BLK
    wide, narrow = head_input_signal.shape[1], write_input_vectors.shape[1]
    rim = jnp.concatenate(
        [part[length - margin :] for part in (head_input_signal, write_input_vectors, read_input_vectors)],
        axis=1,
    )
    rim = from_behind(rim, "sp", 1)
    before = (rim[:, :wide], rim[:, wide : wide + narrow], rim[:, wide + narrow :])
    signal = causal_conv(before[0], head_input_signal, signal_filter_taps)
    write_vec = causal_conv(before[1], write_input_vectors, write_filter_taps)
    read_vec = causal_conv(before[2], read_input_vectors, read_filter_taps)
    time_position = jax.nn.softplus(step_size_input.astype(jnp.float32) + step_size_bias)
    decay_logarithm = position_log_decay - head_decay_rate * time_position
    signal_heads = signal.reshape(blocks, BLK, groups, per_group, HEAD_DIM)
    scaled_blocks = signal_heads * time_position.reshape(blocks, BLK, groups, per_group)[..., None]
    write_blocks = write_vec.reshape(blocks, BLK, groups, STATE)
    read_blocks = read_vec.reshape(blocks, BLK, groups, STATE)
    within_cum = jnp.cumsum(decay_logarithm.reshape(blocks, BLK, groups, per_group), axis=1)
    block_total = within_cum[:, -1]
    running = jnp.cumsum(block_total, axis=0)
    device_total = running[-1]
    causal = jnp.arange(BLK)[:, None] >= jnp.arange(BLK)[None, :]
    cum_heads = jnp.transpose(within_cum, (0, 2, 3, 1))
    differences = cum_heads[..., :, None] - cum_heads[..., None, :]
    decay_matrix = jnp.exp(jnp.where(causal, differences, -jnp.inf))
    tail_decay = jnp.exp(block_total[:, None] - within_cum)
    block_states = product(
        "bsgn,bsgep->bgepn", write_blocks, scaled_blocks * tail_decay[..., None]
    )
    device_state = jnp.sum(
        block_states * jnp.exp(device_total[None] - running)[..., None, None], axis=0
    )
    incoming = carried_in(device_total, device_state, "sp")
    intersection = product("btgn,bsgn->bgts", read_blocks, write_blocks)
    intra_out = product(
        "bgets,bsgep->btgep", intersection[:, :, None] * decay_matrix, scaled_blocks
    )
    readout_scale = jnp.exp(within_cum)
    starts = [incoming]
    for block in range(blocks - 1):
        starts.append(
            starts[-1] * jnp.exp(block_total[block])[..., None, None] + block_states[block]
        )
    near_out = (
        product("btgn,bgepn->btgep", read_blocks, jnp.stack(starts)) * readout_scale[..., None]
    )
    ssd_out = intra_out + near_out
    ssd_out = ssd_out + head_direct_term.reshape(groups, per_group)[:, :, None] * signal_heads
    gated = ssd_out.reshape(length, groups, per_group * HEAD_DIM) * jax.nn.silu(
        output_gate_input.astype(jnp.float32)
    ).reshape(length, groups, per_group * HEAD_DIM)
    norm_scale = lax.rsqrt(jnp.mean(gated * gated, axis=-1, keepdims=True) + 1e-06)
    mixer_out = ((gated * norm_scale).reshape(length, -1) * grouped_norm_gain).astype(jnp.bfloat16)
    return tail(
        mixer_out,
        stream,
        expert_norm_gain,
        chosen_expert_index,
        chosen_expert_weight,
        mixer_output_weight,
        routed_gate_weight,
        routed_up_weight,
        routed_down_weight,
        common_gate_weight,
        common_up_weight,
        common_down_weight,
    )


def solution(mesh):
    in_specs = (
        P(("sp", "tp"), None),
        P("sp", "tp"),
        P("sp", "tp"),
        P("sp", "tp"),
        P("sp", "tp"),
        P("sp", "tp"),
        P("sp", "tp"),
        P(None, "tp"),
        P(None, "tp"),
        P(None, "tp"),
        P("tp"),
        P("tp"),
        P("tp"),
        P("tp"),
        P("tp", None),
        P(),
        P(("sp", "tp"), None),
        P(("sp", "tp"), None),
        P(("sp", "tp"), None, None),
        P(("sp", "tp"), None, None),
        P(("sp", "tp"), None, None),
        P(),
        P(),
        P(),
    )
    out_specs = P(("sp", "tp"), None)
    return jax.shard_map(
        on_device, mesh=mesh, in_specs=in_specs, out_specs=out_specs, check_vma=False
    )
```

```python
import functools

import jax
import jax.numpy as jnp
from jax import lax
from jax.experimental import pallas as pl
from jax.experimental.pallas import tpu as pltpu
from jax.sharding import PartitionSpec as P

STATE = 128
BLK = 128


MESH = pl.DeviceIdType.MESH
PLANES = 4
COLS = 512


def column_chunks(width):
    step = min(COLS, width)
    return [(at, step) for at in range(0, width, step)]


def pick(values, place, which, index):
    chosen = jnp.int32(0)
    for spot, row in enumerate(values):
        chosen = chosen + (place == spot).astype(jnp.int32) * pick_one(row, which)
    return chosen


def pick_one(row, which):
    chosen = jnp.int32(0)
    for spot, value in enumerate(row):
        chosen = chosen + (which == spot).astype(jnp.int32) * value
    return chosen


def tail_kernel(
    planes,
    ring,
    tp_count,
    capacity,
    fanout,
    mixed_ref,
    stream_ref,
    gain_ref,
    table_ref,
    out_weight_hbm,
    gate_hbm,
    up_hbm,
    down_hbm,
    common_gate_hbm,
    common_up_hbm,
    common_down_hbm,
    out_ref,
    out_weight,
    gate,
    up,
    down,
    common_gate,
    common_up,
    common_down,
    tables,
    total,
    residual,
    part_out,
    part_in,
    rows,
    sent,
    arrived,
    flat,
    hidden,
    answer,
    returned,
    sums_out,
    sums_in,
    weight_sem,
    part_send,
    part_recv,
    table_send,
    table_recv,
    rows_up,
    rows_down,
    rows_recv,
    go_send,
    go_recv,
    back_send,
    back_recv,
    sums_send,
    sums_recv,
):
    chip = lax.axis_index("sp")
    core = lax.axis_index("tp")
    chips = ring // tp_count
    plane = chip // chips
    mine = (chip % chips) * tp_count + core
    count, width = rows.shape[1], rows.shape[2]
    order = [sorted(range(planes), key=lambda s: (abs(s - z), s)) for z in range(planes)]

    def in_plane(spot):
        return (plane * chips + spot // tp_count, spot % tp_count)

    def in_line(spot):
        return (spot * chips + chip % chips, core)

    loads = [
        pltpu.make_async_copy(source, target, weight_sem.at[number])
        for number, (source, target) in enumerate(
            [
                (out_weight_hbm, out_weight),
                (common_gate_hbm, common_gate),
                (common_up_hbm, common_up),
                (common_down_hbm, common_down),
                (gate_hbm.at[0], gate),
                (up_hbm.at[0], up),
                (down_hbm.at[0], down),
            ]
        )
    ]
    for load in loads:
        load.start()

    barrier = pltpu.get_barrier_semaphore()
    for ahead in range(1, ring):
        pl.semaphore_signal(
            barrier, inc=1, device_id=in_plane((mine + ahead) % ring), device_id_type=MESH
        )
    for ahead in range(1, planes):
        pl.semaphore_signal(
            barrier, inc=1, device_id=in_line((plane + ahead) % planes), device_id_type=MESH
        )
    pl.semaphore_wait(barrier, ring + planes - 2)

    def table_copy(ahead, owner):
        return pltpu.make_async_remote_copy(
            src_ref=table_ref,
            dst_ref=tables.at[owner],
            send_sem=table_send.at[ahead],
            recv_sem=table_recv.at[owner],
            device_id=in_line((plane + ahead) % planes),
            device_id_type=MESH,
        )

    for ahead in range(1, planes):
        table_copy(ahead, plane).start()
    tables[plane] = table_ref[...]

    def part_copy(ahead):
        return pltpu.make_async_remote_copy(
            src_ref=part_out.at[ahead - 1],
            dst_ref=part_in.at[ahead - 1],
            send_sem=part_send.at[ahead - 1],
            recv_sem=part_recv.at[ahead - 1],
            device_id=(chip, (core + ahead) % tp_count),
            device_id_type=MESH,
        )

    loads[0].wait()
    for ahead in range(1, tp_count):
        owner = (core + ahead) % tp_count
        held = mixed_ref[pl.ds(pl.multiple_of(owner * count, count), count), :]
        for at, step in column_chunks(width):
            part_out[ahead - 1, :, at : at + step] = jnp.dot(
                held, out_weight[:, at : at + step], preferred_element_type=jnp.float32
            ).astype(jnp.bfloat16)
        part_copy(ahead).start()
    held = mixed_ref[pl.ds(pl.multiple_of(core * count, count), count), :]
    for at, step in column_chunks(width):
        total[:, at : at + step] = stream_ref[:, at : at + step].astype(jnp.float32) + jnp.dot(
            held, out_weight[:, at : at + step], preferred_element_type=jnp.float32
        )
    for ahead in range(1, tp_count):
        part_copy(ahead).wait_recv()
    band = 16

    def norm_band(number, carry):
        spot = pl.ds(pl.multiple_of(number * band, band), band)
        summed = total[spot, :]
        for ahead in range(1, tp_count):
            summed = summed + part_in[ahead - 1, spot, :].astype(jnp.float32)
        rounded = summed.astype(jnp.bfloat16)
        wide = rounded.astype(jnp.float32)
        total[spot, :] = wide
        scale = lax.rsqrt(jnp.mean(wide * wide, axis=-1, keepdims=True) + 1e-06)
        rows[plane, spot, :] = (wide * scale * gain_ref[...]).astype(jnp.bfloat16)
        return carry

    lax.fori_loop(0, count // band, norm_band, 0)

    def rows_copy(owner, target, sem):
        return pltpu.make_async_remote_copy(
            src_ref=rows.at[owner],
            dst_ref=rows.at[owner],
            send_sem=sem.at[owner],
            recv_sem=rows_recv.at[owner],
            device_id=in_line(target),
            device_id_type=MESH,
        )

    def go_copy(owner, ahead):
        spot = (mine + ahead) % ring
        return pltpu.make_async_remote_copy(
            src_ref=sent.at[owner, spot],
            dst_ref=arrived.at[owner, mine],
            send_sem=go_send.at[owner, spot],
            recv_sem=go_recv.at[owner, mine],
            device_id=in_plane(spot),
            device_id_type=MESH,
        )

    def go_wait(owner, ahead):
        spot = (mine + ahead) % ring
        return pltpu.make_async_remote_copy(
            src_ref=sent.at[owner, spot],
            dst_ref=arrived.at[owner, spot],
            send_sem=go_send.at[owner, spot],
            recv_sem=go_recv.at[owner, spot],
            device_id=in_plane(spot),
            device_id_type=MESH,
        )

    def back_copy(owner, ahead):
        spot = (mine + ahead) % ring
        return pltpu.make_async_remote_copy(
            src_ref=answer.at[owner, spot],
            dst_ref=returned.at[owner, mine],
            send_sem=back_send.at[owner, spot],
            recv_sem=back_recv.at[owner, mine],
            device_id=in_plane(spot),
            device_id_type=MESH,
        )

    def back_wait(owner, ahead):
        spot = (mine + ahead) % ring
        return pltpu.make_async_remote_copy(
            src_ref=answer.at[owner, spot],
            dst_ref=returned.at[owner, spot],
            send_sem=back_send.at[owner, spot],
            recv_sem=back_recv.at[owner, spot],
            device_id=in_plane(spot),
            device_id_type=MESH,
        )

    def sums_copy(owner):
        return pltpu.make_async_remote_copy(
            src_ref=sums_out.at[owner],
            dst_ref=sums_in.at[plane],
            send_sem=sums_send.at[owner],
            recv_sem=sums_recv.at[plane],
            device_id=in_line(owner),
            device_id_type=MESH,
        )

    def sums_wait(owner):
        return pltpu.make_async_remote_copy(
            src_ref=sums_out.at[owner],
            dst_ref=sums_in.at[owner],
            send_sem=sums_send.at[owner],
            recv_sem=sums_recv.at[owner],
            device_id=in_line(owner),
            device_id_type=MESH,
        )

    def slots_of(owner):
        table = tables[owner]
        first = (plane * ring).astype(jnp.float32)
        names = lax.broadcasted_iota(jnp.int32, (ring, count), 0).astype(jnp.float32) + first
        hits = jnp.zeros((ring, count), jnp.float32)
        share = jnp.zeros((ring, count), jnp.float32)
        for turn in range(fanout):
            named = table[turn : turn + 1, :] == names
            hits = hits + jnp.where(named, 1.0, 0.0)
            share = share + jnp.where(named, table[fanout + turn : fanout + turn + 1, :], 0.0)
        before = lax.broadcasted_iota(jnp.int32, (count, count), 0)
        after = lax.broadcasted_iota(jnp.int32, (count, count), 1)
        earlier = jnp.where(before < after, 1.0, 0.0).astype(jnp.bfloat16)
        slot = jnp.dot(hits.astype(jnp.bfloat16), earlier, preferred_element_type=jnp.float32)
        return jnp.where(hits > 0.5, slot, -1.0), share

    places = lax.broadcasted_iota(jnp.int32, (capacity, count), 0).astype(jnp.float32)

    def wait_table(owner):
        ahead = (owner + planes - plane) % planes
        table_copy(ahead, owner).wait_recv()

    def dispatch(owner):
        @pl.when(owner != plane)
        def _():
            rows_copy(owner, owner, rows_up).wait_recv()
            wait_table(owner)

        @pl.when((owner <= plane) & (plane < planes - 1))
        def _():
            rows_copy(owner, plane + 1, rows_up).start()

        @pl.when((owner >= plane) & (plane > 0))
        def _():
            rows_copy(owner, plane - 1, rows_down).start()

        slot, _ = slots_of(owner)
        chosen = jnp.concatenate(
            [
                jnp.where(slot[spot : spot + 1, :] == places, 1.0, 0.0)
                for spot in range(ring)
            ],
            axis=0,
        ).astype(jnp.bfloat16)
        for at, step in column_chunks(width):
            picked = jnp.dot(
                chosen, rows[owner, :, at : at + step], preferred_element_type=jnp.float32
            )
            for spot in range(ring):
                sent[owner, spot, :, at : at + step] = picked[
                    spot * capacity : (spot + 1) * capacity
                ].astype(jnp.bfloat16)
        for ahead in range(1, ring):
            go_copy(owner, ahead).start()
        arrived[owner, mine] = sent[owner, mine]

    def ffn(x_ref, gate_ref, up_ref, down_ref, hidden_ref, put):
        for at, step in column_chunks(gate_ref.shape[1]):
            half = step // 2
            for lane in (at, at + half):
                g = jnp.dot(
                    x_ref[...], gate_ref[:, lane : lane + half], preferred_element_type=jnp.float32
                )
                u = jnp.dot(
                    x_ref[...], up_ref[:, lane : lane + half], preferred_element_type=jnp.float32
                )
                hidden_ref[:, lane : lane + half] = (jax.nn.silu(g) * u).astype(jnp.bfloat16)
        for at, step in column_chunks(width):
            put(
                at,
                step,
                jnp.dot(
                    hidden_ref[...],
                    down_ref[:, at : at + step],
                    preferred_element_type=jnp.float32,
                ),
            )

    def serve(owner):
        for ahead in range(1, ring):
            go_wait(owner, ahead).wait_recv()
        for at, step in column_chunks(width):
            flat[:, at : at + step] = jnp.concatenate(
                [
                    arrived[owner, spot, :, at : at + step].astype(jnp.float32)
                    for spot in range(ring)
                ],
                axis=0,
            ).astype(jnp.bfloat16)

        def put(at, step, value):
            for spot in range(ring):
                answer[owner, spot, :, at : at + step] = value[
                    spot * capacity : (spot + 1) * capacity
                ].astype(jnp.bfloat16)

        ffn(flat, gate, up, down, hidden, put)
        for ahead in range(1, ring):
            back_copy(owner, ahead).start()
        returned[owner, mine] = answer[owner, mine]

    def collect(owner):
        for ahead in range(1, ring):
            back_wait(owner, ahead).wait_recv()
        slot, share = slots_of(owner)
        spread = jnp.concatenate(
            [
                jnp.where(slot[spot : spot + 1, :] == places, share[spot : spot + 1, :], 0.0)
                for spot in range(ring)
            ],
            axis=0,
        )
        coarse = spread.astype(jnp.bfloat16)
        fine = (spread - coarse.astype(jnp.float32)).astype(jnp.bfloat16)
        contract = (((0,), (0,)), ((), ()))
        for at, step in column_chunks(width):
            back = jnp.concatenate(
                [
                    returned[owner, spot, :, at : at + step].astype(jnp.float32)
                    for spot in range(ring)
                ],
                axis=0,
            ).astype(jnp.bfloat16)
            value = lax.dot_general(coarse, back, contract, preferred_element_type=jnp.float32)
            value = value + lax.dot_general(
                fine, back, contract, preferred_element_type=jnp.float32
            )

            @pl.when(owner == plane)
            def _():
                total[:, at : at + step] += value

            @pl.when(owner != plane)
            def _():
                sums_out[owner, :, at : at + step] = value.astype(jnp.bfloat16)

        @pl.when(owner != plane)
        def _():
            sums_copy(owner).start()

    def source(turn):
        return pick(order, plane, turn, 0)

    def step(turn, carry):
        @pl.when(turn < planes)
        def _():
            dispatch(source(turn))

        @pl.when(turn == 0)
        def _():
            for load in loads[1:]:
                load.wait()

            def put(at, step, value):
                total[:, at : at + step] += value

            ffn(rows.at[plane], common_gate, common_up, common_down, residual, put)

        @pl.when((turn >= 1) & (turn <= planes))
        def _():
            serve(source(turn - 1))

        @pl.when(turn >= 2)
        def _():
            collect(source(turn - 2))

        return carry

    lax.fori_loop(0, planes + 2, step, 0)

    for ahead in range(1, planes):
        sums_wait((plane + ahead) % planes).wait_recv()

    def last_band(number, carry):
        spot = pl.ds(pl.multiple_of(number * band, band), band)
        summed = total[spot, :]
        for ahead in range(1, planes):
            summed = summed + sums_in[(plane + ahead) % planes, spot, :].astype(jnp.float32)
        out_ref[spot, :] = summed.astype(jnp.bfloat16)
        return carry

    lax.fori_loop(0, count // band, last_band, 0)

    for ahead in range(1, tp_count):
        part_copy(ahead).wait_send()
    for ahead in range(1, planes):
        table_copy(ahead, plane).wait_send()
        sums_copy((plane + ahead) % planes).wait_send()
    for owner in range(planes):

        @pl.when((owner <= plane) & (plane < planes - 1))
        def _():
            rows_copy(owner, plane + 1, rows_up).wait_send()

        @pl.when((owner >= plane) & (plane > 0))
        def _():
            rows_copy(owner, plane - 1, rows_down).wait_send()

    def drain(owner, carry):
        for ahead in range(1, ring):
            go_copy(owner, ahead).wait_send()
            back_copy(owner, ahead).wait_send()
        return carry

    lax.fori_loop(0, planes, drain, 0)


def tail(
    mixed,
    stream,
    gain,
    index,
    weight,
    out_weight,
    gate,
    up,
    down,
    common_gate,
    common_up,
    common_down,
):
    sp_count, tp_count = lax.axis_size("sp"), lax.axis_size("tp")
    planes = PLANES if sp_count % PLANES == 0 else 1
    ring = sp_count // planes * tp_count
    count, width = stream.shape
    fanout = index.shape[1]
    experts = sp_count * tp_count
    capacity = max(2, (3 * count * fanout + 2 * experts - 1) // (2 * experts))
    capacity = (capacity + 7) // 8 * 8
    table = jnp.concatenate([index.astype(jnp.float32).T, weight.T], axis=0)
    bf16 = jnp.bfloat16
    vmem, anywhere = pl.BlockSpec(memory_space=pltpu.VMEM), pl.BlockSpec(memory_space=pl.ANY)
    slots = (planes, ring, capacity, width)
    dma = pltpu.SemaphoreType.DMA
    return pl.pallas_call(
        functools.partial(tail_kernel, planes, ring, tp_count, capacity, fanout),
        out_shape=jax.ShapeDtypeStruct((count, width), bf16),
        in_specs=[vmem] * 4 + [anywhere] * 7,
        out_specs=vmem,
        scratch_shapes=[
            pltpu.VMEM(out_weight.shape, bf16),
            pltpu.VMEM(gate.shape[1:], bf16),
            pltpu.VMEM(up.shape[1:], bf16),
            pltpu.VMEM(down.shape[1:], bf16),
            pltpu.VMEM(common_gate.shape, bf16),
            pltpu.VMEM(common_up.shape, bf16),
            pltpu.VMEM(common_down.shape, bf16),
            pltpu.VMEM((planes, 2 * fanout, count), jnp.float32),
            pltpu.VMEM((count, width), jnp.float32),
            pltpu.VMEM((count, common_gate.shape[1]), bf16),
            pltpu.VMEM((tp_count - 1, count, width), bf16),
            pltpu.VMEM((tp_count - 1, count, width), bf16),
            pltpu.VMEM((planes, count, width), bf16),
            pltpu.VMEM(slots, bf16),
            pltpu.VMEM(slots, bf16),
            pltpu.VMEM((ring * capacity, width), bf16),
            pltpu.VMEM((ring * capacity, gate.shape[2]), bf16),
            pltpu.VMEM(slots, bf16),
            pltpu.VMEM(slots, bf16),
            pltpu.VMEM((planes, count, width), bf16),
            pltpu.VMEM((planes, count, width), bf16),
            dma((7,)),
            dma((tp_count - 1,)),
            dma((tp_count - 1,)),
            dma((planes,)),
            dma((planes,)),
            dma((planes,)),
            dma((planes,)),
            dma((planes,)),
            dma((planes, ring)),
            dma((planes, ring)),
            dma((planes, ring)),
            dma((planes, ring)),
            dma((planes,)),
            dma((planes,)),
        ],
        compiler_params=pltpu.CompilerParams(
            collective_id=0, has_side_effects=True, vmem_limit_bytes=60 * 2**20
        ),
    )(
        mixed,
        stream,
        gain.reshape(1, -1),
        table,
        out_weight,
        gate,
        up,
        down,
        common_gate,
        common_up,
        common_down,
    )


def mixer_stage(
    heads,
    groups,
    owners,
    head_dim,
    signal_in,
    write_in,
    read_in,
    gate_in,
    step_in,
    log_in,
    signal_taps,
    write_taps,
    read_taps,
    bias,
    rate,
    direct,
    gain,
    mixed,
    halo_signal,
    halo_write,
    halo_read,
    extended,
    signal,
    write_vec,
    read_vec,
    scaled,
    tailed,
    readout,
    states,
    summed,
    piece_out,
    piece_in,
    decay_out,
    decay_in,
    start_out,
    start_in,
    halo_send,
    halo_recv,
    piece_send,
    piece_recv,
    decay_send,
    decay_recv,
    start_send,
    start_recv,
):
    chip, core = lax.axis_index("sp"), lax.axis_index("tp")
    chips = lax.axis_size("sp")
    length, wide = signal_in.shape
    narrow = write_in.shape[1]
    rim = halo_signal.shape[0]
    taps = signal_taps.shape[0]
    blocks = length // BLK
    per_group = heads // groups
    span = per_group * head_dim
    rows = STATE // owners
    f32, bf16 = jnp.float32, jnp.bfloat16
    exact = lax.Precision.HIGHEST

    def halo_copies(target):
        return [
            pltpu.make_async_remote_copy(
                src_ref=source.at[pl.ds(length - rim, rim), :],
                dst_ref=halo,
                send_sem=halo_send.at[number],
                recv_sem=halo_recv.at[number],
                device_id=(target, core),
                device_id_type=MESH,
            )
            for number, (source, halo) in enumerate(
                [(signal_in, halo_signal), (write_in, halo_write), (read_in, halo_read)]
            )
        ]

    @pl.when(chip < chips - 1)
    def _():
        for copy in halo_copies(chip + 1):
            copy.start()

    timestep = step_in[...].astype(f32) + bias[...]
    timestep = jnp.maximum(timestep, 0.0) + jnp.log1p(jnp.exp(-jnp.abs(timestep)))
    log_decay = log_in[...] - rate[...] * timestep
    first = lax.broadcasted_iota(jnp.int32, (BLK, BLK), 0)
    second = lax.broadcasted_iota(jnp.int32, (BLK, BLK), 1)
    causal = first >= second
    lower = jnp.where(causal, 1.0, 0.0)
    cums = [
        jnp.dot(
            lower,
            log_decay[b * BLK : (b + 1) * BLK],
            precision=exact,
            preferred_element_type=f32,
        )
        for b in range(blocks)
    ]
    part = lax.broadcasted_iota(jnp.int32, (heads, wide), 0)
    lane = lax.broadcasted_iota(jnp.int32, (heads, wide), 1) // head_dim
    widen = jnp.where(part == lane, 1.0, 0.0).astype(bf16)

    def expand(value):
        high = value.astype(bf16)
        rest = value - high.astype(f32)
        middle = rest.astype(bf16)
        low = (rest - middle.astype(f32)).astype(bf16)
        return (
            jnp.dot(high, widen, preferred_element_type=f32)
            + jnp.dot(middle, widen, preferred_element_type=f32)
            + jnp.dot(low, widen, preferred_element_type=f32)
        )

    for b in range(blocks):
        readout[b * BLK : (b + 1) * BLK, :] = expand(jnp.exp(cums[b]))
    decay = readout[BLK - 1 : BLK, :]
    for b in range(1, blocks):
        decay = decay * readout[(b + 1) * BLK - 1 : (b + 1) * BLK, :]
    decay_out[...] = decay

    def decay_copy(owner, device):
        return pltpu.make_async_remote_copy(
            src_ref=decay_out,
            dst_ref=decay_in.at[device],
            send_sem=decay_send.at[owner],
            recv_sem=decay_recv.at[device],
            device_id=(owner, core),
            device_id_type=MESH,
        )

    def piece_copy(owner, device):
        return pltpu.make_async_remote_copy(
            src_ref=piece_out.at[owner],
            dst_ref=piece_in.at[device],
            send_sem=piece_send.at[owner],
            recv_sem=piece_recv.at[device],
            device_id=(owner, core),
            device_id_type=MESH,
        )

    def start_copy(owner, device):
        return pltpu.make_async_remote_copy(
            src_ref=start_out.at[device],
            dst_ref=start_in.at[owner],
            send_sem=start_send.at[device],
            recv_sem=start_recv.at[owner],
            device_id=(device, core),
            device_id_type=MESH,
        )

    def others(number, act):
        for at in range(number):

            @pl.when(at != chip)
            def _():
                act(at)

    others(owners, lambda owner: decay_copy(owner, chip).start())

    @pl.when(chip < owners)
    def _():
        decay_in[chip] = decay_out[...]

    parts = [
        (signal_in, halo_signal, signal_taps, 0, wide),
        (write_in, halo_write, write_taps, wide, narrow),
        (read_in, halo_read, read_taps, wide + narrow, narrow),
    ]
    head_room = 8
    for source, _, _, at, size in parts:
        extended[head_room : head_room + length, at : at + size] = source[...].astype(f32)

    @pl.when(chip > 0)
    def _():
        for copy in halo_copies(chip):
            copy.wait_recv()
        for _, halo, _, at, size in parts:
            extended[0:head_room, at : at + size] = halo[rim - head_room : rim, :].astype(f32)

    @pl.when(chip == 0)
    def _():
        extended[0:head_room, :] = jnp.zeros((head_room, extended.shape[1]), f32)

    def convolve(weights, at, size, put):
        for b in range(blocks):
            for lanes in range(0, size, 256):
                total = None
                for tap in range(taps):
                    begin = head_room - taps + 1 + tap + b * BLK
                    term = (
                        weights[tap : tap + 1, lanes : lanes + 256].astype(f32)
                        * extended[begin : begin + BLK, at + lanes : at + lanes + 256]
                    )
                    total = term if total is None else total + term
                put(b, lanes, jax.nn.silu(total))

    def put_write(b, lanes, value):
        write_vec[b * BLK : (b + 1) * BLK, lanes : lanes + 256] = value.astype(bf16)

    def put_read(b, lanes, value):
        read_vec[b * BLK : (b + 1) * BLK, lanes : lanes + 256] = value.astype(bf16)

    def put_signal(b, lanes, value):
        signal[b * BLK : (b + 1) * BLK, lanes : lanes + 256] = value

    convolve(write_taps, wide, narrow, put_write)
    convolve(signal_taps, 0, wide, put_signal)
    for b in range(blocks):
        spot = slice(b * BLK, (b + 1) * BLK)
        step = timestep[spot]
        scaled[spot, :] = (signal[spot, :] * expand(step)).astype(bf16)
        rest = jnp.exp(cums[b][BLK - 1 : BLK, :] - cums[b])
        tailed[spot, :] = (signal[spot, :] * expand(step * rest)).astype(bf16)
        for g in range(groups):
            states[b, :, g * span : (g + 1) * span] = lax.dot_general(
                write_vec[spot, g * STATE : (g + 1) * STATE],
                tailed[spot, g * span : (g + 1) * span],
                (((0,), (0,)), ((), ())),
                preferred_element_type=f32,
            )
    for owner in range(owners):
        spot = slice(owner * rows, (owner + 1) * rows)
        value = states[0, spot, :]
        for b in range(1, blocks):
            value = value * readout[(b + 1) * BLK - 1 : (b + 1) * BLK, :] + states[b, spot, :]
        piece_out[owner] = value.astype(bf16)
    others(owners, lambda owner: piece_copy(owner, chip).start())

    @pl.when(chip < owners)
    def _():
        piece_in[chip] = piece_out[chip]

    convolve(read_taps, wide + narrow, narrow, put_read)
    spread_direct = expand(jnp.broadcast_to(direct[...], (8, heads)))[0:1, :]
    low_lanes = lax.broadcasted_iota(jnp.int32, (BLK, 2 * head_dim), 1) < head_dim
    for b in range(blocks):
        spot = slice(b * BLK, (b + 1) * BLK)
        turned = cums[b].T
        for g in range(groups):
            inner = slice(g * STATE, (g + 1) * STATE)
            meeting = lax.dot_general(
                read_vec[spot, inner],
                write_vec[spot, inner],
                (((1,), (1,)), ((), ())),
                preferred_element_type=f32,
            )
            for pair in range(per_group // 2):
                head = g * per_group + 2 * pair
                lanes = slice(head * head_dim, (head + 2) * head_dim)
                weights = []
                for at in (head, head + 1):
                    gap = cums[b][:, at : at + 1] - turned[at : at + 1, :]
                    weights.append(
                        (meeting * jnp.exp(jnp.where(causal, gap, -jnp.inf))).astype(bf16)
                    )
                value = scaled[spot, lanes]
                zero = jnp.zeros_like(value)
                both = jnp.concatenate(
                    [jnp.where(low_lanes, value, zero), jnp.where(low_lanes, zero, value)], axis=0
                )
                summed[spot, lanes] = spread_direct[:, lanes] * signal[spot, lanes] + jnp.dot(
                    jnp.concatenate(weights, axis=1), both, preferred_element_type=f32
                )

    @pl.when(chip < owners)
    def _():
        def scan(device, held):
            @pl.when(device != chip)
            def _():
                decay_copy(chip, device).wait_recv()
                piece_copy(chip, device).wait_recv()

            start_out[device] = held.astype(bf16)

            @pl.when(device != chip)
            def _():
                start_copy(chip, device).start()

            return held * decay_in[device] + piece_in[device].astype(f32)

        lax.fori_loop(0, chips, scan, jnp.zeros((rows, wide), f32))
        start_in[chip] = start_out[chip]

    others(owners, lambda owner: start_copy(owner, chip).wait_recv())
    start = jnp.concatenate([start_in[owner].astype(f32) for owner in range(owners)], axis=0)
    for b in range(blocks):
        spot = slice(b * BLK, (b + 1) * BLK)
        if b:
            start = (
                start * readout[b * BLK - 1 : b * BLK, :] + states[b - 1]
            )
        rounded = start.astype(bf16)
        for g in range(groups):
            lanes = slice(g * span, (g + 1) * span)
            near = jnp.dot(
                read_vec[spot, g * STATE : (g + 1) * STATE],
                rounded[:, lanes],
                preferred_element_type=f32,
            )
            value = summed[spot, lanes] + near * readout[spot, lanes]
            value = value * jax.nn.silu(gate_in[spot, lanes].astype(f32))
            scale = lax.rsqrt(jnp.mean(value * value, axis=-1, keepdims=True) + 1e-06)
            mixed[spot, lanes] = (value * scale * gain[:, lanes]).astype(bf16)

    @pl.when(chip < chips - 1)
    def _():
        for copy in halo_copies(chip + 1):
            copy.wait_send()

    others(owners, lambda owner: decay_copy(owner, chip).wait_send())
    others(owners, lambda owner: piece_copy(owner, chip).wait_send())

    @pl.when(chip < owners)
    def _():
        others(chips, lambda device: start_copy(chip, device).wait_send())


def mixer_scratch(chips, owners, length, wide, narrow, blocks):
    f32, bf16 = jnp.float32, jnp.bfloat16
    dma = pltpu.SemaphoreType.DMA
    rows = STATE // owners
    rim = 16
    return [
        pltpu.VMEM((rim, wide), bf16),
        pltpu.VMEM((rim, narrow), bf16),
        pltpu.VMEM((rim, narrow), bf16),
        pltpu.VMEM((length + 8, wide + 2 * narrow), f32),
        pltpu.VMEM((length, wide), f32),
        pltpu.VMEM((length, narrow), bf16),
        pltpu.VMEM((length, narrow), bf16),
        pltpu.VMEM((length, wide), bf16),
        pltpu.VMEM((length, wide), bf16),
        pltpu.VMEM((length, wide), f32),
        pltpu.VMEM((blocks, STATE, wide), f32),
        pltpu.VMEM((length, wide), f32),
        pltpu.VMEM((owners, rows, wide), bf16),
        pltpu.VMEM((chips, rows, wide), bf16),
        pltpu.VMEM((1, wide), f32),
        pltpu.VMEM((chips, 1, wide), f32),
        pltpu.VMEM((chips, rows, wide), bf16),
        pltpu.VMEM((owners, rows, wide), bf16),
        dma((3,)),
        dma((3,)),
        dma((owners,)),
        dma((chips,)),
        dma((owners,)),
        dma((chips,)),
        dma((chips,)),
        dma((owners,)),
    ]


def mixer_kernel(heads, groups, owners, head_dim, *refs):
    chip, core = lax.axis_index("sp"), lax.axis_index("tp")
    chips = lax.axis_size("sp")
    barrier = pltpu.get_barrier_semaphore()
    for ahead in range(1, chips):
        pl.semaphore_signal(
            barrier, inc=1, device_id=((chip + ahead) % chips, core), device_id_type=MESH
        )
    pl.semaphore_wait(barrier, chips - 1)
    mixer_stage(heads, groups, owners, head_dim, *refs)


def mixer(
    signal_in,
    write_in,
    read_in,
    gate_in,
    step_in,
    log_in,
    signal_taps,
    write_taps,
    read_taps,
    bias,
    rate,
    direct,
    gain,
):
    chips = lax.axis_size("sp")
    length, wide = signal_in.shape
    narrow = write_in.shape[1]
    heads = step_in.shape[1]
    owners = min(chips, STATE // 8)
    vmem = pl.BlockSpec(memory_space=pltpu.VMEM)
    return pl.pallas_call(
        functools.partial(mixer_kernel, heads, narrow // STATE, owners, wide // heads),
        out_shape=jax.ShapeDtypeStruct((length, wide), jnp.bfloat16),
        in_specs=[vmem] * 13,
        out_specs=vmem,
        scratch_shapes=mixer_scratch(chips, owners, length, wide, narrow, length // BLK),
        compiler_params=pltpu.CompilerParams(
            collective_id=1, has_side_effects=True, vmem_limit_bytes=60 * 2**20
        ),
    )(
        signal_in,
        write_in,
        read_in,
        gate_in,
        step_in,
        log_in,
        signal_taps,
        write_taps,
        read_taps,
        bias.reshape(1, -1),
        rate.reshape(1, -1),
        direct.reshape(1, -1),
        gain.reshape(1, -1),
    )


def on_device(
    stream,
    head_input_signal,
    write_input_vectors,
    read_input_vectors,
    output_gate_input,
    step_size_input,
    position_log_decay,
    signal_filter_taps,
    write_filter_taps,
    read_filter_taps,
    step_size_bias,
    head_decay_rate,
    head_direct_term,
    grouped_norm_gain,
    mixer_output_weight,
    expert_norm_gain,
    chosen_expert_index,
    chosen_expert_weight,
    routed_gate_weight,
    routed_up_weight,
    routed_down_weight,
    common_gate_weight,
    common_up_weight,
    common_down_weight,
):
    mixer_out = mixer(
        head_input_signal,
        write_input_vectors,
        read_input_vectors,
        output_gate_input,
        step_size_input,
        position_log_decay,
        signal_filter_taps,
        write_filter_taps,
        read_filter_taps,
        step_size_bias,
        head_decay_rate,
        head_direct_term,
        grouped_norm_gain,
    )
    return tail(
        mixer_out,
        stream,
        expert_norm_gain,
        chosen_expert_index,
        chosen_expert_weight,
        mixer_output_weight,
        routed_gate_weight,
        routed_up_weight,
        routed_down_weight,
        common_gate_weight,
        common_up_weight,
        common_down_weight,
    )


def solution(mesh):
    in_specs = (
        P(("sp", "tp"), None),
        P("sp", "tp"),
        P("sp", "tp"),
        P("sp", "tp"),
        P("sp", "tp"),
        P("sp", "tp"),
        P("sp", "tp"),
        P(None, "tp"),
        P(None, "tp"),
        P(None, "tp"),
        P("tp"),
        P("tp"),
        P("tp"),
        P("tp"),
        P("tp", None),
        P(),
        P(("sp", "tp"), None),
        P(("sp", "tp"), None),
        P(("sp", "tp"), None, None),
        P(("sp", "tp"), None, None),
        P(("sp", "tp"), None, None),
        P(),
        P(),
        P(),
    )
    out_specs = P(("sp", "tp"), None)
    return jax.shard_map(
        on_device, mesh=mesh, in_specs=in_specs, out_specs=out_specs, check_vma=False
    )
```

```python
import functools

import jax
import jax.numpy as jnp
from jax import lax
from jax.experimental import pallas as pl
from jax.experimental.pallas import tpu as pltpu
from jax.sharding import PartitionSpec as P

STATE = 128
BLK = 128


MESH = pl.DeviceIdType.MESH
PLANES = 4
COLS = 512


LINE_END = [(0, 0), (0, 1), (3, 0), (0, 2), (1, 1), (1, 2), (0, 3), (2, 2), (2, 1), (1, 3), (2, 3), (1, 0), (2, 0)]
LINE_NEXT = [(0, 1), (0, 2), (0, 0), (3, 0), (1, 2), (0, 3), (2, 2), (1, 0), (1, 3), (2, 0), (2, 3), (1, 1), (2, 1)]


def line_plans(planes):
    if planes == 4:
        mirror = lambda plan: [(kind, 3 - owner) for kind, owner in plan]
        plans = [LINE_END, LINE_NEXT, mirror(LINE_NEXT), mirror(LINE_END)]
    else:
        plans = []
        for z in range(planes):
            near = sorted(range(planes), key=lambda s: (abs(s - z), s))
            plans.append([(0, s) for s in near] + [(3, 0)] + [(k, s) for s in near for k in (1, 2)])
    return [[kind * planes + owner for kind, owner in plan] for plan in plans]


def column_chunks(width):
    step = min(COLS, width)
    return [(at, step) for at in range(0, width, step)]


def pick(values, place, which):
    chosen = jnp.int32(0)
    for spot, row in enumerate(values):
        chosen = chosen + (place == spot).astype(jnp.int32) * pick_one(row, which)
    return chosen


def pick_one(row, which):
    chosen = jnp.int32(0)
    for spot, value in enumerate(row):
        chosen = chosen + (which == spot).astype(jnp.int32) * value
    return chosen


def tail_kernel(
    planes,
    ring,
    tp_count,
    capacity,
    fanout,
    mixed_ref,
    stream_ref,
    gain_ref,
    index_ref,
    weight_ref,
    out_weight_hbm,
    gate_hbm,
    up_hbm,
    down_hbm,
    common_gate_hbm,
    common_up_hbm,
    common_down_hbm,
    out_ref,
    out_weight,
    gate,
    up,
    down,
    common_gate,
    common_up,
    common_down,
    index_tables,
    weight_tables,
    total,
    residual,
    part_out,
    part_in,
    rows,
    sent,
    arrived,
    flat,
    hidden,
    answer,
    returned,
    sums_out,
    sums_in,
    weight_sem,
    part_send,
    part_recv,
    table_send,
    table_recv,
    rows_up,
    rows_down,
    rows_recv,
    go_send,
    go_recv,
    back_send,
    back_recv,
    sums_send,
    sums_recv,
):
    chip = lax.axis_index("sp")
    core = lax.axis_index("tp")
    chips = ring // tp_count
    plane = chip // chips
    mine = (chip % chips) * tp_count + core
    count, width = rows.shape[1], rows.shape[2]
    plans = line_plans(planes)

    def in_plane(spot):
        return (plane * chips + spot // tp_count, spot % tp_count)

    def in_line(spot):
        return (spot * chips + chip % chips, core)

    loads = [
        pltpu.make_async_copy(source, target, weight_sem.at[number])
        for number, (source, target) in enumerate(
            [
                (out_weight_hbm, out_weight),
                (common_gate_hbm, common_gate),
                (common_up_hbm, common_up),
                (common_down_hbm, common_down),
                (gate_hbm.at[0], gate),
                (up_hbm.at[0], up),
                (down_hbm.at[0], down),
            ]
        )
    ]
    for load in loads:
        load.start()

    barrier = pltpu.get_barrier_semaphore()
    for ahead in range(1, ring):
        pl.semaphore_signal(
            barrier, inc=1, device_id=in_plane((mine + ahead) % ring), device_id_type=MESH
        )
    for ahead in range(1, planes):
        pl.semaphore_signal(
            barrier, inc=1, device_id=in_line((plane + ahead) % planes), device_id_type=MESH
        )
    pl.semaphore_wait(barrier, ring + planes - 2)

    def table_copies(ahead, owner):
        return [
            pltpu.make_async_remote_copy(
                src_ref=source,
                dst_ref=held.at[owner],
                send_sem=table_send.at[number, ahead],
                recv_sem=table_recv.at[number, owner],
                device_id=in_line((plane + ahead) % planes),
                device_id_type=MESH,
            )
            for number, (source, held) in enumerate(
                [(index_ref, index_tables), (weight_ref, weight_tables)]
            )
        ]

    for ahead in range(1, planes):
        for copy in table_copies(ahead, plane):
            copy.start()
    index_tables[plane] = index_ref[...]
    weight_tables[plane] = weight_ref[...]

    def part_copy(ahead):
        return pltpu.make_async_remote_copy(
            src_ref=part_out.at[ahead - 1],
            dst_ref=part_in.at[ahead - 1],
            send_sem=part_send.at[ahead - 1],
            recv_sem=part_recv.at[ahead - 1],
            device_id=(chip, (core + ahead) % tp_count),
            device_id_type=MESH,
        )

    loads[0].wait()
    for ahead in range(1, tp_count):
        owner = (core + ahead) % tp_count
        held = mixed_ref[pl.ds(pl.multiple_of(owner * count, count), count), :]
        for at, step in column_chunks(width):
            part_out[ahead - 1, :, at : at + step] = jnp.dot(
                held, out_weight[:, at : at + step], preferred_element_type=jnp.float32
            ).astype(jnp.bfloat16)
        part_copy(ahead).start()
    held = mixed_ref[pl.ds(pl.multiple_of(core * count, count), count), :]
    for at, step in column_chunks(width):
        total[:, at : at + step] = stream_ref[:, at : at + step].astype(jnp.float32) + jnp.dot(
            held, out_weight[:, at : at + step], preferred_element_type=jnp.float32
        )
    for ahead in range(1, tp_count):
        part_copy(ahead).wait_recv()
    band = 16

    def norm_band(number, carry):
        spot = pl.ds(pl.multiple_of(number * band, band), band)
        summed = total[spot, :]
        for ahead in range(1, tp_count):
            summed = summed + part_in[ahead - 1, spot, :].astype(jnp.float32)
        rounded = summed.astype(jnp.bfloat16)
        wide = rounded.astype(jnp.float32)
        total[spot, :] = wide
        scale = lax.rsqrt(jnp.mean(wide * wide, axis=-1, keepdims=True) + 1e-06)
        rows[plane, spot, :] = (wide * scale * gain_ref[...]).astype(jnp.bfloat16)
        return carry

    lax.fori_loop(0, count // band, norm_band, 0)

    def rows_copy(owner, target, sem):
        return pltpu.make_async_remote_copy(
            src_ref=rows.at[owner],
            dst_ref=rows.at[owner],
            send_sem=sem.at[owner],
            recv_sem=rows_recv.at[owner],
            device_id=in_line(target),
            device_id_type=MESH,
        )

    def go_copy(owner, ahead):
        spot = (mine + ahead) % ring
        return pltpu.make_async_remote_copy(
            src_ref=sent.at[owner, spot],
            dst_ref=arrived.at[owner, mine],
            send_sem=go_send.at[owner, spot],
            recv_sem=go_recv.at[owner, mine],
            device_id=in_plane(spot),
            device_id_type=MESH,
        )

    def go_wait(owner, ahead):
        spot = (mine + ahead) % ring
        return pltpu.make_async_remote_copy(
            src_ref=sent.at[owner, spot],
            dst_ref=arrived.at[owner, spot],
            send_sem=go_send.at[owner, spot],
            recv_sem=go_recv.at[owner, spot],
            device_id=in_plane(spot),
            device_id_type=MESH,
        )

    def back_copy(owner, ahead):
        spot = (mine + ahead) % ring
        return pltpu.make_async_remote_copy(
            src_ref=answer.at[owner, spot],
            dst_ref=returned.at[owner, mine],
            send_sem=back_send.at[owner, spot],
            recv_sem=back_recv.at[owner, mine],
            device_id=in_plane(spot),
            device_id_type=MESH,
        )

    def back_wait(owner, ahead):
        spot = (mine + ahead) % ring
        return pltpu.make_async_remote_copy(
            src_ref=answer.at[owner, spot],
            dst_ref=returned.at[owner, spot],
            send_sem=back_send.at[owner, spot],
            recv_sem=back_recv.at[owner, spot],
            device_id=in_plane(spot),
            device_id_type=MESH,
        )

    def sums_copy(owner):
        return pltpu.make_async_remote_copy(
            src_ref=sums_out.at[owner],
            dst_ref=sums_in.at[plane],
            send_sem=sums_send.at[owner],
            recv_sem=sums_recv.at[plane],
            device_id=in_line(owner),
            device_id_type=MESH,
        )

    def sums_wait(owner):
        return pltpu.make_async_remote_copy(
            src_ref=sums_out.at[owner],
            dst_ref=sums_in.at[owner],
            send_sem=sums_send.at[owner],
            recv_sem=sums_recv.at[owner],
            device_id=in_line(owner),
            device_id_type=MESH,
        )

    def slots_of(owner):
        table, parts = index_tables[owner], weight_tables[owner]
        names = lax.broadcasted_iota(jnp.int32, (ring, count), 0) + plane * ring
        hits = jnp.zeros((ring, count), jnp.float32)
        share = jnp.zeros((ring, count), jnp.float32)
        for turn in range(fanout):
            named = table[turn : turn + 1, :] == names
            hits = hits + jnp.where(named, 1.0, 0.0)
            share = share + jnp.where(named, parts[turn : turn + 1, :], 0.0)
        before = lax.broadcasted_iota(jnp.int32, (count, count), 0)
        after = lax.broadcasted_iota(jnp.int32, (count, count), 1)
        earlier = jnp.where(before < after, 1.0, 0.0).astype(jnp.bfloat16)
        slot = jnp.dot(hits.astype(jnp.bfloat16), earlier, preferred_element_type=jnp.float32)
        return jnp.where(hits > 0.5, slot, -1.0), share

    places = lax.broadcasted_iota(jnp.int32, (capacity, count), 0).astype(jnp.float32)

    def wait_table(owner):
        ahead = (owner + planes - plane) % planes
        for copy in table_copies(ahead, owner):
            copy.wait_recv()

    def dispatch(owner):
        @pl.when(owner != plane)
        def _():
            rows_copy(owner, owner, rows_up).wait_recv()
            wait_table(owner)

        @pl.when((owner <= plane) & (plane < planes - 1))
        def _():
            rows_copy(owner, plane + 1, rows_up).start()

        @pl.when((owner >= plane) & (plane > 0))
        def _():
            rows_copy(owner, plane - 1, rows_down).start()

        slot, _ = slots_of(owner)
        chosen = jnp.concatenate(
            [
                jnp.where(slot[spot : spot + 1, :] == places, 1.0, 0.0)
                for spot in range(ring)
            ],
            axis=0,
        ).astype(jnp.bfloat16)
        for at, step in column_chunks(width):
            picked = jnp.dot(
                chosen, rows[owner, :, at : at + step], preferred_element_type=jnp.float32
            )
            for spot in range(ring):
                sent[owner, spot, :, at : at + step] = picked[
                    spot * capacity : (spot + 1) * capacity
                ].astype(jnp.bfloat16)
        for ahead in range(1, ring):
            go_copy(owner, ahead).start()
        arrived[owner, mine] = sent[owner, mine]

    def ffn(x_ref, gate_ref, up_ref, down_ref, hidden_ref, put):
        for at, step in column_chunks(gate_ref.shape[1]):
            half = step // 2
            for lane in (at, at + half):
                g = jnp.dot(
                    x_ref[...], gate_ref[:, lane : lane + half], preferred_element_type=jnp.float32
                )
                u = jnp.dot(
                    x_ref[...], up_ref[:, lane : lane + half], preferred_element_type=jnp.float32
                )
                hidden_ref[:, lane : lane + half] = (jax.nn.silu(g) * u).astype(jnp.bfloat16)
        for at, step in column_chunks(width):
            put(
                at,
                step,
                jnp.dot(
                    hidden_ref[...],
                    down_ref[:, at : at + step],
                    preferred_element_type=jnp.float32,
                ),
            )

    def serve(owner):
        for ahead in range(1, ring):
            go_wait(owner, ahead).wait_recv()
        for at, step in column_chunks(width):
            flat[:, at : at + step] = jnp.concatenate(
                [
                    arrived[owner, spot, :, at : at + step].astype(jnp.float32)
                    for spot in range(ring)
                ],
                axis=0,
            ).astype(jnp.bfloat16)

        def put(at, step, value):
            for spot in range(ring):
                answer[owner, spot, :, at : at + step] = value[
                    spot * capacity : (spot + 1) * capacity
                ].astype(jnp.bfloat16)

        ffn(flat, gate, up, down, hidden, put)
        for ahead in range(1, ring):
            back_copy(owner, ahead).start()
        returned[owner, mine] = answer[owner, mine]

    def collect(owner):
        for ahead in range(1, ring):
            back_wait(owner, ahead).wait_recv()
        slot, share = slots_of(owner)
        spread = jnp.concatenate(
            [
                jnp.where(slot[spot : spot + 1, :] == places, share[spot : spot + 1, :], 0.0)
                for spot in range(ring)
            ],
            axis=0,
        )
        coarse = spread.astype(jnp.bfloat16)
        fine = (spread - coarse.astype(jnp.float32)).astype(jnp.bfloat16)
        contract = (((0,), (0,)), ((), ()))
        for at, step in column_chunks(width):
            back = jnp.concatenate(
                [
                    returned[owner, spot, :, at : at + step].astype(jnp.float32)
                    for spot in range(ring)
                ],
                axis=0,
            ).astype(jnp.bfloat16)
            value = lax.dot_general(coarse, back, contract, preferred_element_type=jnp.float32)
            value = value + lax.dot_general(
                fine, back, contract, preferred_element_type=jnp.float32
            )

            @pl.when(owner == plane)
            def _():
                total[:, at : at + step] += value

            @pl.when(owner != plane)
            def _():
                sums_out[owner, :, at : at + step] = value.astype(jnp.bfloat16)

        @pl.when(owner != plane)
        def _():
            sums_copy(owner).start()

    def share_expert():
        for load in loads[1:4]:
            load.wait()

        def put(at, step, value):
            total[:, at : at + step] += value

        ffn(rows.at[plane], common_gate, common_up, common_down, residual, put)

    def step(turn, carry):
        code = pick(plans, plane, turn)
        kind, owner = code // planes, code % planes

        @pl.when(kind == 0)
        def _():
            dispatch(owner)

        @pl.when(kind == 1)
        def _():
            serve(owner)

        @pl.when(kind == 2)
        def _():
            collect(owner)

        @pl.when(kind == 3)
        def _():
            share_expert()

        return carry

    for load in loads[4:]:
        load.wait()
    lax.fori_loop(0, len(plans[0]), step, 0)

    for ahead in range(1, planes):
        sums_wait((plane + ahead) % planes).wait_recv()

    def last_band(number, carry):
        spot = pl.ds(pl.multiple_of(number * band, band), band)
        summed = total[spot, :]
        for ahead in range(1, planes):
            summed = summed + sums_in[(plane + ahead) % planes, spot, :].astype(jnp.float32)
        out_ref[spot, :] = summed.astype(jnp.bfloat16)
        return carry

    lax.fori_loop(0, count // band, last_band, 0)

    for ahead in range(1, tp_count):
        part_copy(ahead).wait_send()
    for ahead in range(1, planes):
        for copy in table_copies(ahead, plane):
            copy.wait_send()
        sums_copy((plane + ahead) % planes).wait_send()
    for owner in range(planes):

        @pl.when((owner <= plane) & (plane < planes - 1))
        def _():
            rows_copy(owner, plane + 1, rows_up).wait_send()

        @pl.when((owner >= plane) & (plane > 0))
        def _():
            rows_copy(owner, plane - 1, rows_down).wait_send()

    def drain(owner, carry):
        for ahead in range(1, ring):
            go_copy(owner, ahead).wait_send()
            back_copy(owner, ahead).wait_send()
        return carry

    lax.fori_loop(0, planes, drain, 0)


def tail(
    mixed,
    stream,
    gain,
    index,
    weight,
    out_weight,
    gate,
    up,
    down,
    common_gate,
    common_up,
    common_down,
):
    sp_count, tp_count = lax.axis_size("sp"), lax.axis_size("tp")
    planes = PLANES if sp_count % PLANES == 0 else 1
    ring = sp_count // planes * tp_count
    count, width = stream.shape
    fanout = index.shape[1]
    experts = sp_count * tp_count
    capacity = max(2, (3 * count * fanout + 2 * experts - 1) // (2 * experts))
    capacity = (capacity + 7) // 8 * 8
    bf16 = jnp.bfloat16
    vmem, anywhere = pl.BlockSpec(memory_space=pltpu.VMEM), pl.BlockSpec(memory_space=pl.ANY)
    slots = (planes, ring, capacity, width)
    dma = pltpu.SemaphoreType.DMA
    return pl.pallas_call(
        functools.partial(tail_kernel, planes, ring, tp_count, capacity, fanout),
        out_shape=jax.ShapeDtypeStruct((count, width), bf16),
        in_specs=[vmem] * 5 + [anywhere] * 7,
        out_specs=vmem,
        scratch_shapes=[
            pltpu.VMEM(out_weight.shape, bf16),
            pltpu.VMEM(gate.shape[1:], bf16),
            pltpu.VMEM(up.shape[1:], bf16),
            pltpu.VMEM(down.shape[1:], bf16),
            pltpu.VMEM(common_gate.shape, bf16),
            pltpu.VMEM(common_up.shape, bf16),
            pltpu.VMEM(common_down.shape, bf16),
            pltpu.VMEM((planes, fanout, count), jnp.int32),
            pltpu.VMEM((planes, fanout, count), jnp.float32),
            pltpu.VMEM((count, width), jnp.float32),
            pltpu.VMEM((count, common_gate.shape[1]), bf16),
            pltpu.VMEM((tp_count - 1, count, width), bf16),
            pltpu.VMEM((tp_count - 1, count, width), bf16),
            pltpu.VMEM((planes, count, width), bf16),
            pltpu.VMEM(slots, bf16),
            pltpu.VMEM(slots, bf16),
            pltpu.VMEM((ring * capacity, width), bf16),
            pltpu.VMEM((ring * capacity, gate.shape[2]), bf16),
            pltpu.VMEM(slots, bf16),
            pltpu.VMEM(slots, bf16),
            pltpu.VMEM((planes, count, width), bf16),
            pltpu.VMEM((planes, count, width), bf16),
            dma((7,)),
            dma((tp_count - 1,)),
            dma((tp_count - 1,)),
            dma((2, planes)),
            dma((2, planes)),
            dma((planes,)),
            dma((planes,)),
            dma((planes,)),
            dma((planes, ring)),
            dma((planes, ring)),
            dma((planes, ring)),
            dma((planes, ring)),
            dma((planes,)),
            dma((planes,)),
        ],
        compiler_params=pltpu.CompilerParams(
            collective_id=0, has_side_effects=True, vmem_limit_bytes=60 * 2**20
        ),
    )(
        mixed,
        stream,
        gain.reshape(1, -1),
        index.T,
        weight.T,
        out_weight,
        gate,
        up,
        down,
        common_gate,
        common_up,
        common_down,
    )


def mixer_stage(
    heads,
    groups,
    owners,
    head_dim,
    signal_in,
    write_in,
    read_in,
    gate_in,
    step_in,
    log_in,
    signal_taps,
    write_taps,
    read_taps,
    bias,
    rate,
    direct,
    gain,
    mixed,
    halo_signal,
    halo_write,
    halo_read,
    extended,
    signal,
    write_vec,
    read_vec,
    scaled,
    tailed,
    readout,
    states,
    summed,
    piece_out,
    piece_in,
    decay_out,
    decay_in,
    start_out,
    start_in,
    halo_send,
    halo_recv,
    piece_send,
    piece_recv,
    decay_send,
    decay_recv,
    start_send,
    start_recv,
):
    chip, core = lax.axis_index("sp"), lax.axis_index("tp")
    chips = lax.axis_size("sp")
    length, wide = signal_in.shape
    narrow = write_in.shape[1]
    rim = halo_signal.shape[0]
    taps = signal_taps.shape[0]
    blocks = length // BLK
    per_group = heads // groups
    span = per_group * head_dim
    rows = STATE // owners
    f32, bf16 = jnp.float32, jnp.bfloat16
    exact = lax.Precision.HIGHEST

    def halo_copies(target):
        return [
            pltpu.make_async_remote_copy(
                src_ref=source.at[pl.ds(length - rim, rim), :],
                dst_ref=halo,
                send_sem=halo_send.at[number],
                recv_sem=halo_recv.at[number],
                device_id=(target, core),
                device_id_type=MESH,
            )
            for number, (source, halo) in enumerate(
                [(signal_in, halo_signal), (write_in, halo_write), (read_in, halo_read)]
            )
        ]

    @pl.when(chip < chips - 1)
    def _():
        for copy in halo_copies(chip + 1):
            copy.start()

    timestep = step_in[...].astype(f32).T + bias[...]
    timestep = jnp.maximum(timestep, 0.0) + jnp.log1p(jnp.exp(-jnp.abs(timestep)))
    log_decay = log_in[...].T - rate[...] * timestep
    first = lax.broadcasted_iota(jnp.int32, (BLK, BLK), 0)
    second = lax.broadcasted_iota(jnp.int32, (BLK, BLK), 1)
    causal = first >= second
    lower = jnp.where(causal, 1.0, 0.0)
    cums = [
        jnp.dot(
            lower,
            log_decay[b * BLK : (b + 1) * BLK],
            precision=exact,
            preferred_element_type=f32,
        )
        for b in range(blocks)
    ]
    part = lax.broadcasted_iota(jnp.int32, (heads, wide), 0)
    lane = lax.broadcasted_iota(jnp.int32, (heads, wide), 1) // head_dim
    widen = jnp.where(part == lane, 1.0, 0.0).astype(bf16)

    def expand(value):
        high = value.astype(bf16)
        rest = value - high.astype(f32)
        middle = rest.astype(bf16)
        low = (rest - middle.astype(f32)).astype(bf16)
        return (
            jnp.dot(high, widen, preferred_element_type=f32)
            + jnp.dot(middle, widen, preferred_element_type=f32)
            + jnp.dot(low, widen, preferred_element_type=f32)
        )

    for b in range(blocks):
        readout[b * BLK : (b + 1) * BLK, :] = expand(jnp.exp(cums[b]))
    decay = readout[BLK - 1 : BLK, :]
    for b in range(1, blocks):
        decay = decay * readout[(b + 1) * BLK - 1 : (b + 1) * BLK, :]
    decay_out[...] = decay

    def decay_copy(owner, device):
        return pltpu.make_async_remote_copy(
            src_ref=decay_out,
            dst_ref=decay_in.at[device],
            send_sem=decay_send.at[owner],
            recv_sem=decay_recv.at[device],
            device_id=(owner, core),
            device_id_type=MESH,
        )

    def piece_copy(owner, device):
        return pltpu.make_async_remote_copy(
            src_ref=piece_out.at[owner],
            dst_ref=piece_in.at[device],
            send_sem=piece_send.at[owner],
            recv_sem=piece_recv.at[device],
            device_id=(owner, core),
            device_id_type=MESH,
        )

    def start_copy(owner, device):
        return pltpu.make_async_remote_copy(
            src_ref=start_out.at[device],
            dst_ref=start_in.at[owner],
            send_sem=start_send.at[device],
            recv_sem=start_recv.at[owner],
            device_id=(device, core),
            device_id_type=MESH,
        )

    def others(number, act):
        for at in range(number):

            @pl.when(at != chip)
            def _():
                act(at)

    others(owners, lambda owner: decay_copy(owner, chip).start())

    @pl.when(chip < owners)
    def _():
        decay_in[chip] = decay_out[...]

    parts = [
        (signal_in, halo_signal, signal_taps, 0, wide),
        (write_in, halo_write, write_taps, wide, narrow),
        (read_in, halo_read, read_taps, wide + narrow, narrow),
    ]
    head_room = 8
    for source, _, _, at, size in parts:
        extended[head_room : head_room + length, at : at + size] = source[...].astype(f32)

    @pl.when(chip > 0)
    def _():
        for copy in halo_copies(chip):
            copy.wait_recv()
        for _, halo, _, at, size in parts:
            extended[0:head_room, at : at + size] = halo[rim - head_room : rim, :].astype(f32)

    @pl.when(chip == 0)
    def _():
        extended[0:head_room, :] = jnp.zeros((head_room, extended.shape[1]), f32)

    def convolve(weights, at, size, put):
        for b in range(blocks):
            for lanes in range(0, size, 256):
                total = None
                for tap in range(taps):
                    begin = head_room - taps + 1 + tap + b * BLK
                    term = (
                        weights[tap : tap + 1, lanes : lanes + 256].astype(f32)
                        * extended[begin : begin + BLK, at + lanes : at + lanes + 256]
                    )
                    total = term if total is None else total + term
                put(b, lanes, jax.nn.silu(total))

    def put_write(b, lanes, value):
        write_vec[b * BLK : (b + 1) * BLK, lanes : lanes + 256] = value.astype(bf16)

    def put_read(b, lanes, value):
        read_vec[b * BLK : (b + 1) * BLK, lanes : lanes + 256] = value.astype(bf16)

    def put_signal(b, lanes, value):
        signal[b * BLK : (b + 1) * BLK, lanes : lanes + 256] = value

    convolve(write_taps, wide, narrow, put_write)
    convolve(signal_taps, 0, wide, put_signal)
    for b in range(blocks):
        spot = slice(b * BLK, (b + 1) * BLK)
        step = timestep[spot]
        scaled[spot, :] = (signal[spot, :] * expand(step)).astype(bf16)
        rest = jnp.exp(cums[b][BLK - 1 : BLK, :] - cums[b])
        tailed[spot, :] = (signal[spot, :] * expand(step * rest)).astype(bf16)
        for g in range(groups):
            states[b, :, g * span : (g + 1) * span] = lax.dot_general(
                write_vec[spot, g * STATE : (g + 1) * STATE],
                tailed[spot, g * span : (g + 1) * span],
                (((0,), (0,)), ((), ())),
                preferred_element_type=f32,
            )
    for owner in range(owners):
        spot = slice(owner * rows, (owner + 1) * rows)
        value = states[0, spot, :]
        for b in range(1, blocks):
            value = value * readout[(b + 1) * BLK - 1 : (b + 1) * BLK, :] + states[b, spot, :]
        piece_out[owner] = value.astype(bf16)
    others(owners, lambda owner: piece_copy(owner, chip).start())

    @pl.when(chip < owners)
    def _():
        piece_in[chip] = piece_out[chip]

    convolve(read_taps, wide + narrow, narrow, put_read)
    spread_direct = expand(jnp.broadcast_to(direct[...], (8, heads)))[0:1, :]
    low_lanes = lax.broadcasted_iota(jnp.int32, (BLK, 2 * head_dim), 1) < head_dim
    for b in range(blocks):
        spot = slice(b * BLK, (b + 1) * BLK)
        turned = cums[b].T
        for g in range(groups):
            inner = slice(g * STATE, (g + 1) * STATE)
            meeting = lax.dot_general(
                read_vec[spot, inner],
                write_vec[spot, inner],
                (((1,), (1,)), ((), ())),
                preferred_element_type=f32,
            )
            for pair in range(per_group // 2):
                head = g * per_group + 2 * pair
                lanes = slice(head * head_dim, (head + 2) * head_dim)
                weights = []
                for at in (head, head + 1):
                    gap = cums[b][:, at : at + 1] - turned[at : at + 1, :]
                    weights.append(
                        (meeting * jnp.exp(jnp.where(causal, gap, -jnp.inf))).astype(bf16)
                    )
                value = scaled[spot, lanes]
                zero = jnp.zeros_like(value)
                both = jnp.concatenate(
                    [jnp.where(low_lanes, value, zero), jnp.where(low_lanes, zero, value)], axis=0
                )
                summed[spot, lanes] = spread_direct[:, lanes] * signal[spot, lanes] + jnp.dot(
                    jnp.concatenate(weights, axis=1), both, preferred_element_type=f32
                )

    @pl.when(chip < owners)
    def _():
        def scan(device, held):
            @pl.when(device != chip)
            def _():
                decay_copy(chip, device).wait_recv()
                piece_copy(chip, device).wait_recv()

            start_out[device] = held.astype(bf16)

            @pl.when(device != chip)
            def _():
                start_copy(chip, device).start()

            return held * decay_in[device] + piece_in[device].astype(f32)

        lax.fori_loop(0, chips, scan, jnp.zeros((rows, wide), f32))
        start_in[chip] = start_out[chip]

    others(owners, lambda owner: start_copy(owner, chip).wait_recv())
    start = jnp.concatenate([start_in[owner].astype(f32) for owner in range(owners)], axis=0)
    for b in range(blocks):
        spot = slice(b * BLK, (b + 1) * BLK)
        if b:
            start = (
                start * readout[b * BLK - 1 : b * BLK, :] + states[b - 1]
            )
        rounded = start.astype(bf16)
        for g in range(groups):
            lanes = slice(g * span, (g + 1) * span)
            near = jnp.dot(
                read_vec[spot, g * STATE : (g + 1) * STATE],
                rounded[:, lanes],
                preferred_element_type=f32,
            )
            value = summed[spot, lanes] + near * readout[spot, lanes]
            value = value * jax.nn.silu(gate_in[spot, lanes].astype(f32))
            scale = lax.rsqrt(jnp.mean(value * value, axis=-1, keepdims=True) + 1e-06)
            mixed[spot, lanes] = (value * scale * gain[:, lanes]).astype(bf16)

    @pl.when(chip < chips - 1)
    def _():
        for copy in halo_copies(chip + 1):
            copy.wait_send()

    others(owners, lambda owner: decay_copy(owner, chip).wait_send())
    others(owners, lambda owner: piece_copy(owner, chip).wait_send())

    @pl.when(chip < owners)
    def _():
        others(chips, lambda device: start_copy(chip, device).wait_send())


def mixer_scratch(chips, owners, length, wide, narrow, blocks):
    f32, bf16 = jnp.float32, jnp.bfloat16
    dma = pltpu.SemaphoreType.DMA
    rows = STATE // owners
    rim = 16
    return [
        pltpu.VMEM((rim, wide), bf16),
        pltpu.VMEM((rim, narrow), bf16),
        pltpu.VMEM((rim, narrow), bf16),
        pltpu.VMEM((length + 8, wide + 2 * narrow), f32),
        pltpu.VMEM((length, wide), f32),
        pltpu.VMEM((length, narrow), bf16),
        pltpu.VMEM((length, narrow), bf16),
        pltpu.VMEM((length, wide), bf16),
        pltpu.VMEM((length, wide), bf16),
        pltpu.VMEM((length, wide), f32),
        pltpu.VMEM((blocks, STATE, wide), f32),
        pltpu.VMEM((length, wide), f32),
        pltpu.VMEM((owners, rows, wide), bf16),
        pltpu.VMEM((chips, rows, wide), bf16),
        pltpu.VMEM((1, wide), f32),
        pltpu.VMEM((chips, 1, wide), f32),
        pltpu.VMEM((chips, rows, wide), bf16),
        pltpu.VMEM((owners, rows, wide), bf16),
        dma((3,)),
        dma((3,)),
        dma((owners,)),
        dma((chips,)),
        dma((owners,)),
        dma((chips,)),
        dma((chips,)),
        dma((owners,)),
    ]


def mixer_kernel(heads, groups, owners, head_dim, *refs):
    chip, core = lax.axis_index("sp"), lax.axis_index("tp")
    chips = lax.axis_size("sp")
    barrier = pltpu.get_barrier_semaphore()
    for ahead in range(1, chips):
        pl.semaphore_signal(
            barrier, inc=1, device_id=((chip + ahead) % chips, core), device_id_type=MESH
        )
    pl.semaphore_wait(barrier, chips - 1)
    mixer_stage(heads, groups, owners, head_dim, *refs)


def mixer(
    signal_in,
    write_in,
    read_in,
    gate_in,
    step_in,
    log_in,
    signal_taps,
    write_taps,
    read_taps,
    bias,
    rate,
    direct,
    gain,
):
    chips = lax.axis_size("sp")
    length, wide = signal_in.shape
    narrow = write_in.shape[1]
    heads = step_in.shape[1]
    owners = min(chips, STATE // 8)
    vmem = pl.BlockSpec(memory_space=pltpu.VMEM)
    return pl.pallas_call(
        functools.partial(mixer_kernel, heads, narrow // STATE, owners, wide // heads),
        out_shape=jax.ShapeDtypeStruct((length, wide), jnp.bfloat16),
        in_specs=[vmem] * 13,
        out_specs=vmem,
        scratch_shapes=mixer_scratch(chips, owners, length, wide, narrow, length // BLK),
        compiler_params=pltpu.CompilerParams(
            collective_id=1, has_side_effects=True, vmem_limit_bytes=60 * 2**20
        ),
    )(
        signal_in,
        write_in,
        read_in,
        gate_in,
        step_in.T,
        log_in.T,
        signal_taps,
        write_taps,
        read_taps,
        bias.reshape(1, -1),
        rate.reshape(1, -1),
        direct.reshape(1, -1),
        gain.reshape(1, -1),
    )


def on_device(
    stream,
    head_input_signal,
    write_input_vectors,
    read_input_vectors,
    output_gate_input,
    step_size_input,
    position_log_decay,
    signal_filter_taps,
    write_filter_taps,
    read_filter_taps,
    step_size_bias,
    head_decay_rate,
    head_direct_term,
    grouped_norm_gain,
    mixer_output_weight,
    expert_norm_gain,
    chosen_expert_index,
    chosen_expert_weight,
    routed_gate_weight,
    routed_up_weight,
    routed_down_weight,
    common_gate_weight,
    common_up_weight,
    common_down_weight,
):
    mixer_out = mixer(
        head_input_signal,
        write_input_vectors,
        read_input_vectors,
        output_gate_input,
        step_size_input,
        position_log_decay,
        signal_filter_taps,
        write_filter_taps,
        read_filter_taps,
        step_size_bias,
        head_decay_rate,
        head_direct_term,
        grouped_norm_gain,
    )
    return tail(
        mixer_out,
        stream,
        expert_norm_gain,
        chosen_expert_index,
        chosen_expert_weight,
        mixer_output_weight,
        routed_gate_weight,
        routed_up_weight,
        routed_down_weight,
        common_gate_weight,
        common_up_weight,
        common_down_weight,
    )


def solution(mesh):
    in_specs = (
        P(("sp", "tp"), None),
        P("sp", "tp"),
        P("sp", "tp"),
        P("sp", "tp"),
        P("sp", "tp"),
        P("sp", "tp"),
        P("sp", "tp"),
        P(None, "tp"),
        P(None, "tp"),
        P(None, "tp"),
        P("tp"),
        P("tp"),
        P("tp"),
        P("tp"),
        P("tp", None),
        P(),
        P(("sp", "tp"), None),
        P(("sp", "tp"), None),
        P(("sp", "tp"), None, None),
        P(("sp", "tp"), None, None),
        P(("sp", "tp"), None, None),
        P(),
        P(),
        P(),
    )
    out_specs = P(("sp", "tp"), None)
    return jax.shard_map(
        on_device, mesh=mesh, in_specs=in_specs, out_specs=out_specs, check_vma=False
    )
```

```python
import functools

import jax
import jax.numpy as jnp
from jax import lax
from jax.experimental import pallas as pl
from jax.experimental.pallas import tpu as pltpu
from jax.sharding import PartitionSpec as P

STATE = 128
BLK = 128


MESH = pl.DeviceIdType.MESH
PLANES = 4
HALVES = 2
COLS = 512


LINE_END = [
    (0, 0, 0), (0, 0, 1), (0, 1, 0), (1, 0, 0), (0, 2, 0), (0, 2, 1),
    (0, 3, 0), (1, 2, 0), (2, 2, 0), (0, 3, 1), (0, 1, 1), (2, 2, 1),
    (1, 3, 0), (2, 3, 0), (1, 1, 0), (3, 0, 0), (2, 3, 1), (2, 0, 0),
    (2, 1, 0), (2, 1, 1), (2, 0, 1),
]
LINE_NEXT = [
    (0, 1, 0), (0, 1, 1), (0, 0, 0), (0, 2, 0), (0, 2, 1), (0, 3, 0),
    (1, 2, 0), (0, 0, 1), (2, 2, 0), (0, 3, 1), (2, 2, 1), (1, 0, 0),
    (2, 0, 0), (1, 3, 0), (1, 1, 0), (2, 0, 1), (2, 3, 0), (3, 1, 0),
    (2, 1, 0), (2, 1, 1), (2, 3, 1),
]


def line_plans(planes, halves):
    if (planes, halves) == (4, 2):
        mirror = lambda plan: [(kind, 3 - owner, half) for kind, owner, half in plan]
        plans = [LINE_END, LINE_NEXT, mirror(LINE_NEXT), mirror(LINE_END)]
    else:
        plans = []
        for z in range(planes):
            near = sorted(range(planes), key=lambda s: (abs(s - z), s))
            plan = [(0, s, h) for s in near for h in range(halves)] + [(3, 0, 0)]
            for s in near:
                plan += [(1, s, 0)] + [(2, s, h) for h in range(halves)]
            plans.append(plan)
    return [[(k * planes + s) * halves + h for k, s, h in plan] for plan in plans]


def column_chunks(width):
    step = min(COLS, width)
    return [(at, step) for at in range(0, width, step)]


def pick(values, place, which):
    chosen = jnp.int32(0)
    for spot, row in enumerate(values):
        chosen = chosen + (place == spot).astype(jnp.int32) * pick_one(row, which)
    return chosen


def pick_one(row, which):
    chosen = jnp.int32(0)
    for spot, value in enumerate(row):
        chosen = chosen + (which == spot).astype(jnp.int32) * value
    return chosen


def tail_stage(
    planes,
    ring,
    tp_count,
    capacity,
    fanout,
    mix,
    mixed_ref,
    stream_ref,
    gain_ref,
    index_ref,
    weight_ref,
    out_weight_hbm,
    gate_hbm,
    up_hbm,
    down_hbm,
    common_gate_hbm,
    common_up_hbm,
    common_down_hbm,
    out_ref,
    out_weight,
    gate,
    up,
    down,
    common_gate,
    common_up,
    common_down,
    index_tables,
    weight_tables,
    total,
    residual,
    part_out,
    part_in,
    normed,
    rows,
    sent,
    arrived,
    flat,
    hidden,
    answer,
    returned,
    sums_own,
    sums_out,
    sums_in,
    weight_sem,
    part_send,
    part_recv,
    table_send,
    table_recv,
    rows_up,
    rows_down,
    rows_recv,
    go_send,
    go_recv,
    back_send,
    back_recv,
    sums_send,
    sums_recv,
):
    chip = lax.axis_index("sp")
    core = lax.axis_index("tp")
    chips = ring // tp_count
    plane = chip // chips
    mine = (chip % chips) * tp_count + core
    count, width = stream_ref.shape
    halves = rows.shape[1]
    part = width // halves
    plans = line_plans(planes, halves)

    def in_plane(spot):
        return (plane * chips + spot // tp_count, spot % tp_count)

    def in_line(spot):
        return (spot * chips + chip % chips, core)

    loads = [
        pltpu.make_async_copy(source, target, weight_sem.at[number])
        for number, (source, target) in enumerate(
            [
                (out_weight_hbm, out_weight),
                (common_gate_hbm, common_gate),
                (common_up_hbm, common_up),
                (common_down_hbm, common_down),
                (gate_hbm.at[0], gate),
                (up_hbm.at[0], up),
                (down_hbm.at[0], down),
            ]
        )
    ]
    for load in loads:
        load.start()

    barrier = pltpu.get_barrier_semaphore()
    all_chips = lax.axis_size("sp")
    for ahead in range(1, all_chips):
        pl.semaphore_signal(
            barrier, inc=1, device_id=((chip + ahead) % all_chips, core), device_id_type=MESH
        )
    for spot in range(chips):
        for ahead in range(1, tp_count):
            pl.semaphore_signal(
                barrier,
                inc=1,
                device_id=(plane * chips + spot, (core + ahead) % tp_count),
                device_id_type=MESH,
            )
    pl.semaphore_wait(barrier, all_chips - 1 + chips * (tp_count - 1))

    def table_copies(ahead, owner):
        return [
            pltpu.make_async_remote_copy(
                src_ref=source,
                dst_ref=held.at[owner],
                send_sem=table_send.at[number, ahead],
                recv_sem=table_recv.at[number, owner],
                device_id=in_line((plane + ahead) % planes),
                device_id_type=MESH,
            )
            for number, (source, held) in enumerate(
                [(index_ref, index_tables), (weight_ref, weight_tables)]
            )
        ]

    for ahead in range(1, planes):
        for copy in table_copies(ahead, plane):
            copy.start()
    index_tables[plane] = index_ref[...]
    weight_tables[plane] = weight_ref[...]
    mix()

    def part_copies(ahead):
        return [
            pltpu.make_async_remote_copy(
                src_ref=part_out.at[ahead - 1, :, pl.ds(at, step)],
                dst_ref=part_in.at[ahead - 1, :, pl.ds(at, step)],
                send_sem=part_send.at[ahead - 1, number],
                recv_sem=part_recv.at[ahead - 1, number],
                device_id=(chip, (core + ahead) % tp_count),
                device_id_type=MESH,
            )
            for number, (at, step) in enumerate(column_chunks(width))
        ]

    loads[0].wait()
    for ahead in range(1, tp_count):
        owner = (core + ahead) % tp_count
        held = mixed_ref[pl.ds(pl.multiple_of(owner * count, count), count), :]
        copies = part_copies(ahead)
        for number, (at, step) in enumerate(column_chunks(width)):
            part_out[ahead - 1, :, at : at + step] = jnp.dot(
                held, out_weight[:, at : at + step], preferred_element_type=jnp.float32
            ).astype(jnp.bfloat16)
            copies[number].start()
    held = mixed_ref[pl.ds(pl.multiple_of(core * count, count), count), :]
    for at, step in column_chunks(width):
        total[:, at : at + step] = stream_ref[:, at : at + step].astype(jnp.float32) + jnp.dot(
            held, out_weight[:, at : at + step], preferred_element_type=jnp.float32
        )
    for ahead in range(1, tp_count):
        for copy in part_copies(ahead):
            copy.wait_recv()
    band = 16

    def norm_band(number, carry):
        spot = pl.ds(pl.multiple_of(number * band, band), band)
        summed = total[spot, :]
        for ahead in range(1, tp_count):
            summed = summed + part_in[ahead - 1, spot, :].astype(jnp.float32)
        rounded = summed.astype(jnp.bfloat16)
        wide = rounded.astype(jnp.float32)
        total[spot, :] = wide
        scale = lax.rsqrt(jnp.mean(wide * wide, axis=-1, keepdims=True) + 1e-06)
        value = (wide * scale * gain_ref[...]).astype(jnp.bfloat16)
        normed[spot, :] = value
        for half in range(halves):
            rows[plane, half, spot, :] = value[:, half * part : (half + 1) * part]
        return carry

    lax.fori_loop(0, count // band, norm_band, 0)

    def rows_copy(owner, half, target, sem):
        return pltpu.make_async_remote_copy(
            src_ref=rows.at[owner, half],
            dst_ref=rows.at[owner, half],
            send_sem=sem.at[owner, half],
            recv_sem=rows_recv.at[owner, half],
            device_id=in_line(target),
            device_id_type=MESH,
        )

    def block_copy(source, target, send, recv, owner, half, ahead):
        spot = (mine + ahead) % ring
        return pltpu.make_async_remote_copy(
            src_ref=source.at[owner, half, spot],
            dst_ref=target.at[owner, half, mine],
            send_sem=send.at[owner, half],
            recv_sem=recv.at[owner, half],
            device_id=in_plane(spot),
            device_id_type=MESH,
        )

    def block_wait(source, target, send, recv, owner, half):
        return pltpu.make_async_remote_copy(
            src_ref=source.at[owner, half, pl.ds(0, ring - 1)],
            dst_ref=target.at[owner, half, pl.ds(0, ring - 1)],
            send_sem=send.at[owner, half],
            recv_sem=recv.at[owner, half],
            device_id=in_plane((mine + 1) % ring),
            device_id_type=MESH,
        )

    go = (sent, arrived, go_send, go_recv)
    back = (answer, returned, back_send, back_recv)

    def sums_copy(owner, half):
        return pltpu.make_async_remote_copy(
            src_ref=sums_out.at[owner, half],
            dst_ref=sums_in.at[plane, half],
            send_sem=sums_send.at[owner, half],
            recv_sem=sums_recv.at[plane, half],
            device_id=in_line(owner),
            device_id_type=MESH,
        )

    def sums_wait(owner, half):
        return pltpu.make_async_remote_copy(
            src_ref=sums_out.at[owner, half],
            dst_ref=sums_in.at[owner, half],
            send_sem=sums_send.at[owner, half],
            recv_sem=sums_recv.at[owner, half],
            device_id=in_line(owner),
            device_id_type=MESH,
        )

    def slots_of(owner):
        table, parts = index_tables[owner], weight_tables[owner]
        names = lax.broadcasted_iota(jnp.int32, (ring, count), 0) + plane * ring
        hits = jnp.zeros((ring, count), jnp.float32)
        share = jnp.zeros((ring, count), jnp.float32)
        for turn in range(fanout):
            named = table[turn : turn + 1, :] == names
            hits = hits + jnp.where(named, 1.0, 0.0)
            share = share + jnp.where(named, parts[turn : turn + 1, :], 0.0)
        before = lax.broadcasted_iota(jnp.int32, (count, count), 0)
        after = lax.broadcasted_iota(jnp.int32, (count, count), 1)
        earlier = jnp.where(before < after, 1.0, 0.0).astype(jnp.bfloat16)
        slot = jnp.dot(hits.astype(jnp.bfloat16), earlier, preferred_element_type=jnp.float32)
        return jnp.where(hits > 0.5, slot, -1.0), share

    places = lax.broadcasted_iota(jnp.int32, (capacity, count), 0).astype(jnp.float32)

    def wait_table(owner):
        ahead = (owner + planes - plane) % planes
        for copy in table_copies(ahead, owner):
            copy.wait_recv()

    def dispatch(owner, half):
        @pl.when(owner != plane)
        def _():
            rows_copy(owner, half, owner, rows_up).wait_recv()

        @pl.when((owner <= plane) & (plane < planes - 1))
        def _():
            rows_copy(owner, half, plane + 1, rows_up).start()

        @pl.when((owner >= plane) & (plane > 0))
        def _():
            rows_copy(owner, half, plane - 1, rows_down).start()

        @pl.when((owner != plane) & (half == 0))
        def _():
            wait_table(owner)

        slot, _ = slots_of(owner)
        chosen = jnp.concatenate(
            [
                jnp.where(slot[spot : spot + 1, :] == places, 1.0, 0.0)
                for spot in range(ring)
            ],
            axis=0,
        ).astype(jnp.bfloat16)
        for at, step in column_chunks(part):
            picked = jnp.dot(
                chosen, rows[owner, half, :, at : at + step], preferred_element_type=jnp.float32
            )
            for spot in range(ring):
                sent[owner, half, spot, :, at : at + step] = picked[
                    spot * capacity : (spot + 1) * capacity
                ].astype(jnp.bfloat16)
        for ahead in range(1, ring):
            block_copy(*go, owner, half, ahead).start()
        arrived[owner, half, mine] = sent[owner, half, mine]

    def ffn(x_ref, gate_ref, up_ref, down_ref, hidden_ref, put):
        for at, step in column_chunks(gate_ref.shape[1]):
            half = step // 2
            for lane in (at, at + half):
                g = jnp.dot(
                    x_ref[...], gate_ref[:, lane : lane + half], preferred_element_type=jnp.float32
                )
                u = jnp.dot(
                    x_ref[...], up_ref[:, lane : lane + half], preferred_element_type=jnp.float32
                )
                hidden_ref[:, lane : lane + half] = (jax.nn.silu(g) * u).astype(jnp.bfloat16)
        for at, step in column_chunks(width):
            put(
                at,
                step,
                jnp.dot(
                    hidden_ref[...],
                    down_ref[:, at : at + step],
                    preferred_element_type=jnp.float32,
                ),
            )

    def serve(owner):
        for half in range(halves):
            block_wait(*go, owner, half).wait_recv()
            for at, step in column_chunks(part):
                flat[:, half * part + at : half * part + at + step] = jnp.concatenate(
                    [
                        arrived[owner, half, spot, :, at : at + step].astype(jnp.float32)
                        for spot in range(ring)
                    ],
                    axis=0,
                ).astype(jnp.bfloat16)

        def put(at, step, value):
            half, lane = at // part, at % part
            for spot in range(ring):
                answer[owner, half, spot, :, lane : lane + step] = value[
                    spot * capacity : (spot + 1) * capacity
                ].astype(jnp.bfloat16)
            if lane + step == part:
                for ahead in range(1, ring):
                    block_copy(*back, owner, half, ahead).start()

        ffn(flat, gate, up, down, hidden, put)
        for half in range(halves):
            returned[owner, half, mine] = answer[owner, half, mine]

    def collect(owner, half):
        block_wait(*back, owner, half).wait_recv()
        slot, share = slots_of(owner)
        spread = jnp.concatenate(
            [
                jnp.where(slot[spot : spot + 1, :] == places, share[spot : spot + 1, :], 0.0)
                for spot in range(ring)
            ],
            axis=0,
        )
        coarse = spread.astype(jnp.bfloat16)
        fine = (spread - coarse.astype(jnp.float32)).astype(jnp.bfloat16)
        contract = (((0,), (0,)), ((), ()))
        for at, step in column_chunks(part):
            blocks = jnp.concatenate(
                [
                    returned[owner, half, spot, :, at : at + step].astype(jnp.float32)
                    for spot in range(ring)
                ],
                axis=0,
            ).astype(jnp.bfloat16)
            value = lax.dot_general(coarse, blocks, contract, preferred_element_type=jnp.float32)
            value = value + lax.dot_general(
                fine, blocks, contract, preferred_element_type=jnp.float32
            )

            @pl.when(owner == plane)
            def _():
                sums_own[half, :, at : at + step] = value

            @pl.when(owner != plane)
            def _():
                sums_out[owner, half, :, at : at + step] = value.astype(jnp.bfloat16)

        @pl.when(owner != plane)
        def _():
            sums_copy(owner, half).start()

    def share_expert():
        for load in loads[1:4]:
            load.wait()

        def put(at, step, value):
            total[:, at : at + step] += value

        ffn(normed, common_gate, common_up, common_down, residual, put)

    def step(turn, carry):
        code = pick(plans, plane, turn)
        half, owner, kind = code % halves, code // halves % planes, code // (halves * planes)

        @pl.when(kind == 0)
        def _():
            dispatch(owner, half)

        @pl.when(kind == 1)
        def _():
            serve(owner)

        @pl.when(kind == 2)
        def _():
            collect(owner, half)

        @pl.when(kind == 3)
        def _():
            share_expert()

        return carry

    for load in loads[4:]:
        load.wait()
    lax.fori_loop(0, len(plans[0]), step, 0)

    for ahead in range(1, planes):
        for half in range(halves):
            sums_wait((plane + ahead) % planes, half).wait_recv()

    def last_band(number, carry):
        spot = pl.ds(pl.multiple_of(number * band, band), band)
        for half in range(halves):
            lanes = slice(half * part, (half + 1) * part)
            value = total[spot, lanes] + sums_own[half, spot, :]
            for ahead in range(1, planes):
                value = value + sums_in[(plane + ahead) % planes, half, spot, :].astype(
                    jnp.float32
                )
            out_ref[spot, lanes] = value.astype(jnp.bfloat16)
        return carry

    lax.fori_loop(0, count // band, last_band, 0)

    for ahead in range(1, tp_count):
        for copy in part_copies(ahead):
            copy.wait_send()
    for ahead in range(1, planes):
        for copy in table_copies(ahead, plane):
            copy.wait_send()

    def drain(code, carry):
        owner, half = code // halves, code % halves
        block_wait(*go, owner, half).wait_send()
        block_wait(*back, owner, half).wait_send()

        @pl.when(owner != plane)
        def _():
            sums_copy(owner, half).wait_send()

        @pl.when((owner <= plane) & (plane < planes - 1))
        def _():
            rows_copy(owner, half, plane + 1, rows_up).wait_send()

        @pl.when((owner >= plane) & (plane > 0))
        def _():
            rows_copy(owner, half, plane - 1, rows_down).wait_send()

        return carry

    lax.fori_loop(0, planes * halves, drain, 0)


def mixer_stage(
    heads,
    groups,
    owners,
    head_dim,
    signal_in,
    write_in,
    read_in,
    gate_in,
    step_in,
    log_in,
    signal_taps,
    write_taps,
    read_taps,
    bias,
    rate,
    direct,
    gain,
    mixed,
    halo_signal,
    halo_write,
    halo_read,
    extended,
    signal,
    write_vec,
    read_vec,
    scaled,
    tailed,
    readout,
    states,
    summed,
    piece_out,
    piece_in,
    decay_out,
    decay_in,
    start_out,
    start_in,
    halo_send,
    halo_recv,
    piece_send,
    piece_recv,
    decay_send,
    decay_recv,
    start_send,
    start_recv,
):
    chip, core = lax.axis_index("sp"), lax.axis_index("tp")
    chips = lax.axis_size("sp")
    length, wide = signal_in.shape
    narrow = write_in.shape[1]
    rim = halo_signal.shape[0]
    taps = signal_taps.shape[0]
    blocks = length // BLK
    per_group = heads // groups
    span = per_group * head_dim
    rows = STATE // owners
    f32, bf16 = jnp.float32, jnp.bfloat16
    exact = lax.Precision.HIGHEST

    def halo_copies(target):
        return [
            pltpu.make_async_remote_copy(
                src_ref=source.at[pl.ds(length - rim, rim), :],
                dst_ref=halo,
                send_sem=halo_send.at[number],
                recv_sem=halo_recv.at[number],
                device_id=(target, core),
                device_id_type=MESH,
            )
            for number, (source, halo) in enumerate(
                [(signal_in, halo_signal), (write_in, halo_write), (read_in, halo_read)]
            )
        ]

    @pl.when(chip < chips - 1)
    def _():
        for copy in halo_copies(chip + 1):
            copy.start()

    timestep = step_in[...].astype(f32).T + bias[...]
    timestep = jnp.maximum(timestep, 0.0) + jnp.log1p(jnp.exp(-jnp.abs(timestep)))
    log_decay = log_in[...].T - rate[...] * timestep
    first = lax.broadcasted_iota(jnp.int32, (BLK, BLK), 0)
    second = lax.broadcasted_iota(jnp.int32, (BLK, BLK), 1)
    causal = first >= second
    lower = jnp.where(causal, 1.0, 0.0)
    cums = [
        jnp.dot(
            lower,
            log_decay[b * BLK : (b + 1) * BLK],
            precision=exact,
            preferred_element_type=f32,
        )
        for b in range(blocks)
    ]
    part = lax.broadcasted_iota(jnp.int32, (heads, wide), 0)
    lane = lax.broadcasted_iota(jnp.int32, (heads, wide), 1) // head_dim
    widen = jnp.where(part == lane, 1.0, 0.0).astype(bf16)

    def expand(value):
        high = value.astype(bf16)
        rest = value - high.astype(f32)
        middle = rest.astype(bf16)
        low = (rest - middle.astype(f32)).astype(bf16)
        return (
            jnp.dot(high, widen, preferred_element_type=f32)
            + jnp.dot(middle, widen, preferred_element_type=f32)
            + jnp.dot(low, widen, preferred_element_type=f32)
        )

    for b in range(blocks):
        readout[b * BLK : (b + 1) * BLK, :] = expand(jnp.exp(cums[b]))
    decay = readout[BLK - 1 : BLK, :]
    for b in range(1, blocks):
        decay = decay * readout[(b + 1) * BLK - 1 : (b + 1) * BLK, :]
    decay_out[...] = decay

    def decay_copy(owner, device):
        return pltpu.make_async_remote_copy(
            src_ref=decay_out,
            dst_ref=decay_in.at[device],
            send_sem=decay_send.at[owner],
            recv_sem=decay_recv.at[device],
            device_id=(owner, core),
            device_id_type=MESH,
        )

    def piece_copy(owner, device):
        return pltpu.make_async_remote_copy(
            src_ref=piece_out.at[owner],
            dst_ref=piece_in.at[device],
            send_sem=piece_send.at[owner],
            recv_sem=piece_recv.at[device],
            device_id=(owner, core),
            device_id_type=MESH,
        )

    def start_copy(owner, device):
        return pltpu.make_async_remote_copy(
            src_ref=start_out.at[device],
            dst_ref=start_in.at[owner],
            send_sem=start_send.at[device],
            recv_sem=start_recv.at[owner],
            device_id=(device, core),
            device_id_type=MESH,
        )

    def others(number, act):
        for at in range(number):

            @pl.when(at != chip)
            def _():
                act(at)

    others(owners, lambda owner: decay_copy(owner, chip).start())

    @pl.when(chip < owners)
    def _():
        decay_in[chip] = decay_out[...]

    parts = [
        (signal_in, halo_signal, signal_taps, 0, wide),
        (write_in, halo_write, write_taps, wide, narrow),
        (read_in, halo_read, read_taps, wide + narrow, narrow),
    ]
    head_room = 8
    for source, _, _, at, size in parts:
        extended[head_room : head_room + length, at : at + size] = source[...].astype(f32)

    @pl.when(chip > 0)
    def _():
        for copy in halo_copies(chip):
            copy.wait_recv()
        for _, halo, _, at, size in parts:
            extended[0:head_room, at : at + size] = halo[rim - head_room : rim, :].astype(f32)

    @pl.when(chip == 0)
    def _():
        extended[0:head_room, :] = jnp.zeros((head_room, extended.shape[1]), f32)

    def convolve(weights, at, size, put):
        for b in range(blocks):
            for lanes in range(0, size, 256):
                total = None
                for tap in range(taps):
                    begin = head_room - taps + 1 + tap + b * BLK
                    term = (
                        weights[tap : tap + 1, lanes : lanes + 256].astype(f32)
                        * extended[begin : begin + BLK, at + lanes : at + lanes + 256]
                    )
                    total = term if total is None else total + term
                put(b, lanes, jax.nn.silu(total))

    def put_write(b, lanes, value):
        write_vec[b * BLK : (b + 1) * BLK, lanes : lanes + 256] = value.astype(bf16)

    def put_read(b, lanes, value):
        read_vec[b * BLK : (b + 1) * BLK, lanes : lanes + 256] = value.astype(bf16)

    def put_signal(b, lanes, value):
        signal[b * BLK : (b + 1) * BLK, lanes : lanes + 256] = value

    convolve(write_taps, wide, narrow, put_write)
    convolve(signal_taps, 0, wide, put_signal)
    for b in range(blocks):
        spot = slice(b * BLK, (b + 1) * BLK)
        step = timestep[spot]
        scaled[spot, :] = (signal[spot, :] * expand(step)).astype(bf16)
        rest = jnp.exp(cums[b][BLK - 1 : BLK, :] - cums[b])
        tailed[spot, :] = (signal[spot, :] * expand(step * rest)).astype(bf16)
        for g in range(groups):
            states[b, :, g * span : (g + 1) * span] = lax.dot_general(
                write_vec[spot, g * STATE : (g + 1) * STATE],
                tailed[spot, g * span : (g + 1) * span],
                (((0,), (0,)), ((), ())),
                preferred_element_type=f32,
            )
    for owner in range(owners):
        spot = slice(owner * rows, (owner + 1) * rows)
        value = states[0, spot, :]
        for b in range(1, blocks):
            value = value * readout[(b + 1) * BLK - 1 : (b + 1) * BLK, :] + states[b, spot, :]
        piece_out[owner] = value.astype(bf16)
    others(owners, lambda owner: piece_copy(owner, chip).start())

    @pl.when(chip < owners)
    def _():
        piece_in[chip] = piece_out[chip]

    convolve(read_taps, wide + narrow, narrow, put_read)
    spread_direct = expand(jnp.broadcast_to(direct[...], (8, heads)))[0:1, :]
    low_lanes = lax.broadcasted_iota(jnp.int32, (BLK, 2 * head_dim), 1) < head_dim
    for b in range(blocks):
        spot = slice(b * BLK, (b + 1) * BLK)
        turned = cums[b].T
        for g in range(groups):
            inner = slice(g * STATE, (g + 1) * STATE)
            meeting = lax.dot_general(
                read_vec[spot, inner],
                write_vec[spot, inner],
                (((1,), (1,)), ((), ())),
                preferred_element_type=f32,
            )
            for pair in range(per_group // 2):
                head = g * per_group + 2 * pair
                lanes = slice(head * head_dim, (head + 2) * head_dim)
                weights = []
                for at in (head, head + 1):
                    gap = cums[b][:, at : at + 1] - turned[at : at + 1, :]
                    weights.append(
                        (meeting * jnp.exp(jnp.where(causal, gap, -jnp.inf))).astype(bf16)
                    )
                value = scaled[spot, lanes]
                zero = jnp.zeros_like(value)
                both = jnp.concatenate(
                    [jnp.where(low_lanes, value, zero), jnp.where(low_lanes, zero, value)], axis=0
                )
                summed[spot, lanes] = spread_direct[:, lanes] * signal[spot, lanes] + jnp.dot(
                    jnp.concatenate(weights, axis=1), both, preferred_element_type=f32
                )

    @pl.when(chip < owners)
    def _():
        def scan(device, held):
            @pl.when(device != chip)
            def _():
                decay_copy(chip, device).wait_recv()
                piece_copy(chip, device).wait_recv()

            start_out[device] = held.astype(bf16)

            @pl.when(device != chip)
            def _():
                start_copy(chip, device).start()

            return held * decay_in[device] + piece_in[device].astype(f32)

        lax.fori_loop(0, chips, scan, jnp.zeros((rows, wide), f32))
        start_in[chip] = start_out[chip]

    others(owners, lambda owner: start_copy(owner, chip).wait_recv())
    start = jnp.concatenate([start_in[owner].astype(f32) for owner in range(owners)], axis=0)
    for b in range(blocks):
        spot = slice(b * BLK, (b + 1) * BLK)
        if b:
            start = (
                start * readout[b * BLK - 1 : b * BLK, :] + states[b - 1]
            )
        rounded = start.astype(bf16)
        for g in range(groups):
            lanes = slice(g * span, (g + 1) * span)
            near = jnp.dot(
                read_vec[spot, g * STATE : (g + 1) * STATE],
                rounded[:, lanes],
                preferred_element_type=f32,
            )
            value = summed[spot, lanes] + near * readout[spot, lanes]
            value = value * jax.nn.silu(gate_in[spot, lanes].astype(f32))
            scale = lax.rsqrt(jnp.mean(value * value, axis=-1, keepdims=True) + 1e-06)
            mixed[spot, lanes] = (value * scale * gain[:, lanes]).astype(bf16)

    @pl.when(chip < chips - 1)
    def _():
        for copy in halo_copies(chip + 1):
            copy.wait_send()

    others(owners, lambda owner: decay_copy(owner, chip).wait_send())
    others(owners, lambda owner: piece_copy(owner, chip).wait_send())

    @pl.when(chip < owners)
    def _():
        others(chips, lambda device: start_copy(chip, device).wait_send())


def mixer_scratch(chips, owners, length, wide, narrow, blocks):
    f32, bf16 = jnp.float32, jnp.bfloat16
    dma = pltpu.SemaphoreType.DMA
    rows = STATE // owners
    rim = 16
    return [
        pltpu.VMEM((rim, wide), bf16),
        pltpu.VMEM((rim, narrow), bf16),
        pltpu.VMEM((rim, narrow), bf16),
        pltpu.VMEM((length + 8, wide + 2 * narrow), f32),
        pltpu.VMEM((length, wide), f32),
        pltpu.VMEM((length, narrow), bf16),
        pltpu.VMEM((length, narrow), bf16),
        pltpu.VMEM((length, wide), bf16),
        pltpu.VMEM((length, wide), bf16),
        pltpu.VMEM((length, wide), f32),
        pltpu.VMEM((blocks, STATE, wide), f32),
        pltpu.VMEM((length, wide), f32),
        pltpu.VMEM((owners, rows, wide), bf16),
        pltpu.VMEM((chips, rows, wide), bf16),
        pltpu.VMEM((1, wide), f32),
        pltpu.VMEM((chips, 1, wide), f32),
        pltpu.VMEM((chips, rows, wide), bf16),
        pltpu.VMEM((owners, rows, wide), bf16),
        dma((3,)),
        dma((3,)),
        dma((owners,)),
        dma((chips,)),
        dma((owners,)),
        dma((chips,)),
        dma((chips,)),
        dma((owners,)),
    ]


def layer_kernel(tail_sizes, mixer_sizes, mixer_scratch_count, *refs):
    mixer_in, tail_in, out = refs[:13], refs[13:24], refs[24]
    mixed = refs[25]
    mixer_refs = refs[26 : 26 + mixer_scratch_count]
    tail_refs = refs[26 + mixer_scratch_count :]

    def mix():
        mixer_stage(*mixer_sizes, *mixer_in, mixed, *mixer_refs)

    tail_stage(*tail_sizes, mix, mixed, *tail_in, out, *tail_refs)


def layer(mixer_in, tail_in):
    sp_count, tp_count = lax.axis_size("sp"), lax.axis_size("tp")
    bf16, f32 = jnp.bfloat16, jnp.float32
    dma = pltpu.SemaphoreType.DMA
    vmem, anywhere = pl.BlockSpec(memory_space=pltpu.VMEM), pl.BlockSpec(memory_space=pl.ANY)
    length, wide = mixer_in[0].shape
    narrow = mixer_in[1].shape[1]
    heads = mixer_in[4].shape[0]
    owners = min(sp_count, STATE // 8)
    mixer_sizes = (heads, narrow // STATE, owners, wide // heads)
    mixer_refs = mixer_scratch(sp_count, owners, length, wide, narrow, length // BLK)
    stream, _, index, _, out_weight, gate, up, down, common_gate, common_up, common_down = tail_in
    planes = PLANES if sp_count % PLANES == 0 else 1
    ring = sp_count // planes * tp_count
    count, width = stream.shape
    fanout = index.shape[0]
    experts = sp_count * tp_count
    capacity = max(2, (3 * count * fanout + 2 * experts - 1) // (2 * experts))
    capacity = (capacity + 7) // 8 * 8
    part = width // HALVES
    chunks = len(column_chunks(width))
    slots = (planes, HALVES, ring, capacity, part)
    pieces = (planes, HALVES, count, part)
    return pl.pallas_call(
        functools.partial(
            layer_kernel,
            (planes, ring, tp_count, capacity, fanout),
            mixer_sizes,
            len(mixer_refs),
        ),
        out_shape=jax.ShapeDtypeStruct((count, width), bf16),
        in_specs=[vmem] * 17 + [anywhere] * 7,
        out_specs=vmem,
        scratch_shapes=[
            pltpu.VMEM((length, wide), bf16),
            *mixer_refs,
            pltpu.VMEM(out_weight.shape, bf16),
            pltpu.VMEM(gate.shape[1:], bf16),
            pltpu.VMEM(up.shape[1:], bf16),
            pltpu.VMEM(down.shape[1:], bf16),
            pltpu.VMEM(common_gate.shape, bf16),
            pltpu.VMEM(common_up.shape, bf16),
            pltpu.VMEM(common_down.shape, bf16),
            pltpu.VMEM((planes, fanout, count), jnp.int32),
            pltpu.VMEM((planes, fanout, count), f32),
            pltpu.VMEM((count, width), f32),
            pltpu.VMEM((count, common_gate.shape[1]), bf16),
            pltpu.VMEM((tp_count - 1, count, width), bf16),
            pltpu.VMEM((tp_count - 1, count, width), bf16),
            pltpu.VMEM((count, width), bf16),
            pltpu.VMEM(pieces, bf16),
            pltpu.VMEM(slots, bf16),
            pltpu.VMEM(slots, bf16),
            pltpu.VMEM((ring * capacity, width), bf16),
            pltpu.VMEM((ring * capacity, gate.shape[2]), bf16),
            pltpu.VMEM(slots, bf16),
            pltpu.VMEM(slots, bf16),
            pltpu.VMEM(pieces[1:], f32),
            pltpu.VMEM(pieces, bf16),
            pltpu.VMEM(pieces, bf16),
            dma((7,)),
            dma((tp_count - 1, chunks)),
            dma((tp_count - 1, chunks)),
            dma((2, planes)),
            dma((2, planes)),
            *[dma((planes, HALVES))] * 9,
        ],
        compiler_params=pltpu.CompilerParams(
            collective_id=0, has_side_effects=True, vmem_limit_bytes=62 * 2**20
        ),
    )(*mixer_in, *tail_in)


def on_device(
    stream,
    head_input_signal,
    write_input_vectors,
    read_input_vectors,
    output_gate_input,
    step_size_input,
    position_log_decay,
    signal_filter_taps,
    write_filter_taps,
    read_filter_taps,
    step_size_bias,
    head_decay_rate,
    head_direct_term,
    grouped_norm_gain,
    mixer_output_weight,
    expert_norm_gain,
    chosen_expert_index,
    chosen_expert_weight,
    routed_gate_weight,
    routed_up_weight,
    routed_down_weight,
    common_gate_weight,
    common_up_weight,
    common_down_weight,
):
    row = lambda part: part.reshape(1, -1)
    return layer(
        (
            head_input_signal,
            write_input_vectors,
            read_input_vectors,
            output_gate_input,
            step_size_input.T,
            position_log_decay.T,
            signal_filter_taps,
            write_filter_taps,
            read_filter_taps,
            row(step_size_bias),
            row(head_decay_rate),
            row(head_direct_term),
            row(grouped_norm_gain),
        ),
        (
            stream,
            row(expert_norm_gain),
            chosen_expert_index.T,
            chosen_expert_weight.T,
            mixer_output_weight,
            routed_gate_weight,
            routed_up_weight,
            routed_down_weight,
            common_gate_weight,
            common_up_weight,
            common_down_weight,
        ),
    )


def solution(mesh):
    in_specs = (
        P(("sp", "tp"), None),
        P("sp", "tp"),
        P("sp", "tp"),
        P("sp", "tp"),
        P("sp", "tp"),
        P("sp", "tp"),
        P("sp", "tp"),
        P(None, "tp"),
        P(None, "tp"),
        P(None, "tp"),
        P("tp"),
        P("tp"),
        P("tp"),
        P("tp"),
        P("tp", None),
        P(),
        P(("sp", "tp"), None),
        P(("sp", "tp"), None),
        P(("sp", "tp"), None, None),
        P(("sp", "tp"), None, None),
        P(("sp", "tp"), None, None),
        P(),
        P(),
        P(),
    )
    out_specs = P(("sp", "tp"), None)
    return jax.shard_map(
        on_device, mesh=mesh, in_specs=in_specs, out_specs=out_specs, check_vma=False
    )
```

```python
import functools

import jax
import jax.numpy as jnp
from jax import lax
from jax.experimental import pallas as pl
from jax.experimental.pallas import tpu as pltpu
from jax.sharding import PartitionSpec as P

STATE = 128
BLK = 128


MESH = pl.DeviceIdType.MESH
PLANES = 4
HALVES = 2
COLS = 512


LINE_END = [
    (0, 0, 0), (0, 0, 1), (0, 1, 0), (0, 1, 1), (0, 2, 0), (0, 2, 1),
    (0, 3, 0), (1, 2, 0), (2, 2, 0), (0, 3, 1), (2, 2, 1), (3, 0, 0),
    (1, 3, 0), (2, 3, 0), (1, 1, 0), (1, 0, 0), (2, 3, 1), (2, 1, 0),
    (2, 1, 1), (2, 0, 0), (2, 0, 1),
]
LINE_NEXT = [
    (0, 1, 0), (0, 1, 1), (3, 1, 0), (0, 0, 0), (0, 2, 0), (0, 2, 1),
    (0, 3, 0), (0, 0, 1), (1, 2, 0), (1, 0, 0), (0, 3, 1), (1, 1, 0),
    (2, 0, 0), (2, 2, 0), (1, 3, 0), (2, 1, 0), (2, 2, 1), (2, 0, 1),
    (2, 3, 0), (2, 3, 1), (2, 1, 1),
]


def line_plans(planes, halves):
    if (planes, halves) == (4, 2):
        mirror = lambda plan: [(kind, 3 - owner, half) for kind, owner, half in plan]
        plans = [LINE_END, LINE_NEXT, mirror(LINE_NEXT), mirror(LINE_END)]
    else:
        plans = []
        for z in range(planes):
            near = sorted(range(planes), key=lambda s: (abs(s - z), s))
            plan = [(0, s, h) for s in near for h in range(halves)] + [(3, 0, 0)]
            for s in near:
                plan += [(1, s, 0)] + [(2, s, h) for h in range(halves)]
            plans.append(plan)
    return [[(k * planes + s) * halves + h for k, s, h in plan] for plan in plans]


def column_chunks(width):
    step = min(COLS, width)
    return [(at, step) for at in range(0, width, step)]


def pick(values, place, which):
    chosen = jnp.int32(0)
    for spot, row in enumerate(values):
        chosen = chosen + (place == spot).astype(jnp.int32) * pick_one(row, which)
    return chosen


def pick_one(row, which):
    chosen = jnp.int32(0)
    for spot, value in enumerate(row):
        chosen = chosen + (which == spot).astype(jnp.int32) * value
    return chosen


def bytes_of(ref, number, send_sem, recv_sem):
    view = ref.at[pl.ds(0, number)]
    return pltpu.make_async_remote_copy(
        src_ref=view,
        dst_ref=view,
        send_sem=send_sem,
        recv_sem=recv_sem,
        device_id=(lax.axis_index("sp"), lax.axis_index("tp")),
        device_id_type=MESH,
    )


def tail_stage(
    planes,
    ring,
    tp_count,
    capacity,
    fanout,
    mix,
    mixed_ref,
    stream_ref,
    gain_ref,
    index_ref,
    weight_ref,
    out_weight_hbm,
    gate_hbm,
    up_hbm,
    down_hbm,
    common_gate_hbm,
    common_up_hbm,
    common_down_hbm,
    out_ref,
    out_weight,
    gate,
    up,
    down,
    common_gate,
    common_up,
    common_down,
    index_tables,
    weight_tables,
    total,
    residual,
    part_out,
    part_in,
    normed,
    rows,
    sent,
    arrived,
    flat,
    hidden,
    answer,
    returned,
    sums_own,
    sums_out,
    sums_in,
    relay_in,
    weight_sem,
    part_send,
    part_recv,
    table_send,
    table_recv,
    rows_up,
    rows_down,
    rows_recv,
    go_send,
    go_recv,
    back_send,
    back_recv,
    sums_send,
    sums_recv,
    relay_recv,
):
    chip = lax.axis_index("sp")
    core = lax.axis_index("tp")
    chips = ring // tp_count
    plane = chip // chips
    mine = (chip % chips) * tp_count + core
    count, width = stream_ref.shape
    halves = rows.shape[1]
    part = width // halves
    plans = line_plans(planes, halves)

    def in_plane(spot):
        return (plane * chips + spot // tp_count, spot % tp_count)

    def in_line(spot):
        return (spot * chips + chip % chips, core)

    loads = [
        pltpu.make_async_copy(source, target, weight_sem.at[number])
        for number, (source, target) in enumerate(
            [
                (out_weight_hbm, out_weight),
                (common_gate_hbm, common_gate),
                (common_up_hbm, common_up),
                (common_down_hbm, common_down),
                (gate_hbm.at[0], gate),
                (up_hbm.at[0], up),
                (down_hbm.at[0], down),
            ]
        )
    ]
    for load in loads:
        load.start()

    barrier = pltpu.get_barrier_semaphore()
    all_chips = lax.axis_size("sp")
    for ahead in range(1, all_chips):
        pl.semaphore_signal(
            barrier, inc=1, device_id=((chip + ahead) % all_chips, core), device_id_type=MESH
        )
    for spot in range(chips):
        for ahead in range(1, tp_count):
            pl.semaphore_signal(
                barrier,
                inc=1,
                device_id=(plane * chips + spot, (core + ahead) % tp_count),
                device_id_type=MESH,
            )
    pl.semaphore_wait(barrier, all_chips - 1 + chips * (tp_count - 1))

    def table_copies(ahead, owner):
        return [
            pltpu.make_async_remote_copy(
                src_ref=source,
                dst_ref=held.at[owner],
                send_sem=table_send.at[number],
                recv_sem=table_recv.at[number],
                device_id=in_line((plane + ahead) % planes),
                device_id_type=MESH,
            )
            for number, (source, held) in enumerate(
                [(index_ref, index_tables), (weight_ref, weight_tables)]
            )
        ]

    for ahead in range(1, planes):
        for copy in table_copies(ahead, plane):
            copy.start()
    index_tables[plane] = index_ref[...]
    weight_tables[plane] = weight_ref[...]
    relayed = planes == 4
    if relayed:

        @pl.when(plane == 0)
        def _():
            sums_in[planes - 1] = jnp.zeros(sums_in.shape[1:], jnp.bfloat16)

        @pl.when(plane == planes - 1)
        def _():
            sums_in[0] = jnp.zeros(sums_in.shape[1:], jnp.bfloat16)

    mix()
    table_totals = [
        bytes_of(held, planes - 1, table_send.at[number], table_recv.at[number])
        for number, held in enumerate([index_tables, weight_tables])
    ]
    if planes > 1:
        for total_copy in table_totals:
            total_copy.wait_recv()

    def part_copies(ahead):
        return [
            pltpu.make_async_remote_copy(
                src_ref=part_out.at[ahead - 1, :, pl.ds(at, step)],
                dst_ref=part_in.at[ahead - 1, :, pl.ds(at, step)],
                send_sem=part_send.at[ahead - 1],
                recv_sem=part_recv.at[ahead - 1, number],
                device_id=(chip, (core + ahead) % tp_count),
                device_id_type=MESH,
            )
            for number, (at, step) in enumerate(column_chunks(width))
        ]

    loads[0].wait()
    for ahead in range(1, tp_count):
        owner = (core + ahead) % tp_count
        held = mixed_ref[pl.ds(pl.multiple_of(owner * count, count), count), :]
        copies = part_copies(ahead)
        for number, (at, step) in enumerate(column_chunks(width)):
            part_out[ahead - 1, :, at : at + step] = jnp.dot(
                held, out_weight[:, at : at + step], preferred_element_type=jnp.float32
            ).astype(jnp.bfloat16)
            copies[number].start()
    held = mixed_ref[pl.ds(pl.multiple_of(core * count, count), count), :]
    for at, step in column_chunks(width):
        total[:, at : at + step] = stream_ref[:, at : at + step].astype(jnp.float32) + jnp.dot(
            held, out_weight[:, at : at + step], preferred_element_type=jnp.float32
        )
    for ahead in range(1, tp_count):
        for copy in part_copies(ahead):
            copy.wait_recv()
    band = 16

    def norm_band(number, carry):
        spot = pl.ds(pl.multiple_of(number * band, band), band)
        summed = total[spot, :]
        for ahead in range(1, tp_count):
            summed = summed + part_in[ahead - 1, spot, :].astype(jnp.float32)
        rounded = summed.astype(jnp.bfloat16)
        wide = rounded.astype(jnp.float32)
        total[spot, :] = wide
        scale = lax.rsqrt(jnp.mean(wide * wide, axis=-1, keepdims=True) + 1e-06)
        value = (wide * scale * gain_ref[...]).astype(jnp.bfloat16)
        normed[spot, :] = value
        for half in range(halves):
            rows[plane, half, spot, :] = value[:, half * part : (half + 1) * part]
        return carry

    lax.fori_loop(0, count // band, norm_band, 0)

    def rows_copy(owner, half, target, sem):
        return pltpu.make_async_remote_copy(
            src_ref=rows.at[owner, half],
            dst_ref=rows.at[owner, half],
            send_sem=sem.at[owner, half],
            recv_sem=rows_recv.at[owner, half],
            device_id=in_line(target),
            device_id_type=MESH,
        )

    def block_copy(source, target, send, recv, owner, half, ahead):
        spot = (mine + ahead) % ring
        return pltpu.make_async_remote_copy(
            src_ref=source.at[owner, half, spot],
            dst_ref=target.at[owner, half, mine],
            send_sem=send.at[0],
            recv_sem=recv.at[owner, half],
            device_id=in_plane(spot),
            device_id_type=MESH,
        )

    def block_wait(source, target, send, recv, owner, half):
        return pltpu.make_async_remote_copy(
            src_ref=source.at[owner, half, pl.ds(0, ring - 1)],
            dst_ref=target.at[owner, half, pl.ds(0, ring - 1)],
            send_sem=send.at[0],
            recv_sem=recv.at[owner, half],
            device_id=in_plane((mine + 1) % ring),
            device_id_type=MESH,
        )

    go = (sent, arrived, go_send, go_recv)
    back = (answer, returned, back_send, back_recv)

    def sums_copy(owner, half):
        return pltpu.make_async_remote_copy(
            src_ref=sums_out.at[owner, half],
            dst_ref=sums_in.at[plane, half],
            send_sem=sums_send.at[0],
            recv_sem=sums_recv.at[0],
            device_id=in_line(owner),
            device_id_type=MESH,
        )

    def relay_copy(owner, half):
        return pltpu.make_async_remote_copy(
            src_ref=sums_out.at[owner, half],
            dst_ref=relay_in.at[half],
            send_sem=sums_send.at[0],
            recv_sem=relay_recv.at[half],
            device_id=in_line(plane + 1 - 2 * (plane // (planes - 1))),
            device_id_type=MESH,
        )

    def slots_of(owner):
        table, parts = index_tables[owner], weight_tables[owner]
        names = lax.broadcasted_iota(jnp.int32, (ring, count), 0) + plane * ring
        hits = jnp.zeros((ring, count), jnp.float32)
        share = jnp.zeros((ring, count), jnp.float32)
        for turn in range(fanout):
            named = table[turn : turn + 1, :] == names
            hits = hits + jnp.where(named, 1.0, 0.0)
            share = share + jnp.where(named, parts[turn : turn + 1, :], 0.0)
        before = lax.broadcasted_iota(jnp.int32, (count, count), 0)
        after = lax.broadcasted_iota(jnp.int32, (count, count), 1)
        earlier = jnp.where(before < after, 1.0, 0.0).astype(jnp.bfloat16)
        slot = jnp.dot(hits.astype(jnp.bfloat16), earlier, preferred_element_type=jnp.float32)
        return jnp.where(hits > 0.5, slot, -1.0), share

    places = lax.broadcasted_iota(jnp.int32, (capacity, count), 0).astype(jnp.float32)

    def dispatch(owner, half):
        @pl.when(owner != plane)
        def _():
            rows_copy(owner, half, owner, rows_up).wait_recv()

        @pl.when((owner <= plane) & (plane < planes - 1))
        def _():
            rows_copy(owner, half, plane + 1, rows_up).start()

        @pl.when((owner >= plane) & (plane > 0))
        def _():
            rows_copy(owner, half, plane - 1, rows_down).start()

        slot, _ = slots_of(owner)
        chosen = jnp.concatenate(
            [
                jnp.where(slot[spot : spot + 1, :] == places, 1.0, 0.0)
                for spot in range(ring)
            ],
            axis=0,
        ).astype(jnp.bfloat16)
        for at, step in column_chunks(part):
            picked = jnp.dot(
                chosen, rows[owner, half, :, at : at + step], preferred_element_type=jnp.float32
            )
            for spot in range(ring):
                sent[owner, half, spot, :, at : at + step] = picked[
                    spot * capacity : (spot + 1) * capacity
                ].astype(jnp.bfloat16)
        for ahead in range(1, ring):
            block_copy(*go, owner, half, ahead).start()
        arrived[owner, half, mine] = sent[owner, half, mine]

    def ffn(x_ref, gate_ref, up_ref, down_ref, hidden_ref, put):
        for at, step in column_chunks(gate_ref.shape[1]):
            half = step // 2
            for lane in (at, at + half):
                g = jnp.dot(
                    x_ref[...], gate_ref[:, lane : lane + half], preferred_element_type=jnp.float32
                )
                u = jnp.dot(
                    x_ref[...], up_ref[:, lane : lane + half], preferred_element_type=jnp.float32
                )
                hidden_ref[:, lane : lane + half] = (jax.nn.silu(g) * u).astype(jnp.bfloat16)
        for at, step in column_chunks(width):
            put(
                at,
                step,
                jnp.dot(
                    hidden_ref[...],
                    down_ref[:, at : at + step],
                    preferred_element_type=jnp.float32,
                ),
            )

    def serve(owner):
        for half in range(halves):
            block_wait(*go, owner, half).wait_recv()
            for at, step in column_chunks(part):
                flat[:, half * part + at : half * part + at + step] = jnp.concatenate(
                    [
                        arrived[owner, half, spot, :, at : at + step].astype(jnp.float32)
                        for spot in range(ring)
                    ],
                    axis=0,
                ).astype(jnp.bfloat16)

        def put(at, step, value):
            half, lane = at // part, at % part
            for spot in range(ring):
                answer[owner, half, spot, :, lane : lane + step] = value[
                    spot * capacity : (spot + 1) * capacity
                ].astype(jnp.bfloat16)
            if lane + step == part:
                for ahead in range(1, ring):
                    block_copy(*back, owner, half, ahead).start()

        ffn(flat, gate, up, down, hidden, put)
        for half in range(halves):
            returned[owner, half, mine] = answer[owner, half, mine]

    def collect(owner, half):
        block_wait(*back, owner, half).wait_recv()
        ends = helps = jnp.bool_(False)
        if relayed:
            last = planes - 1
            ends = ((plane == 0) & (owner == last)) | ((plane == last) & (owner == 0))
            helps = ((plane == 1) & (owner == last)) | ((plane == last - 1) & (owner == 0))

            @pl.when(helps)
            def _():
                relay_copy(owner, half).wait_recv()

        slot, share = slots_of(owner)
        spread = jnp.concatenate(
            [
                jnp.where(slot[spot : spot + 1, :] == places, share[spot : spot + 1, :], 0.0)
                for spot in range(ring)
            ],
            axis=0,
        )
        coarse = spread.astype(jnp.bfloat16)
        fine = (spread - coarse.astype(jnp.float32)).astype(jnp.bfloat16)
        contract = (((0,), (0,)), ((), ()))
        for at, step in column_chunks(part):
            blocks = jnp.concatenate(
                [
                    returned[owner, half, spot, :, at : at + step].astype(jnp.float32)
                    for spot in range(ring)
                ],
                axis=0,
            ).astype(jnp.bfloat16)
            value = lax.dot_general(coarse, blocks, contract, preferred_element_type=jnp.float32)
            value = value + lax.dot_general(
                fine, blocks, contract, preferred_element_type=jnp.float32
            )

            @pl.when(owner == plane)
            def _():
                sums_own[half, :, at : at + step] = value

            @pl.when((owner != plane) & ~helps)
            def _():
                sums_out[owner, half, :, at : at + step] = value.astype(jnp.bfloat16)

            if relayed:

                @pl.when(helps)
                def _():
                    sums_out[owner, half, :, at : at + step] = (
                        value + relay_in[half, :, at : at + step].astype(jnp.float32)
                    ).astype(jnp.bfloat16)

        @pl.when((owner != plane) & ~ends)
        def _():
            sums_copy(owner, half).start()

        if relayed:

            @pl.when(ends)
            def _():
                relay_copy(owner, half).start()

    def share_expert():
        for load in loads[1:4]:
            load.wait()

        def put(at, step, value):
            total[:, at : at + step] += value

        ffn(normed, common_gate, common_up, common_down, residual, put)

    def step(turn, carry):
        code = pick(plans, plane, turn)
        half, owner, kind = code % halves, code // halves % planes, code // (halves * planes)

        @pl.when(kind == 0)
        def _():
            dispatch(owner, half)

        @pl.when(kind == 1)
        def _():
            serve(owner)

        @pl.when(kind == 2)
        def _():
            collect(owner, half)

        @pl.when(kind == 3)
        def _():
            share_expert()

        return carry

    for load in loads[4:]:
        load.wait()
    lax.fori_loop(0, len(plans[0]), step, 0)

    for ahead in range(1, tp_count):
        pltpu.make_async_remote_copy(
            src_ref=part_out.at[ahead - 1],
            dst_ref=part_in.at[ahead - 1],
            send_sem=part_send.at[ahead - 1],
            recv_sem=part_recv.at[ahead - 1, 0],
            device_id=(chip, (core + ahead) % tp_count),
            device_id_type=MESH,
        ).wait_send()
    for source, target, send, recv in (go, back):
        pltpu.make_async_remote_copy(
            src_ref=source.at[:, :, pl.ds(0, ring - 1)],
            dst_ref=target.at[:, :, pl.ds(0, ring - 1)],
            send_sem=send.at[0],
            recv_sem=recv.at[0, 0],
            device_id=in_plane((mine + 1) % ring),
            device_id_type=MESH,
        ).wait_send()

    def drain(code, carry):
        owner, half = code // halves, code % halves

        @pl.when((owner <= plane) & (plane < planes - 1))
        def _():
            rows_copy(owner, half, plane + 1, rows_up).wait_send()

        @pl.when((owner >= plane) & (plane > 0))
        def _():
            rows_copy(owner, half, plane - 1, rows_down).wait_send()

        return carry

    lax.fori_loop(0, planes * halves, drain, 0)
    if planes > 1:
        for total_copy in table_totals:
            total_copy.wait_send()
        bytes_of(sums_out, planes - 1, sums_send.at[0], sums_recv.at[0]).wait_send()
        if relayed:
            at_end = (plane == 0) | (plane == planes - 1)

            @pl.when(at_end)
            def _():
                bytes_of(sums_in, planes - 2, sums_send.at[0], sums_recv.at[0]).wait_recv()

            @pl.when(~at_end)
            def _():
                bytes_of(sums_in, planes - 1, sums_send.at[0], sums_recv.at[0]).wait_recv()

        else:
            bytes_of(sums_in, planes - 1, sums_send.at[0], sums_recv.at[0]).wait_recv()

    def last_band(number, carry):
        spot = pl.ds(pl.multiple_of(number * band, band), band)
        for half in range(halves):
            lanes = slice(half * part, (half + 1) * part)
            value = total[spot, lanes] + sums_own[half, spot, :]
            for ahead in range(1, planes):
                value = value + sums_in[(plane + ahead) % planes, half, spot, :].astype(
                    jnp.float32
                )
            out_ref[spot, lanes] = value.astype(jnp.bfloat16)
        return carry

    lax.fori_loop(0, count // band, last_band, 0)


def mixer_stage(
    heads,
    groups,
    owners,
    head_dim,
    gate_ready,
    signal_in,
    write_in,
    read_in,
    gate_in,
    step_in,
    log_in,
    signal_taps,
    write_taps,
    read_taps,
    bias,
    rate,
    direct,
    gain,
    mixed,
    halo_signal,
    halo_write,
    halo_read,
    extended,
    signal,
    write_vec,
    read_vec,
    scaled,
    tailed,
    readout,
    states,
    summed,
    piece_out,
    piece_in,
    decay_out,
    decay_in,
    start_out,
    start_in,
    halo_send,
    halo_recv,
    piece_send,
    piece_recv,
    decay_send,
    decay_recv,
    start_send,
    start_recv,
):
    chip, core = lax.axis_index("sp"), lax.axis_index("tp")
    chips = lax.axis_size("sp")
    length, wide = signal_in.shape
    narrow = write_in.shape[1]
    rim = halo_signal.shape[0]
    taps = signal_taps.shape[0]
    blocks = length // BLK
    per_group = heads // groups
    span = per_group * head_dim
    rows = STATE // owners
    f32, bf16 = jnp.float32, jnp.bfloat16
    exact = lax.Precision.HIGHEST

    def halo_copies(target):
        return [
            pltpu.make_async_remote_copy(
                src_ref=source.at[pl.ds(length - rim, rim), :],
                dst_ref=halo,
                send_sem=halo_send.at[number],
                recv_sem=halo_recv.at[number],
                device_id=(target, core),
                device_id_type=MESH,
            )
            for number, (source, halo) in enumerate(
                [(signal_in, halo_signal), (write_in, halo_write), (read_in, halo_read)]
            )
        ]

    @pl.when(chip < chips - 1)
    def _():
        for copy in halo_copies(chip + 1):
            copy.start()

    timestep = step_in[...].astype(f32).T + bias[...]
    timestep = jnp.maximum(timestep, 0.0) + jnp.log1p(jnp.exp(-jnp.abs(timestep)))
    log_decay = log_in[...].T - rate[...] * timestep
    first = lax.broadcasted_iota(jnp.int32, (BLK, BLK), 0)
    second = lax.broadcasted_iota(jnp.int32, (BLK, BLK), 1)
    causal = first >= second
    lower = jnp.where(causal, 1.0, 0.0)
    cums = [
        jnp.dot(
            lower,
            log_decay[b * BLK : (b + 1) * BLK],
            precision=exact,
            preferred_element_type=f32,
        )
        for b in range(blocks)
    ]
    part = lax.broadcasted_iota(jnp.int32, (heads, wide), 0)
    lane = lax.broadcasted_iota(jnp.int32, (heads, wide), 1) // head_dim
    widen = jnp.where(part == lane, 1.0, 0.0).astype(bf16)

    def expand(value):
        high = value.astype(bf16)
        rest = value - high.astype(f32)
        middle = rest.astype(bf16)
        low = (rest - middle.astype(f32)).astype(bf16)
        return (
            jnp.dot(high, widen, preferred_element_type=f32)
            + jnp.dot(middle, widen, preferred_element_type=f32)
            + jnp.dot(low, widen, preferred_element_type=f32)
        )

    for b in range(blocks):
        readout[b * BLK : (b + 1) * BLK, :] = expand(jnp.exp(cums[b]))
    decay = readout[BLK - 1 : BLK, :]
    for b in range(1, blocks):
        decay = decay * readout[(b + 1) * BLK - 1 : (b + 1) * BLK, :]
    decay_out[...] = decay

    def decay_copy(owner, device):
        return pltpu.make_async_remote_copy(
            src_ref=decay_out,
            dst_ref=decay_in.at[device],
            send_sem=decay_send.at[0],
            recv_sem=decay_recv.at[0],
            device_id=(owner, core),
            device_id_type=MESH,
        )

    def piece_copy(owner, device):
        return pltpu.make_async_remote_copy(
            src_ref=piece_out.at[owner],
            dst_ref=piece_in.at[device],
            send_sem=piece_send.at[0],
            recv_sem=piece_recv.at[device],
            device_id=(owner, core),
            device_id_type=MESH,
        )

    def start_copy(owner, device):
        return pltpu.make_async_remote_copy(
            src_ref=start_out.at[device],
            dst_ref=start_in.at[owner],
            send_sem=start_send.at[0],
            recv_sem=start_recv.at[0],
            device_id=(device, core),
            device_id_type=MESH,
        )

    def others(number, act):
        for at in range(number):

            @pl.when(at != chip)
            def _():
                act(at)

    def with_others(act):
        if owners == chips:
            act(owners - 1)
        else:

            @pl.when(chip < owners)
            def _():
                act(owners - 1)

            @pl.when(chip >= owners)
            def _():
                act(owners)

    others(owners, lambda owner: decay_copy(owner, chip).start())

    @pl.when(chip < owners)
    def _():
        decay_in[chip] = decay_out[...]

    parts = [
        (signal_in, halo_signal, signal_taps, 0, wide),
        (write_in, halo_write, write_taps, wide, narrow),
        (read_in, halo_read, read_taps, wide + narrow, narrow),
    ]
    head_room = 8
    for source, _, _, at, size in parts:
        extended[head_room : head_room + length, at : at + size] = source[...].astype(f32)

    def convolve(b, weights, at, size, put):
        for lanes in range(0, size, 256):
            total = None
            for tap in range(taps):
                begin = head_room - taps + 1 + tap + b * BLK
                term = (
                    weights[tap : tap + 1, lanes : lanes + 256].astype(f32)
                    * extended[begin : begin + BLK, at + lanes : at + lanes + 256]
                )
                total = term if total is None else total + term
            put(b, lanes, jax.nn.silu(total))

    def put_write(b, lanes, value):
        write_vec[b * BLK : (b + 1) * BLK, lanes : lanes + 256] = value.astype(bf16)

    def put_read(b, lanes, value):
        read_vec[b * BLK : (b + 1) * BLK, lanes : lanes + 256] = value.astype(bf16)

    def put_signal(b, lanes, value):
        signal[b * BLK : (b + 1) * BLK, lanes : lanes + 256] = value

    def state_of(b):
        convolve(b, write_taps, wide, narrow, put_write)
        convolve(b, signal_taps, 0, wide, put_signal)
        spot = slice(b * BLK, (b + 1) * BLK)
        step = timestep[spot]
        scaled[spot, :] = (signal[spot, :] * expand(step)).astype(bf16)
        rest = jnp.exp(cums[b][BLK - 1 : BLK, :] - cums[b])
        tailed[spot, :] = (signal[spot, :] * expand(step * rest)).astype(bf16)
        for g in range(groups):
            states[b, :, g * span : (g + 1) * span] = lax.dot_general(
                write_vec[spot, g * STATE : (g + 1) * STATE],
                tailed[spot, g * span : (g + 1) * span],
                (((0,), (0,)), ((), ())),
                preferred_element_type=f32,
            )

    spread_direct = expand(jnp.broadcast_to(direct[...], (8, heads)))[0:1, :]
    low_lanes = lax.broadcasted_iota(jnp.int32, (BLK, 2 * head_dim), 1) < head_dim

    def within(b):
        convolve(b, read_taps, wide + narrow, narrow, put_read)
        spot = slice(b * BLK, (b + 1) * BLK)
        turned = cums[b].T
        for g in range(groups):
            inner = slice(g * STATE, (g + 1) * STATE)
            meeting = lax.dot_general(
                read_vec[spot, inner],
                write_vec[spot, inner],
                (((1,), (1,)), ((), ())),
                preferred_element_type=f32,
            )
            for pair in range(per_group // 2):
                head = g * per_group + 2 * pair
                lanes = slice(head * head_dim, (head + 2) * head_dim)
                weights = []
                for at in (head, head + 1):
                    gap = cums[b][:, at : at + 1] - turned[at : at + 1, :]
                    weights.append(
                        (meeting * jnp.exp(jnp.where(causal, gap, -jnp.inf))).astype(bf16)
                    )
                value = scaled[spot, lanes]
                zero = jnp.zeros_like(value)
                both = jnp.concatenate(
                    [jnp.where(low_lanes, value, zero), jnp.where(low_lanes, zero, value)], axis=0
                )
                summed[spot, lanes] = spread_direct[:, lanes] * signal[spot, lanes] + jnp.dot(
                    jnp.concatenate(weights, axis=1), both, preferred_element_type=f32
                )

    for b in range(1, blocks):
        state_of(b)
        within(b)

    @pl.when(chip > 0)
    def _():
        for copy in halo_copies(chip):
            copy.wait_recv()
        for _, halo, _, at, size in parts:
            extended[0:head_room, at : at + size] = halo[rim - head_room : rim, :].astype(f32)

    @pl.when(chip == 0)
    def _():
        extended[0:head_room, :] = jnp.zeros((head_room, extended.shape[1]), f32)

    state_of(0)
    for owner in range(owners):
        spot = slice(owner * rows, (owner + 1) * rows)
        value = states[0, spot, :]
        for b in range(1, blocks):
            value = value * readout[(b + 1) * BLK - 1 : (b + 1) * BLK, :] + states[b, spot, :]
        piece_out[owner] = value.astype(bf16)
    others(owners, lambda owner: piece_copy(owner, chip).start())

    @pl.when(chip < owners)
    def _():
        piece_in[chip] = piece_out[chip]

    within(0)

    @pl.when(chip < owners)
    def _():
        bytes_of(decay_in, chips - 1, decay_send.at[0], decay_recv.at[0]).wait_recv()

        def scan(device, held):
            @pl.when(device != chip)
            def _():
                piece_copy(chip, device).wait_recv()

            start_out[device] = held.astype(bf16)

            @pl.when(device != chip)
            def _():
                start_copy(chip, device).start()

            return held * decay_in[device] + piece_in[device].astype(f32)

        lax.fori_loop(0, chips, scan, jnp.zeros((rows, wide), f32))
        start_in[chip] = start_out[chip]

    with_others(
        lambda number: bytes_of(start_in, number, start_send.at[0], start_recv.at[0]).wait_recv()
    )
    gate_ready()
    start = jnp.concatenate([start_in[owner].astype(f32) for owner in range(owners)], axis=0)
    for b in range(blocks):
        spot = slice(b * BLK, (b + 1) * BLK)
        if b:
            start = (
                start * readout[b * BLK - 1 : b * BLK, :] + states[b - 1]
            )
        rounded = start.astype(bf16)
        for g in range(groups):
            lanes = slice(g * span, (g + 1) * span)
            near = jnp.dot(
                read_vec[spot, g * STATE : (g + 1) * STATE],
                rounded[:, lanes],
                preferred_element_type=f32,
            )
            value = summed[spot, lanes] + near * readout[spot, lanes]
            value = value * jax.nn.silu(gate_in[spot, lanes].astype(f32))
            scale = lax.rsqrt(jnp.mean(value * value, axis=-1, keepdims=True) + 1e-06)
            mixed[spot, lanes] = (value * scale * gain[:, lanes]).astype(bf16)

    @pl.when(chip < chips - 1)
    def _():
        for copy in halo_copies(chip + 1):
            copy.wait_send()

    with_others(
        lambda number: bytes_of(decay_in, number, decay_send.at[0], decay_recv.at[0]).wait_send()
    )
    with_others(
        lambda number: bytes_of(piece_out, number, piece_send.at[0], piece_recv.at[0]).wait_send()
    )

    @pl.when(chip < owners)
    def _():
        bytes_of(start_out, chips - 1, start_send.at[0], start_recv.at[0]).wait_send()


def mixer_scratch(chips, owners, length, wide, narrow, blocks):
    f32, bf16 = jnp.float32, jnp.bfloat16
    dma = pltpu.SemaphoreType.DMA
    rows = STATE // owners
    rim = 16
    return [
        pltpu.VMEM((rim, wide), bf16),
        pltpu.VMEM((rim, narrow), bf16),
        pltpu.VMEM((rim, narrow), bf16),
        pltpu.VMEM((length + 8, wide + 2 * narrow), f32),
        pltpu.VMEM((length, wide), f32),
        pltpu.VMEM((length, narrow), bf16),
        pltpu.VMEM((length, narrow), bf16),
        pltpu.VMEM((length, wide), bf16),
        pltpu.VMEM((length, wide), bf16),
        pltpu.VMEM((length, wide), f32),
        pltpu.VMEM((blocks, STATE, wide), f32),
        pltpu.VMEM((length, wide), f32),
        pltpu.VMEM((owners, rows, wide), bf16),
        pltpu.VMEM((chips, rows, wide), bf16),
        pltpu.VMEM((1, wide), f32),
        pltpu.VMEM((chips, 1, wide), f32),
        pltpu.VMEM((chips, rows, wide), bf16),
        pltpu.VMEM((owners, rows, wide), bf16),
        dma((3,)),
        dma((3,)),
        dma((1,)),
        dma((chips,)),
        dma((1,)),
        dma((1,)),
        dma((1,)),
        dma((1,)),
    ]


def layer_kernel(tail_sizes, mixer_sizes, mixer_scratch_count, *refs):
    mixer_in, tail_in, out = refs[:13], refs[13:24], refs[24]
    mixed, gate_held, stream_held, early_sem = refs[25:29]
    mixer_refs = refs[29 : 29 + mixer_scratch_count]
    tail_refs = refs[29 + mixer_scratch_count :]
    gate_load = pltpu.make_async_copy(mixer_in[3], gate_held, early_sem.at[0])
    stream_load = pltpu.make_async_copy(tail_in[0], stream_held, early_sem.at[1])
    gate_load.start()
    stream_load.start()
    held_in = (*mixer_in[:3], gate_held, *mixer_in[4:])

    def mix():
        mixer_stage(*mixer_sizes, gate_load.wait, *held_in, mixed, *mixer_refs)
        stream_load.wait()

    tail_stage(*tail_sizes, mix, mixed, stream_held, *tail_in[1:], out, *tail_refs)


def layer(mixer_in, tail_in):
    sp_count, tp_count = lax.axis_size("sp"), lax.axis_size("tp")
    bf16, f32 = jnp.bfloat16, jnp.float32
    dma = pltpu.SemaphoreType.DMA
    vmem, anywhere = pl.BlockSpec(memory_space=pltpu.VMEM), pl.BlockSpec(memory_space=pl.ANY)
    length, wide = mixer_in[0].shape
    narrow = mixer_in[1].shape[1]
    heads = mixer_in[4].shape[0]
    owners = min(sp_count, STATE // 8)
    mixer_sizes = (heads, narrow // STATE, owners, wide // heads)
    mixer_refs = mixer_scratch(sp_count, owners, length, wide, narrow, length // BLK)
    stream, _, index, _, out_weight, gate, up, down, common_gate, common_up, common_down = tail_in
    planes = PLANES if sp_count % PLANES == 0 else 1
    ring = sp_count // planes * tp_count
    count, width = stream.shape
    fanout = index.shape[0]
    experts = sp_count * tp_count
    capacity = max(2, (3 * count * fanout + 2 * experts - 1) // (2 * experts))
    capacity = (capacity + 7) // 8 * 8
    part = width // HALVES
    chunks = len(column_chunks(width))
    slots = (planes, HALVES, ring, capacity, part)
    pieces = (planes, HALVES, count, part)
    return pl.pallas_call(
        functools.partial(
            layer_kernel,
            (planes, ring, tp_count, capacity, fanout),
            mixer_sizes,
            len(mixer_refs),
        ),
        out_shape=pltpu.VMEM((count, width), bf16),
        in_specs=[vmem] * 3 + [anywhere] + [vmem] * 9 + [anywhere] + [vmem] * 3 + [anywhere] * 7,
        out_specs=vmem,
        scratch_shapes=[
            pltpu.VMEM((length, wide), bf16),
            pltpu.VMEM((length, wide), bf16),
            pltpu.VMEM((count, width), bf16),
            dma((2,)),
            *mixer_refs,
            pltpu.VMEM(out_weight.shape, bf16),
            pltpu.VMEM(gate.shape[1:], bf16),
            pltpu.VMEM(up.shape[1:], bf16),
            pltpu.VMEM(down.shape[1:], bf16),
            pltpu.VMEM(common_gate.shape, bf16),
            pltpu.VMEM(common_up.shape, bf16),
            pltpu.VMEM(common_down.shape, bf16),
            pltpu.VMEM((planes, fanout, count), jnp.int32),
            pltpu.VMEM((planes, fanout, count), f32),
            pltpu.VMEM((count, width), f32),
            pltpu.VMEM((count, common_gate.shape[1]), bf16),
            pltpu.VMEM((tp_count - 1, count, width), bf16),
            pltpu.VMEM((tp_count - 1, count, width), bf16),
            pltpu.VMEM((count, width), bf16),
            pltpu.VMEM(pieces, bf16),
            pltpu.VMEM(slots, bf16),
            pltpu.VMEM(slots, bf16),
            pltpu.VMEM((ring * capacity, width), bf16),
            pltpu.VMEM((ring * capacity, gate.shape[2]), bf16),
            pltpu.VMEM(slots, bf16),
            pltpu.VMEM(slots, bf16),
            pltpu.VMEM(pieces[1:], f32),
            pltpu.VMEM(pieces, bf16),
            pltpu.VMEM(pieces, bf16),
            pltpu.VMEM(pieces[1:], bf16),
            dma((7,)),
            dma((tp_count - 1,)),
            dma((tp_count - 1, chunks)),
            dma((2,)),
            dma((2,)),
            *[dma((planes, HALVES))] * 3,
            dma((1,)),
            dma((planes, HALVES)),
            dma((1,)),
            dma((planes, HALVES)),
            dma((1,)),
            dma((1,)),
            dma((HALVES,)),
        ],
        compiler_params=pltpu.CompilerParams(
            collective_id=0, has_side_effects=True, vmem_limit_bytes=62 * 2**20
        ),
    )(*mixer_in, *tail_in)


def on_device(
    stream,
    head_input_signal,
    write_input_vectors,
    read_input_vectors,
    output_gate_input,
    step_size_input,
    position_log_decay,
    signal_filter_taps,
    write_filter_taps,
    read_filter_taps,
    step_size_bias,
    head_decay_rate,
    head_direct_term,
    grouped_norm_gain,
    mixer_output_weight,
    expert_norm_gain,
    chosen_expert_index,
    chosen_expert_weight,
    routed_gate_weight,
    routed_up_weight,
    routed_down_weight,
    common_gate_weight,
    common_up_weight,
    common_down_weight,
):
    row = lambda part: part.reshape(1, -1)
    return layer(
        (
            head_input_signal,
            write_input_vectors,
            read_input_vectors,
            output_gate_input,
            step_size_input.T,
            position_log_decay.T,
            signal_filter_taps,
            write_filter_taps,
            read_filter_taps,
            row(step_size_bias),
            row(head_decay_rate),
            row(head_direct_term),
            row(grouped_norm_gain),
        ),
        (
            stream,
            row(expert_norm_gain),
            chosen_expert_index.T,
            chosen_expert_weight.T,
            mixer_output_weight,
            routed_gate_weight,
            routed_up_weight,
            routed_down_weight,
            common_gate_weight,
            common_up_weight,
            common_down_weight,
        ),
    )


def solution(mesh):
    in_specs = (
        P(("sp", "tp"), None),
        P("sp", "tp"),
        P("sp", "tp"),
        P("sp", "tp"),
        P("sp", "tp"),
        P("sp", "tp"),
        P("sp", "tp"),
        P(None, "tp"),
        P(None, "tp"),
        P(None, "tp"),
        P("tp"),
        P("tp"),
        P("tp"),
        P("tp"),
        P("tp", None),
        P(),
        P(("sp", "tp"), None),
        P(("sp", "tp"), None),
        P(("sp", "tp"), None, None),
        P(("sp", "tp"), None, None),
        P(("sp", "tp"), None, None),
        P(),
        P(),
        P(),
    )
    out_specs = P(("sp", "tp"), None)
    return jax.shard_map(
        on_device, mesh=mesh, in_specs=in_specs, out_specs=out_specs, check_vma=False
    )
```

```python
import functools

import jax
import jax.numpy as jnp
from jax import lax
from jax.experimental import pallas as pl
from jax.experimental.pallas import tpu as pltpu
from jax.sharding import PartitionSpec as P

STATE = 128
BLK = 128


MESH = pl.DeviceIdType.MESH
PLANES = 4
HALVES = 2
COLS = 512


LINE_END = [
    (0, 0, 0), (0, 0, 1), (0, 1, 0), (0, 1, 1), (0, 2, 0), (0, 2, 1),
    (0, 3, 0), (1, 2, 0), (2, 2, 0), (0, 3, 1), (2, 2, 1), (3, 0, 0),
    (1, 3, 0), (2, 3, 0), (1, 1, 0), (1, 0, 0), (2, 3, 1), (2, 1, 0),
    (2, 1, 1), (2, 0, 0), (2, 0, 1),
]
LINE_NEXT = [
    (0, 1, 0), (0, 1, 1), (3, 1, 0), (0, 0, 0), (0, 2, 0), (0, 2, 1),
    (0, 3, 0), (0, 0, 1), (1, 2, 0), (1, 0, 0), (0, 3, 1), (1, 1, 0),
    (2, 0, 0), (2, 2, 0), (1, 3, 0), (2, 1, 0), (2, 2, 1), (2, 0, 1),
    (2, 3, 0), (2, 3, 1), (2, 1, 1),
]


def line_plans(planes, halves):
    if (planes, halves) == (4, 2):
        mirror = lambda plan: [(kind, 3 - owner, half) for kind, owner, half in plan]
        plans = [LINE_END, LINE_NEXT, mirror(LINE_NEXT), mirror(LINE_END)]
    else:
        plans = []
        for z in range(planes):
            near = sorted(range(planes), key=lambda s: (abs(s - z), s))
            plan = [(0, s, h) for s in near for h in range(halves)] + [(3, 0, 0)]
            for s in near:
                plan += [(1, s, 0)] + [(2, s, h) for h in range(halves)]
            plans.append(plan)
    return [[(k * planes + s) * halves + h for k, s, h in plan] for plan in plans]


def column_chunks(width):
    step = min(COLS, width)
    return [(at, step) for at in range(0, width, step)]


def pick(values, place, which):
    chosen = jnp.int32(0)
    for spot, row in enumerate(values):
        chosen = chosen + (place == spot).astype(jnp.int32) * pick_one(row, which)
    return chosen


def pick_one(row, which):
    chosen = jnp.int32(0)
    for spot, value in enumerate(row):
        chosen = chosen + (which == spot).astype(jnp.int32) * value
    return chosen


def bytes_of(ref, number, send_sem, recv_sem):
    view = ref.at[pl.ds(0, number)]
    return pltpu.make_async_remote_copy(
        src_ref=view,
        dst_ref=view,
        send_sem=send_sem,
        recv_sem=recv_sem,
        device_id=(lax.axis_index("sp"), lax.axis_index("tp")),
        device_id_type=MESH,
    )


def tail_stage(
    planes,
    ring,
    tp_count,
    capacity,
    fanout,
    steps,
    mixed_ref,
    stream_ref,
    gain_ref,
    index_ref,
    weight_ref,
    out_weight_hbm,
    gate_hbm,
    up_hbm,
    down_hbm,
    common_gate_hbm,
    common_up_hbm,
    common_down_hbm,
    out_ref,
    out_weight,
    gate,
    up,
    down,
    common_gate,
    common_up,
    common_down,
    index_tables,
    weight_tables,
    total,
    residual,
    part_out,
    part_in,
    normed,
    rows,
    sent,
    arrived,
    flat,
    hidden,
    answer,
    returned,
    sums_own,
    sums_out,
    sums_in,
    relay_in,
    weight_sem,
    part_send,
    part_recv,
    table_send,
    table_recv,
    rows_up,
    rows_down,
    rows_recv,
    go_send,
    go_recv,
    back_send,
    back_recv,
    sums_send,
    sums_recv,
    relay_recv,
):
    chip = lax.axis_index("sp")
    core = lax.axis_index("tp")
    chips = ring // tp_count
    plane = chip // chips
    mine = (chip % chips) * tp_count + core
    count, width = stream_ref.shape
    halves = rows.shape[1]
    part = width // halves
    plans = line_plans(planes, halves)

    def in_plane(spot):
        return (plane * chips + spot // tp_count, spot % tp_count)

    def in_line(spot):
        return (spot * chips + chip % chips, core)

    loads = [
        pltpu.make_async_copy(source, target, weight_sem.at[number])
        for number, (source, target) in enumerate(
            [
                (out_weight_hbm, out_weight),
                (common_gate_hbm, common_gate),
                (common_up_hbm, common_up),
                (common_down_hbm, common_down),
                (gate_hbm.at[0], gate),
                (up_hbm.at[0], up),
                (down_hbm.at[0], down),
            ]
        )
    ]
    barrier = pltpu.get_barrier_semaphore()
    all_chips = lax.axis_size("sp")
    for ahead in range(1, all_chips):
        pl.semaphore_signal(
            barrier, inc=1, device_id=((chip + ahead) % all_chips, core), device_id_type=MESH
        )
    for spot in range(chips):
        for ahead in range(1, tp_count):
            pl.semaphore_signal(
                barrier,
                inc=1,
                device_id=(plane * chips + spot, (core + ahead) % tp_count),
                device_id_type=MESH,
            )
    load_inputs, inputs_ready, mix = steps
    load_inputs()
    for load in loads:
        load.start()
    pl.semaphore_wait(barrier, all_chips - 1 + chips * (tp_count - 1))
    inputs_ready()

    def table_copies(ahead, owner):
        return [
            pltpu.make_async_remote_copy(
                src_ref=source,
                dst_ref=held.at[owner],
                send_sem=table_send.at[number],
                recv_sem=table_recv.at[number],
                device_id=in_line((plane + ahead) % planes),
                device_id_type=MESH,
            )
            for number, (source, held) in enumerate(
                [(index_ref, index_tables), (weight_ref, weight_tables)]
            )
        ]

    for ahead in range(1, planes):
        for copy in table_copies(ahead, plane):
            copy.start()
    index_tables[plane] = index_ref[...]
    weight_tables[plane] = weight_ref[...]
    relayed = planes == 4
    if relayed:

        @pl.when(plane == 0)
        def _():
            sums_in[planes - 1] = jnp.zeros(sums_in.shape[1:], jnp.bfloat16)

        @pl.when(plane == planes - 1)
        def _():
            sums_in[0] = jnp.zeros(sums_in.shape[1:], jnp.bfloat16)

    mix()
    table_totals = [
        bytes_of(held, planes - 1, table_send.at[number], table_recv.at[number])
        for number, held in enumerate([index_tables, weight_tables])
    ]
    if planes > 1:
        for total_copy in table_totals:
            total_copy.wait_recv()

    def part_copies(ahead):
        return [
            pltpu.make_async_remote_copy(
                src_ref=part_out.at[ahead - 1, :, pl.ds(at, step)],
                dst_ref=part_in.at[ahead - 1, :, pl.ds(at, step)],
                send_sem=part_send.at[ahead - 1],
                recv_sem=part_recv.at[ahead - 1, number],
                device_id=(chip, (core + ahead) % tp_count),
                device_id_type=MESH,
            )
            for number, (at, step) in enumerate(column_chunks(width))
        ]

    loads[0].wait()
    for ahead in range(1, tp_count):
        owner = (core + ahead) % tp_count
        held = mixed_ref[pl.ds(pl.multiple_of(owner * count, count), count), :]
        copies = part_copies(ahead)
        for number, (at, step) in enumerate(column_chunks(width)):
            part_out[ahead - 1, :, at : at + step] = jnp.dot(
                held, out_weight[:, at : at + step], preferred_element_type=jnp.float32
            ).astype(jnp.bfloat16)
            copies[number].start()
    held = mixed_ref[pl.ds(pl.multiple_of(core * count, count), count), :]
    for at, step in column_chunks(width):
        total[:, at : at + step] = stream_ref[:, at : at + step].astype(jnp.float32) + jnp.dot(
            held, out_weight[:, at : at + step], preferred_element_type=jnp.float32
        )
    for ahead in range(1, tp_count):
        for copy in part_copies(ahead):
            copy.wait_recv()
    band = 16

    def norm_band(number, carry):
        spot = pl.ds(pl.multiple_of(number * band, band), band)
        summed = total[spot, :]
        for ahead in range(1, tp_count):
            summed = summed + part_in[ahead - 1, spot, :].astype(jnp.float32)
        rounded = summed.astype(jnp.bfloat16)
        wide = rounded.astype(jnp.float32)
        total[spot, :] = wide
        scale = lax.rsqrt(jnp.mean(wide * wide, axis=-1, keepdims=True) + 1e-06)
        value = (wide * scale * gain_ref[...]).astype(jnp.bfloat16)
        normed[spot, :] = value
        for half in range(halves):
            rows[plane, half, spot, :] = value[:, half * part : (half + 1) * part]
        return carry

    lax.fori_loop(0, count // band, norm_band, 0, unroll=2)

    def rows_copy(owner, half, target, sem):
        return pltpu.make_async_remote_copy(
            src_ref=rows.at[owner, half],
            dst_ref=rows.at[owner, half],
            send_sem=sem.at[owner, half],
            recv_sem=rows_recv.at[owner, half],
            device_id=in_line(target),
            device_id_type=MESH,
        )

    def block_copy(source, target, send, recv, owner, half, ahead):
        spot = (mine + ahead) % ring
        return pltpu.make_async_remote_copy(
            src_ref=source.at[owner, half, spot],
            dst_ref=target.at[owner, half, mine],
            send_sem=send.at[0],
            recv_sem=recv.at[owner, half],
            device_id=in_plane(spot),
            device_id_type=MESH,
        )

    def block_wait(source, target, send, recv, owner, half):
        return pltpu.make_async_remote_copy(
            src_ref=source.at[owner, half, pl.ds(0, ring - 1)],
            dst_ref=target.at[owner, half, pl.ds(0, ring - 1)],
            send_sem=send.at[0],
            recv_sem=recv.at[owner, half],
            device_id=in_plane((mine + 1) % ring),
            device_id_type=MESH,
        )

    go = (sent, arrived, go_send, go_recv)
    back = (answer, returned, back_send, back_recv)

    def sums_copy(owner, half):
        return pltpu.make_async_remote_copy(
            src_ref=sums_out.at[owner, half],
            dst_ref=sums_in.at[plane, half],
            send_sem=sums_send.at[0],
            recv_sem=sums_recv.at[0],
            device_id=in_line(owner),
            device_id_type=MESH,
        )

    def relay_copy(owner, half):
        return pltpu.make_async_remote_copy(
            src_ref=sums_out.at[owner, half],
            dst_ref=relay_in.at[half],
            send_sem=sums_send.at[0],
            recv_sem=relay_recv.at[half],
            device_id=in_line(plane + 1 - 2 * (plane // (planes - 1))),
            device_id_type=MESH,
        )

    def slots_of(owner):
        table, parts = index_tables[owner], weight_tables[owner]
        names = lax.broadcasted_iota(jnp.int32, (ring, count), 0) + plane * ring
        hits = jnp.zeros((ring, count), jnp.float32)
        share = jnp.zeros((ring, count), jnp.float32)
        for turn in range(fanout):
            named = table[turn : turn + 1, :] == names
            hits = hits + jnp.where(named, 1.0, 0.0)
            share = share + jnp.where(named, parts[turn : turn + 1, :], 0.0)
        before = lax.broadcasted_iota(jnp.int32, (count, count), 0)
        after = lax.broadcasted_iota(jnp.int32, (count, count), 1)
        earlier = jnp.where(before < after, 1.0, 0.0).astype(jnp.bfloat16)
        slot = jnp.dot(hits.astype(jnp.bfloat16), earlier, preferred_element_type=jnp.float32)
        return jnp.where(hits > 0.5, slot, -1.0), share

    places = lax.broadcasted_iota(jnp.int32, (capacity, count), 0).astype(jnp.float32)

    def dispatch(owner, half):
        @pl.when(owner != plane)
        def _():
            rows_copy(owner, half, owner, rows_up).wait_recv()

        @pl.when((owner <= plane) & (plane < planes - 1))
        def _():
            rows_copy(owner, half, plane + 1, rows_up).start()

        @pl.when((owner >= plane) & (plane > 0))
        def _():
            rows_copy(owner, half, plane - 1, rows_down).start()

        slot, _ = slots_of(owner)
        chosen = jnp.concatenate(
            [
                jnp.where(slot[spot : spot + 1, :] == places, 1.0, 0.0)
                for spot in range(ring)
            ],
            axis=0,
        ).astype(jnp.bfloat16)
        for at, step in column_chunks(part):
            picked = jnp.dot(
                chosen, rows[owner, half, :, at : at + step], preferred_element_type=jnp.float32
            )
            for spot in range(ring):
                sent[owner, half, spot, :, at : at + step] = picked[
                    spot * capacity : (spot + 1) * capacity
                ].astype(jnp.bfloat16)
        for ahead in range(1, ring):
            block_copy(*go, owner, half, ahead).start()
        arrived[owner, half, mine] = sent[owner, half, mine]

    def ffn(x_ref, gate_ref, up_ref, down_ref, hidden_ref, put):
        for at, step in column_chunks(gate_ref.shape[1]):
            half = step // 2
            for lane in (at, at + half):
                g = jnp.dot(
                    x_ref[...], gate_ref[:, lane : lane + half], preferred_element_type=jnp.float32
                )
                u = jnp.dot(
                    x_ref[...], up_ref[:, lane : lane + half], preferred_element_type=jnp.float32
                )
                hidden_ref[:, lane : lane + half] = (jax.nn.silu(g) * u).astype(jnp.bfloat16)
        for at, step in column_chunks(width):
            put(
                at,
                step,
                jnp.dot(
                    hidden_ref[...],
                    down_ref[:, at : at + step],
                    preferred_element_type=jnp.float32,
                ),
            )

    def serve(owner):
        for half in range(halves):
            block_wait(*go, owner, half).wait_recv()
            for at, step in column_chunks(part):
                flat[:, half * part + at : half * part + at + step] = jnp.concatenate(
                    [
                        arrived[owner, half, spot, :, at : at + step].astype(jnp.float32)
                        for spot in range(ring)
                    ],
                    axis=0,
                ).astype(jnp.bfloat16)

        def put(at, step, value):
            half, lane = at // part, at % part
            for spot in range(ring):
                answer[owner, half, spot, :, lane : lane + step] = value[
                    spot * capacity : (spot + 1) * capacity
                ].astype(jnp.bfloat16)
            if lane + step == part:
                for ahead in range(1, ring):
                    block_copy(*back, owner, half, ahead).start()

        ffn(flat, gate, up, down, hidden, put)
        for half in range(halves):
            returned[owner, half, mine] = answer[owner, half, mine]

    def collect(owner, half):
        block_wait(*back, owner, half).wait_recv()
        ends = helps = jnp.bool_(False)
        if relayed:
            last = planes - 1
            ends = ((plane == 0) & (owner == last)) | ((plane == last) & (owner == 0))
            helps = ((plane == 1) & (owner == last)) | ((plane == last - 1) & (owner == 0))

            @pl.when(helps)
            def _():
                relay_copy(owner, half).wait_recv()

        slot, share = slots_of(owner)
        spread = jnp.concatenate(
            [
                jnp.where(slot[spot : spot + 1, :] == places, share[spot : spot + 1, :], 0.0)
                for spot in range(ring)
            ],
            axis=0,
        )
        coarse = spread.astype(jnp.bfloat16)
        fine = (spread - coarse.astype(jnp.float32)).astype(jnp.bfloat16)
        contract = (((0,), (0,)), ((), ()))
        for at, step in column_chunks(part):
            blocks = jnp.concatenate(
                [
                    returned[owner, half, spot, :, at : at + step].astype(jnp.float32)
                    for spot in range(ring)
                ],
                axis=0,
            ).astype(jnp.bfloat16)
            value = lax.dot_general(coarse, blocks, contract, preferred_element_type=jnp.float32)
            value = value + lax.dot_general(
                fine, blocks, contract, preferred_element_type=jnp.float32
            )

            @pl.when(owner == plane)
            def _():
                sums_own[half, :, at : at + step] = value

            @pl.when((owner != plane) & ~helps)
            def _():
                sums_out[owner, half, :, at : at + step] = value.astype(jnp.bfloat16)

            if relayed:

                @pl.when(helps)
                def _():
                    sums_out[owner, half, :, at : at + step] = (
                        value + relay_in[half, :, at : at + step].astype(jnp.float32)
                    ).astype(jnp.bfloat16)

        @pl.when((owner != plane) & ~ends)
        def _():
            sums_copy(owner, half).start()

        if relayed:

            @pl.when(ends)
            def _():
                relay_copy(owner, half).start()

    def share_expert():
        for load in loads[1:4]:
            load.wait()

        def put(at, step, value):
            total[:, at : at + step] += value

        ffn(normed, common_gate, common_up, common_down, residual, put)

    def step(turn, carry):
        code = pick(plans, plane, turn)
        half, owner, kind = code % halves, code // halves % planes, code // (halves * planes)

        @pl.when(kind == 0)
        def _():
            dispatch(owner, half)

        @pl.when(kind == 1)
        def _():
            serve(owner)

        @pl.when(kind == 2)
        def _():
            collect(owner, half)

        @pl.when(kind == 3)
        def _():
            share_expert()

        return carry

    for load in loads[4:]:
        load.wait()
    lax.fori_loop(0, len(plans[0]), step, 0)

    for ahead in range(1, tp_count):
        pltpu.make_async_remote_copy(
            src_ref=part_out.at[ahead - 1],
            dst_ref=part_in.at[ahead - 1],
            send_sem=part_send.at[ahead - 1],
            recv_sem=part_recv.at[ahead - 1, 0],
            device_id=(chip, (core + ahead) % tp_count),
            device_id_type=MESH,
        ).wait_send()
    for source, target, send, recv in (go, back):
        pltpu.make_async_remote_copy(
            src_ref=source.at[:, :, pl.ds(0, ring - 1)],
            dst_ref=target.at[:, :, pl.ds(0, ring - 1)],
            send_sem=send.at[0],
            recv_sem=recv.at[0, 0],
            device_id=in_plane((mine + 1) % ring),
            device_id_type=MESH,
        ).wait_send()

    def drain(code, carry):
        owner, half = code // halves, code % halves

        @pl.when((owner <= plane) & (plane < planes - 1))
        def _():
            rows_copy(owner, half, plane + 1, rows_up).wait_send()

        @pl.when((owner >= plane) & (plane > 0))
        def _():
            rows_copy(owner, half, plane - 1, rows_down).wait_send()

        return carry

    lax.fori_loop(0, planes * halves, drain, 0)
    if planes > 1:
        for total_copy in table_totals:
            total_copy.wait_send()
        bytes_of(sums_out, planes - 1, sums_send.at[0], sums_recv.at[0]).wait_send()
        if relayed:
            at_end = (plane == 0) | (plane == planes - 1)

            @pl.when(at_end)
            def _():
                bytes_of(sums_in, planes - 2, sums_send.at[0], sums_recv.at[0]).wait_recv()

            @pl.when(~at_end)
            def _():
                bytes_of(sums_in, planes - 1, sums_send.at[0], sums_recv.at[0]).wait_recv()

        else:
            bytes_of(sums_in, planes - 1, sums_send.at[0], sums_recv.at[0]).wait_recv()

    def last_band(number, carry):
        spot = pl.ds(pl.multiple_of(number * band, band), band)
        for half in range(halves):
            lanes = slice(half * part, (half + 1) * part)
            value = total[spot, lanes] + sums_own[half, spot, :]
            for ahead in range(1, planes):
                value = value + sums_in[(plane + ahead) % planes, half, spot, :].astype(
                    jnp.float32
                )
            out_ref[spot, lanes] = value.astype(jnp.bfloat16)
        return carry

    lax.fori_loop(0, count // band, last_band, 0)


def mixer_stage(
    heads,
    groups,
    owners,
    head_dim,
    gate_ready,
    signal_in,
    write_in,
    read_in,
    gate_in,
    step_in,
    log_in,
    signal_taps,
    write_taps,
    read_taps,
    bias,
    rate,
    direct,
    gain,
    mixed,
    halo_signal,
    halo_write,
    halo_read,
    extended,
    signal,
    write_vec,
    read_vec,
    scaled,
    tailed,
    readout,
    states,
    summed,
    piece_out,
    piece_in,
    decay_out,
    decay_in,
    start_out,
    start_in,
    halo_send,
    halo_recv,
    piece_send,
    piece_recv,
    decay_send,
    decay_recv,
    start_send,
    start_recv,
):
    chip, core = lax.axis_index("sp"), lax.axis_index("tp")
    chips = lax.axis_size("sp")
    length, wide = signal_in.shape
    narrow = write_in.shape[1]
    rim = halo_signal.shape[0]
    taps = signal_taps.shape[0]
    blocks = length // BLK
    per_group = heads // groups
    span = per_group * head_dim
    rows = STATE // owners
    f32, bf16 = jnp.float32, jnp.bfloat16
    exact = lax.Precision.HIGHEST

    def halo_copies(target):
        return [
            pltpu.make_async_remote_copy(
                src_ref=source.at[pl.ds(length - rim, rim), :],
                dst_ref=halo,
                send_sem=halo_send.at[number],
                recv_sem=halo_recv.at[number],
                device_id=(target, core),
                device_id_type=MESH,
            )
            for number, (source, halo) in enumerate(
                [(signal_in, halo_signal), (write_in, halo_write), (read_in, halo_read)]
            )
        ]

    @pl.when(chip < chips - 1)
    def _():
        for copy in halo_copies(chip + 1):
            copy.start()

    timestep = step_in[...].astype(f32).T + bias[...]
    timestep = jnp.maximum(timestep, 0.0) + jnp.log1p(jnp.exp(-jnp.abs(timestep)))
    log_decay = log_in[...].T - rate[...] * timestep
    first = lax.broadcasted_iota(jnp.int32, (BLK, BLK), 0)
    second = lax.broadcasted_iota(jnp.int32, (BLK, BLK), 1)
    causal = first >= second
    lower = jnp.where(causal, 1.0, 0.0)
    cums = [
        jnp.dot(
            lower,
            log_decay[b * BLK : (b + 1) * BLK],
            precision=exact,
            preferred_element_type=f32,
        )
        for b in range(blocks)
    ]
    part = lax.broadcasted_iota(jnp.int32, (heads, wide), 0)
    lane = lax.broadcasted_iota(jnp.int32, (heads, wide), 1) // head_dim
    widen = jnp.where(part == lane, 1.0, 0.0).astype(bf16)

    def expand(value):
        high = value.astype(bf16)
        rest = value - high.astype(f32)
        middle = rest.astype(bf16)
        low = (rest - middle.astype(f32)).astype(bf16)
        return (
            jnp.dot(high, widen, preferred_element_type=f32)
            + jnp.dot(middle, widen, preferred_element_type=f32)
            + jnp.dot(low, widen, preferred_element_type=f32)
        )

    for b in range(blocks):
        readout[b * BLK : (b + 1) * BLK, :] = expand(jnp.exp(cums[b]))
    decay = readout[BLK - 1 : BLK, :]
    for b in range(1, blocks):
        decay = decay * readout[(b + 1) * BLK - 1 : (b + 1) * BLK, :]
    decay_out[...] = decay

    def decay_copy(owner, device):
        return pltpu.make_async_remote_copy(
            src_ref=decay_out,
            dst_ref=decay_in.at[device],
            send_sem=decay_send.at[0],
            recv_sem=decay_recv.at[0],
            device_id=(owner, core),
            device_id_type=MESH,
        )

    def piece_copy(owner, device):
        return pltpu.make_async_remote_copy(
            src_ref=piece_out.at[owner],
            dst_ref=piece_in.at[device],
            send_sem=piece_send.at[0],
            recv_sem=piece_recv.at[device],
            device_id=(owner, core),
            device_id_type=MESH,
        )

    def start_copy(owner, device):
        return pltpu.make_async_remote_copy(
            src_ref=start_out.at[device],
            dst_ref=start_in.at[owner],
            send_sem=start_send.at[0],
            recv_sem=start_recv.at[0],
            device_id=(device, core),
            device_id_type=MESH,
        )

    def others(number, act):
        for at in range(number):

            @pl.when(at != chip)
            def _():
                act(at)

    def with_others(act):
        if owners == chips:
            act(owners - 1)
        else:

            @pl.when(chip < owners)
            def _():
                act(owners - 1)

            @pl.when(chip >= owners)
            def _():
                act(owners)

    others(owners, lambda owner: decay_copy(owner, chip).start())

    @pl.when(chip < owners)
    def _():
        decay_in[chip] = decay_out[...]

    parts = [
        (signal_in, halo_signal, signal_taps, 0, wide),
        (write_in, halo_write, write_taps, wide, narrow),
        (read_in, halo_read, read_taps, wide + narrow, narrow),
    ]
    head_room = 8
    for source, _, _, at, size in parts:
        extended[head_room : head_room + length, at : at + size] = source[...].astype(f32)

    def convolve(b, weights, at, size, put):
        for lanes in range(0, size, 256):
            total = None
            for tap in range(taps):
                begin = head_room - taps + 1 + tap + b * BLK
                term = (
                    weights[tap : tap + 1, lanes : lanes + 256].astype(f32)
                    * extended[begin : begin + BLK, at + lanes : at + lanes + 256]
                )
                total = term if total is None else total + term
            put(b, lanes, jax.nn.silu(total))

    def put_write(b, lanes, value):
        write_vec[b * BLK : (b + 1) * BLK, lanes : lanes + 256] = value.astype(bf16)

    def put_read(b, lanes, value):
        read_vec[b * BLK : (b + 1) * BLK, lanes : lanes + 256] = value.astype(bf16)

    def put_signal(b, lanes, value):
        signal[b * BLK : (b + 1) * BLK, lanes : lanes + 256] = value

    def state_of(b):
        convolve(b, write_taps, wide, narrow, put_write)
        convolve(b, signal_taps, 0, wide, put_signal)
        spot = slice(b * BLK, (b + 1) * BLK)
        step = timestep[spot]
        scaled[spot, :] = (signal[spot, :] * expand(step)).astype(bf16)
        rest = jnp.exp(cums[b][BLK - 1 : BLK, :] - cums[b])
        tailed[spot, :] = (signal[spot, :] * expand(step * rest)).astype(bf16)
        for g in range(groups):
            states[b, :, g * span : (g + 1) * span] = lax.dot_general(
                write_vec[spot, g * STATE : (g + 1) * STATE],
                tailed[spot, g * span : (g + 1) * span],
                (((0,), (0,)), ((), ())),
                preferred_element_type=f32,
            )

    spread_direct = expand(jnp.broadcast_to(direct[...], (8, heads)))[0:1, :]
    low_lanes = lax.broadcasted_iota(jnp.int32, (BLK, 2 * head_dim), 1) < head_dim

    def within(b):
        convolve(b, read_taps, wide + narrow, narrow, put_read)
        spot = slice(b * BLK, (b + 1) * BLK)
        turned = cums[b].T
        for g in range(groups):
            inner = slice(g * STATE, (g + 1) * STATE)
            meeting = lax.dot_general(
                read_vec[spot, inner],
                write_vec[spot, inner],
                (((1,), (1,)), ((), ())),
                preferred_element_type=f32,
            )
            for pair in range(per_group // 2):
                head = g * per_group + 2 * pair
                lanes = slice(head * head_dim, (head + 2) * head_dim)
                weights = []
                for at in (head, head + 1):
                    gap = cums[b][:, at : at + 1] - turned[at : at + 1, :]
                    weights.append(
                        (meeting * jnp.exp(jnp.where(causal, gap, -jnp.inf))).astype(bf16)
                    )
                value = scaled[spot, lanes]
                zero = jnp.zeros_like(value)
                both = jnp.concatenate(
                    [jnp.where(low_lanes, value, zero), jnp.where(low_lanes, zero, value)], axis=0
                )
                summed[spot, lanes] = spread_direct[:, lanes] * signal[spot, lanes] + jnp.dot(
                    jnp.concatenate(weights, axis=1), both, preferred_element_type=f32
                )

    for b in range(1, blocks):
        state_of(b)
        within(b)

    @pl.when(chip > 0)
    def _():
        for copy in halo_copies(chip):
            copy.wait_recv()
        for _, halo, _, at, size in parts:
            extended[0:head_room, at : at + size] = halo[rim - head_room : rim, :].astype(f32)

    @pl.when(chip == 0)
    def _():
        extended[0:head_room, :] = jnp.zeros((head_room, extended.shape[1]), f32)

    state_of(0)
    for owner in range(owners):
        spot = slice(owner * rows, (owner + 1) * rows)
        value = states[0, spot, :]
        for b in range(1, blocks):
            value = value * readout[(b + 1) * BLK - 1 : (b + 1) * BLK, :] + states[b, spot, :]
        piece_out[owner] = value.astype(bf16)
    others(owners, lambda owner: piece_copy(owner, chip).start())

    @pl.when(chip < owners)
    def _():
        piece_in[chip] = piece_out[chip]

    within(0)

    @pl.when(chip < owners)
    def _():
        bytes_of(decay_in, chips - 1, decay_send.at[0], decay_recv.at[0]).wait_recv()

        def scan(device, held):
            @pl.when(device != chip)
            def _():
                piece_copy(chip, device).wait_recv()

            start_out[device] = held.astype(bf16)

            @pl.when(device != chip)
            def _():
                start_copy(chip, device).start()

            return held * decay_in[device] + piece_in[device].astype(f32)

        lax.fori_loop(0, chips, scan, jnp.zeros((rows, wide), f32))
        start_in[chip] = start_out[chip]

    with_others(
        lambda number: bytes_of(start_in, number, start_send.at[0], start_recv.at[0]).wait_recv()
    )
    gate_ready()
    start = jnp.concatenate([start_in[owner].astype(f32) for owner in range(owners)], axis=0)
    for b in range(blocks):
        spot = slice(b * BLK, (b + 1) * BLK)
        if b:
            start = (
                start * readout[b * BLK - 1 : b * BLK, :] + states[b - 1]
            )
        rounded = start.astype(bf16)
        for g in range(groups):
            lanes = slice(g * span, (g + 1) * span)
            near = jnp.dot(
                read_vec[spot, g * STATE : (g + 1) * STATE],
                rounded[:, lanes],
                preferred_element_type=f32,
            )
            value = summed[spot, lanes] + near * readout[spot, lanes]
            value = value * jax.nn.silu(gate_in[spot, lanes].astype(f32))
            scale = lax.rsqrt(jnp.mean(value * value, axis=-1, keepdims=True) + 1e-06)
            mixed[spot, lanes] = (value * scale * gain[:, lanes]).astype(bf16)

    @pl.when(chip < chips - 1)
    def _():
        for copy in halo_copies(chip + 1):
            copy.wait_send()

    with_others(
        lambda number: bytes_of(decay_in, number, decay_send.at[0], decay_recv.at[0]).wait_send()
    )
    with_others(
        lambda number: bytes_of(piece_out, number, piece_send.at[0], piece_recv.at[0]).wait_send()
    )

    @pl.when(chip < owners)
    def _():
        bytes_of(start_out, chips - 1, start_send.at[0], start_recv.at[0]).wait_send()


def mixer_scratch(chips, owners, length, wide, narrow, blocks):
    f32, bf16 = jnp.float32, jnp.bfloat16
    dma = pltpu.SemaphoreType.DMA
    rows = STATE // owners
    rim = 16
    return [
        pltpu.VMEM((rim, wide), bf16),
        pltpu.VMEM((rim, narrow), bf16),
        pltpu.VMEM((rim, narrow), bf16),
        pltpu.VMEM((length + 8, wide + 2 * narrow), f32),
        pltpu.VMEM((length, wide), f32),
        pltpu.VMEM((length, narrow), bf16),
        pltpu.VMEM((length, narrow), bf16),
        pltpu.VMEM((length, wide), bf16),
        pltpu.VMEM((length, wide), bf16),
        pltpu.VMEM((length, wide), f32),
        pltpu.VMEM((blocks, STATE, wide), f32),
        pltpu.VMEM((length, wide), f32),
        pltpu.VMEM((owners, rows, wide), bf16),
        pltpu.VMEM((chips, rows, wide), bf16),
        pltpu.VMEM((1, wide), f32),
        pltpu.VMEM((chips, 1, wide), f32),
        pltpu.VMEM((chips, rows, wide), bf16),
        pltpu.VMEM((owners, rows, wide), bf16),
        dma((3,)),
        dma((3,)),
        dma((1,)),
        dma((chips,)),
        dma((1,)),
        dma((1,)),
        dma((1,)),
        dma((1,)),
    ]


def layer_kernel(tail_sizes, mixer_sizes, mixer_scratch_count, *refs):
    mixer_in, tail_in, out = refs[:13], refs[13:24], refs[24]
    mixed, early_sem = refs[25:27]
    held, refs = refs[27:44], refs[44:]
    mixer_refs, tail_refs = refs[:mixer_scratch_count], refs[mixer_scratch_count:]
    early = [
        pltpu.make_async_copy(source, target, early_sem.at[number])
        for number, (source, target) in enumerate(zip((*mixer_in, *tail_in[:4]), held))
    ]
    late = (3, 13, 14)

    def load_inputs():
        for number in sorted(range(17), key=lambda number: number in late):
            early[number].start()

    def inputs_ready():
        for number in range(17):
            if number not in late:
                early[number].wait()

    def mix():
        mixer_stage(*mixer_sizes, early[3].wait, *held[:13], mixed, *mixer_refs)
        early[13].wait()
        early[14].wait()

    steps = (load_inputs, inputs_ready, mix)
    tail_stage(*tail_sizes, steps, mixed, *held[13:], *tail_in[4:], out, *tail_refs)


def layer(mixer_in, tail_in):
    sp_count, tp_count = lax.axis_size("sp"), lax.axis_size("tp")
    bf16, f32 = jnp.bfloat16, jnp.float32
    dma = pltpu.SemaphoreType.DMA
    vmem, anywhere = pl.BlockSpec(memory_space=pltpu.VMEM), pl.BlockSpec(memory_space=pl.ANY)
    length, wide = mixer_in[0].shape
    narrow = mixer_in[1].shape[1]
    heads = mixer_in[4].shape[0]
    owners = min(sp_count, STATE // 8)
    mixer_sizes = (heads, narrow // STATE, owners, wide // heads)
    mixer_refs = mixer_scratch(sp_count, owners, length, wide, narrow, length // BLK)
    stream, _, index, _, out_weight, gate, up, down, common_gate, common_up, common_down = tail_in
    planes = PLANES if sp_count % PLANES == 0 else 1
    ring = sp_count // planes * tp_count
    count, width = stream.shape
    fanout = index.shape[0]
    experts = sp_count * tp_count
    capacity = max(2, (3 * count * fanout + 2 * experts - 1) // (2 * experts))
    capacity = (capacity + 7) // 8 * 8
    part = width // HALVES
    chunks = len(column_chunks(width))
    slots = (planes, HALVES, ring, capacity, part)
    pieces = (planes, HALVES, count, part)
    return pl.pallas_call(
        functools.partial(
            layer_kernel,
            (planes, ring, tp_count, capacity, fanout),
            mixer_sizes,
            len(mixer_refs),
        ),
        out_shape=pltpu.VMEM((count, width), bf16),
        in_specs=[anywhere] * 24,
        out_specs=vmem,
        scratch_shapes=[
            pltpu.VMEM((length, wide), bf16),
            dma((17,)),
            *[pltpu.VMEM(part.shape, part.dtype) for part in (*mixer_in, *tail_in[:4])],
            *mixer_refs,
            pltpu.VMEM(out_weight.shape, bf16),
            pltpu.VMEM(gate.shape[1:], bf16),
            pltpu.VMEM(up.shape[1:], bf16),
            pltpu.VMEM(down.shape[1:], bf16),
            pltpu.VMEM(common_gate.shape, bf16),
            pltpu.VMEM(common_up.shape, bf16),
            pltpu.VMEM(common_down.shape, bf16),
            pltpu.VMEM((planes, fanout, count), jnp.int32),
            pltpu.VMEM((planes, fanout, count), f32),
            pltpu.VMEM((count, width), f32),
            pltpu.VMEM((count, common_gate.shape[1]), bf16),
            pltpu.VMEM((tp_count - 1, count, width), bf16),
            pltpu.VMEM((tp_count - 1, count, width), bf16),
            pltpu.VMEM((count, width), bf16),
            pltpu.VMEM(pieces, bf16),
            pltpu.VMEM(slots, bf16),
            pltpu.VMEM(slots, bf16),
            pltpu.VMEM((ring * capacity, width), bf16),
            pltpu.VMEM((ring * capacity, gate.shape[2]), bf16),
            pltpu.VMEM(slots, bf16),
            pltpu.VMEM(slots, bf16),
            pltpu.VMEM(pieces[1:], f32),
            pltpu.VMEM(pieces, bf16),
            pltpu.VMEM(pieces, bf16),
            pltpu.VMEM(pieces[1:], bf16),
            dma((7,)),
            dma((tp_count - 1,)),
            dma((tp_count - 1, chunks)),
            dma((2,)),
            dma((2,)),
            *[dma((planes, HALVES))] * 3,
            dma((1,)),
            dma((planes, HALVES)),
            dma((1,)),
            dma((planes, HALVES)),
            dma((1,)),
            dma((1,)),
            dma((HALVES,)),
        ],
        compiler_params=pltpu.CompilerParams(
            collective_id=0, has_side_effects=True, vmem_limit_bytes=62 * 2**20
        ),
    )(*mixer_in, *tail_in)


def on_device(
    stream,
    head_input_signal,
    write_input_vectors,
    read_input_vectors,
    output_gate_input,
    step_size_input,
    position_log_decay,
    signal_filter_taps,
    write_filter_taps,
    read_filter_taps,
    step_size_bias,
    head_decay_rate,
    head_direct_term,
    grouped_norm_gain,
    mixer_output_weight,
    expert_norm_gain,
    chosen_expert_index,
    chosen_expert_weight,
    routed_gate_weight,
    routed_up_weight,
    routed_down_weight,
    common_gate_weight,
    common_up_weight,
    common_down_weight,
):
    row = lambda part: part.reshape(1, -1)
    return layer(
        (
            head_input_signal,
            write_input_vectors,
            read_input_vectors,
            output_gate_input,
            step_size_input.T,
            position_log_decay.T,
            signal_filter_taps,
            write_filter_taps,
            read_filter_taps,
            row(step_size_bias),
            row(head_decay_rate),
            row(head_direct_term),
            row(grouped_norm_gain),
        ),
        (
            stream,
            row(expert_norm_gain),
            chosen_expert_index.T,
            chosen_expert_weight.T,
            mixer_output_weight,
            routed_gate_weight,
            routed_up_weight,
            routed_down_weight,
            common_gate_weight,
            common_up_weight,
            common_down_weight,
        ),
    )


def solution(mesh):
    in_specs = (
        P(("sp", "tp"), None),
        P("sp", "tp"),
        P("sp", "tp"),
        P("sp", "tp"),
        P("sp", "tp"),
        P("sp", "tp"),
        P("sp", "tp"),
        P(None, "tp"),
        P(None, "tp"),
        P(None, "tp"),
        P("tp"),
        P("tp"),
        P("tp"),
        P("tp"),
        P("tp", None),
        P(),
        P(("sp", "tp"), None),
        P(("sp", "tp"), None),
        P(("sp", "tp"), None, None),
        P(("sp", "tp"), None, None),
        P(("sp", "tp"), None, None),
        P(),
        P(),
        P(),
    )
    out_specs = P(("sp", "tp"), None)
    return jax.shard_map(
        on_device, mesh=mesh, in_specs=in_specs, out_specs=out_specs, check_vma=False
    )
```

```python
import functools

import jax
import jax.numpy as jnp
from jax import lax
from jax.experimental import pallas as pl
from jax.experimental.pallas import tpu as pltpu
from jax.sharding import PartitionSpec as P

STATE = 128
BLK = 128


MESH = pl.DeviceIdType.MESH
PLANES = 4
PARTS = 4
COLS = 512


LINE_END = [
    (0, 0, 0), (3, 0, 0), (0, 0, 1), (0, 0, 2), (0, 0, 3), (0, 1, 0),
    (0, 1, 1), (0, 2, 0), (0, 2, 1), (0, 3, 0), (0, 3, 1), (0, 3, 2),
    (0, 3, 3), (0, 1, 2), (1, 3, 0), (0, 2, 2), (2, 3, 0), (0, 2, 3),
    (2, 3, 1), (0, 1, 3), (2, 3, 2), (2, 3, 3), (1, 2, 0), (1, 1, 0),
    (2, 2, 0), (2, 2, 1), (2, 2, 2), (1, 0, 0), (2, 2, 3), (2, 1, 0),
    (2, 1, 1), (2, 1, 2), (2, 0, 0), (2, 1, 3), (2, 0, 1), (2, 0, 2),
    (2, 0, 3),
]
LINE_NEXT = [
    (0, 1, 0), (0, 1, 1), (0, 2, 0), (0, 0, 0), (0, 2, 1), (0, 0, 1),
    (0, 3, 0), (0, 0, 2), (0, 3, 1), (0, 0, 3), (0, 3, 2), (0, 3, 3),
    (0, 1, 2), (1, 0, 0), (0, 2, 2), (0, 1, 3), (0, 2, 3), (1, 3, 0),
    (2, 0, 0), (1, 2, 0), (2, 3, 0), (2, 3, 1), (3, 1, 0), (2, 3, 2),
    (2, 3, 3), (2, 0, 1), (2, 2, 0), (1, 1, 0), (2, 2, 1), (2, 1, 0),
    (2, 0, 2), (2, 2, 2), (2, 1, 1), (2, 2, 3), (2, 0, 3), (2, 1, 2),
    (2, 1, 3),
]


def line_plans(planes, parts):
    code = lambda plan: [(k * planes + s) * parts + h for k, s, h in plan]
    if (planes, parts) == (4, 4):
        return [code(LINE_END), code(LINE_NEXT)]
    plan = [(0, s, h) for s in range(planes) for h in range(parts)] + [(3, 0, 0)]
    for s in range(planes):
        plan += [(1, s, 0)] + [(2, s, h) for h in range(parts)]
    return [code(plan)] * 2


def column_chunks(width):
    step = min(COLS, width)
    return [(at, step) for at in range(0, width, step)]


def pick(plans, inner, turn):
    chosen = jnp.int32(0)
    for spot, (end, near) in enumerate(zip(*plans)):
        chosen = chosen + (turn == spot).astype(jnp.int32) * (end + inner * (near - end))
    return chosen


def bytes_of(ref, number, send_sem, recv_sem):
    view = ref.at[pl.ds(0, number)]
    return pltpu.make_async_remote_copy(
        src_ref=view,
        dst_ref=view,
        send_sem=send_sem,
        recv_sem=recv_sem,
        device_id=(lax.axis_index("sp"), lax.axis_index("tp")),
        device_id_type=MESH,
    )


def tail_stage(
    planes,
    ring,
    tp_count,
    capacity,
    fanout,
    steps,
    mixed_ref,
    stream_ref,
    gain_ref,
    index_ref,
    weight_ref,
    out_weight_hbm,
    gate_hbm,
    up_hbm,
    down_hbm,
    common_gate_hbm,
    common_up_hbm,
    common_down_hbm,
    out_ref,
    out_weight,
    gate,
    up,
    down,
    common_gate,
    common_up,
    common_down,
    index_tables,
    weight_tables,
    total,
    residual,
    part_out,
    part_in,
    normed,
    rows,
    sent,
    arrived,
    flat,
    hidden,
    answer,
    returned,
    sums_own,
    sums_out,
    sums_in,
    relay_in,
    weight_sem,
    part_send,
    part_recv,
    table_send,
    table_recv,
    rows_up,
    rows_down,
    rows_recv,
    go_send,
    go_recv,
    back_send,
    back_recv,
    sums_send,
    sums_recv,
    relay_recv,
):
    chip = lax.axis_index("sp")
    core = lax.axis_index("tp")
    chips = ring // tp_count
    plane = chip // chips
    mine = (chip % chips) * tp_count + core
    count, width = stream_ref.shape
    halves = rows.shape[1]
    part = width // halves
    plans = line_plans(planes, halves)
    relayed = planes == 4

    def in_plane(spot):
        return (plane * chips + spot // tp_count, spot % tp_count)

    def in_line(spot):
        return (spot * chips + chip % chips, core)

    loads = [
        pltpu.make_async_copy(source, target, weight_sem.at[number])
        for number, (source, target) in enumerate(
            [
                (out_weight_hbm, out_weight),
                (common_gate_hbm, common_gate),
                (common_up_hbm, common_up),
                (common_down_hbm, common_down),
                (gate_hbm.at[0], gate),
                (up_hbm.at[0], up),
                (down_hbm.at[0], down),
            ]
        )
    ]
    barrier = pltpu.get_barrier_semaphore()
    all_chips = lax.axis_size("sp")
    for ahead in range(1, all_chips):
        pl.semaphore_signal(
            barrier, inc=1, device_id=((chip + ahead) % all_chips, core), device_id_type=MESH
        )
    for spot in range(chips):
        for ahead in range(1, tp_count):
            pl.semaphore_signal(
                barrier,
                inc=1,
                device_id=(plane * chips + spot, (core + ahead) % tp_count),
                device_id_type=MESH,
            )
    load_inputs, inputs_ready, mix = steps
    load_inputs()
    for load in loads:
        load.start()
    pl.semaphore_wait(barrier, all_chips - 1 + chips * (tp_count - 1))
    inputs_ready()

    def table_copies(ahead, owner):
        return [
            pltpu.make_async_remote_copy(
                src_ref=source,
                dst_ref=held.at[owner],
                send_sem=table_send.at[number],
                recv_sem=table_recv.at[number],
                device_id=in_line((plane + ahead) % planes),
                device_id_type=MESH,
            )
            for number, (source, held) in enumerate(
                [(index_ref, index_tables), (weight_ref, weight_tables)]
            )
        ]

    for ahead in range(1, planes):
        for copy in table_copies(ahead, plane):
            copy.start()
    index_tables[plane] = index_ref[...]
    weight_tables[plane] = weight_ref[...]
    if relayed:

        @pl.when(plane == 1)
        def _():
            sums_in[3] = jnp.zeros(sums_in.shape[1:], jnp.bfloat16)

        @pl.when(plane == 2)
        def _():
            sums_in[0] = jnp.zeros(sums_in.shape[1:], jnp.bfloat16)

    mix()
    table_totals = [
        bytes_of(held, planes - 1, table_send.at[number], table_recv.at[number])
        for number, held in enumerate([index_tables, weight_tables])
    ]
    if planes > 1:
        for total_copy in table_totals:
            total_copy.wait_recv()

    def part_copies(ahead):
        return [
            pltpu.make_async_remote_copy(
                src_ref=part_out.at[ahead - 1, :, pl.ds(at, step)],
                dst_ref=part_in.at[ahead - 1, :, pl.ds(at, step)],
                send_sem=part_send.at[ahead - 1],
                recv_sem=part_recv.at[ahead - 1, number],
                device_id=(chip, (core + ahead) % tp_count),
                device_id_type=MESH,
            )
            for number, (at, step) in enumerate(column_chunks(width))
        ]

    loads[0].wait()
    for ahead in range(1, tp_count):
        owner = (core + ahead) % tp_count
        held = mixed_ref[pl.ds(pl.multiple_of(owner * count, count), count), :]
        copies = part_copies(ahead)
        for number, (at, step) in enumerate(column_chunks(width)):
            part_out[ahead - 1, :, at : at + step] = jnp.dot(
                held, out_weight[:, at : at + step], preferred_element_type=jnp.float32
            ).astype(jnp.bfloat16)
            copies[number].start()
    held = mixed_ref[pl.ds(pl.multiple_of(core * count, count), count), :]
    for at, step in column_chunks(width):
        total[:, at : at + step] = stream_ref[:, at : at + step].astype(jnp.float32) + jnp.dot(
            held, out_weight[:, at : at + step], preferred_element_type=jnp.float32
        )
    for ahead in range(1, tp_count):
        for copy in part_copies(ahead):
            copy.wait_recv()
    band = 16

    def norm_band(number, carry):
        spot = pl.ds(pl.multiple_of(number * band, band), band)
        summed = total[spot, :]
        for ahead in range(1, tp_count):
            summed = summed + part_in[ahead - 1, spot, :].astype(jnp.float32)
        rounded = summed.astype(jnp.bfloat16)
        wide = rounded.astype(jnp.float32)
        total[spot, :] = wide
        scale = lax.rsqrt(jnp.mean(wide * wide, axis=-1, keepdims=True) + 1e-06)
        value = (wide * scale * gain_ref[...]).astype(jnp.bfloat16)
        normed[spot, :] = value
        for half in range(halves):
            rows[plane, half, spot, :] = value[:, half * part : (half + 1) * part]
        return carry

    lax.fori_loop(0, count // band, norm_band, 0, unroll=2)

    def rows_copy(owner, half, target, sem):
        return pltpu.make_async_remote_copy(
            src_ref=rows.at[owner, half],
            dst_ref=rows.at[owner, half],
            send_sem=sem.at[owner, half],
            recv_sem=rows_recv.at[owner, half],
            device_id=in_line(target),
            device_id_type=MESH,
        )

    def block_copy(source, target, send, recv, owner, half, ahead):
        spot = (mine + ahead) % ring
        return pltpu.make_async_remote_copy(
            src_ref=source.at[owner, half, spot],
            dst_ref=target.at[owner, half, mine],
            send_sem=send.at[0],
            recv_sem=recv.at[owner, half],
            device_id=in_plane(spot),
            device_id_type=MESH,
        )

    def block_wait(source, target, send, recv, owner, half):
        return pltpu.make_async_remote_copy(
            src_ref=source.at[owner, half, pl.ds(0, ring - 1)],
            dst_ref=target.at[owner, half, pl.ds(0, ring - 1)],
            send_sem=send.at[0],
            recv_sem=recv.at[owner, half],
            device_id=in_plane((mine + 1) % ring),
            device_id_type=MESH,
        )

    go = (sent, arrived, go_send, go_recv)
    back = (answer, returned, back_send, back_recv)

    def sums_copy(owner, half):
        return pltpu.make_async_remote_copy(
            src_ref=sums_out.at[owner, half],
            dst_ref=sums_in.at[plane, half],
            send_sem=sums_send.at[0],
            recv_sem=sums_recv.at[0],
            device_id=in_line(owner),
            device_id_type=MESH,
        )

    def relay_copy(owner, half):
        return pltpu.make_async_remote_copy(
            src_ref=sums_out.at[owner, half],
            dst_ref=relay_in.at[half],
            send_sem=sums_send.at[0],
            recv_sem=relay_recv.at[half],
            device_id=in_line(plane + 1 - 2 * (plane // (planes - 1))),
            device_id_type=MESH,
        )

    def slots_of(owner):
        table, parts = index_tables[owner], weight_tables[owner]
        names = lax.broadcasted_iota(jnp.int32, (ring, count), 0) + plane * ring
        hits = jnp.zeros((ring, count), jnp.float32)
        share = jnp.zeros((ring, count), jnp.float32)
        for turn in range(fanout):
            named = table[turn : turn + 1, :] == names
            hits = hits + jnp.where(named, 1.0, 0.0)
            share = share + jnp.where(named, parts[turn : turn + 1, :], 0.0)
        before = lax.broadcasted_iota(jnp.int32, (count, count), 0)
        after = lax.broadcasted_iota(jnp.int32, (count, count), 1)
        earlier = jnp.where(before < after, 1.0, 0.0).astype(jnp.bfloat16)
        slot = jnp.dot(hits.astype(jnp.bfloat16), earlier, preferred_element_type=jnp.float32)
        return jnp.where(hits > 0.5, slot, -1.0), share

    places = lax.broadcasted_iota(jnp.int32, (capacity, count), 0).astype(jnp.float32)

    def dispatch(owner, half):
        @pl.when(owner != plane)
        def _():
            rows_copy(owner, half, owner, rows_up).wait_recv()

        @pl.when((owner <= plane) & (plane < planes - 1))
        def _():
            rows_copy(owner, half, plane + 1, rows_up).start()

        @pl.when((owner >= plane) & (plane > 0))
        def _():
            rows_copy(owner, half, plane - 1, rows_down).start()

        slot, _ = slots_of(owner)
        chosen = jnp.concatenate(
            [
                jnp.where(slot[spot : spot + 1, :] == places, 1.0, 0.0)
                for spot in range(ring)
            ],
            axis=0,
        ).astype(jnp.bfloat16)
        for at, step in column_chunks(part):
            picked = jnp.dot(
                chosen, rows[owner, half, :, at : at + step], preferred_element_type=jnp.float32
            )
            for spot in range(ring):
                sent[owner, half, spot, :, at : at + step] = picked[
                    spot * capacity : (spot + 1) * capacity
                ].astype(jnp.bfloat16)
        for ahead in range(1, ring):
            block_copy(*go, owner, half, ahead).start()
        arrived[owner, half, mine] = sent[owner, half, mine]

    def ffn(x_ref, gate_ref, up_ref, down_ref, hidden_ref, put):
        for at, step in column_chunks(gate_ref.shape[1]):
            half = step // 2
            for lane in (at, at + half):
                g = jnp.dot(
                    x_ref[...], gate_ref[:, lane : lane + half], preferred_element_type=jnp.float32
                )
                u = jnp.dot(
                    x_ref[...], up_ref[:, lane : lane + half], preferred_element_type=jnp.float32
                )
                hidden_ref[:, lane : lane + half] = (jax.nn.silu(g) * u).astype(jnp.bfloat16)
        for at, step in column_chunks(width):
            put(
                at,
                step,
                jnp.dot(
                    hidden_ref[...],
                    down_ref[:, at : at + step],
                    preferred_element_type=jnp.float32,
                ),
            )

    def serve(owner):
        for half in range(halves):
            block_wait(*go, owner, half).wait_recv()
            for at, step in column_chunks(part):
                flat[:, half * part + at : half * part + at + step] = jnp.concatenate(
                    [
                        arrived[owner, half, spot, :, at : at + step].astype(jnp.float32)
                        for spot in range(ring)
                    ],
                    axis=0,
                ).astype(jnp.bfloat16)

        def put(at, step, value):
            half, lane = at // part, at % part
            for spot in range(ring):
                answer[owner, half, spot, :, lane : lane + step] = value[
                    spot * capacity : (spot + 1) * capacity
                ].astype(jnp.bfloat16)
            if lane + step == part:
                for ahead in range(1, ring):
                    block_copy(*back, owner, half, ahead).start()

        ffn(flat, gate, up, down, hidden, put)
        for half in range(halves):
            returned[owner, half, mine] = answer[owner, half, mine]

    def collect(owner, half):
        block_wait(*back, owner, half).wait_recv()
        ends = helps = jnp.bool_(False)
        if relayed:
            ends = ((plane == 0) & (owner == 2)) | ((plane == 3) & (owner == 1))
            helps = ((plane == 1) & (owner == 2)) | ((plane == 2) & (owner == 1))

            @pl.when(helps)
            def _():
                relay_copy(owner, half).wait_recv()

        slot, share = slots_of(owner)
        spread = jnp.concatenate(
            [
                jnp.where(slot[spot : spot + 1, :] == places, share[spot : spot + 1, :], 0.0)
                for spot in range(ring)
            ],
            axis=0,
        )
        coarse = spread.astype(jnp.bfloat16)
        fine = (spread - coarse.astype(jnp.float32)).astype(jnp.bfloat16)
        contract = (((0,), (0,)), ((), ()))
        for at, step in column_chunks(part):
            blocks = jnp.concatenate(
                [
                    returned[owner, half, spot, :, at : at + step].astype(jnp.float32)
                    for spot in range(ring)
                ],
                axis=0,
            ).astype(jnp.bfloat16)
            value = lax.dot_general(coarse, blocks, contract, preferred_element_type=jnp.float32)
            value = value + lax.dot_general(
                fine, blocks, contract, preferred_element_type=jnp.float32
            )

            @pl.when(owner == plane)
            def _():
                sums_own[half, :, at : at + step] = value

            @pl.when((owner != plane) & ~helps)
            def _():
                sums_out[owner, half, :, at : at + step] = value.astype(jnp.bfloat16)

            if relayed:

                @pl.when(helps)
                def _():
                    sums_out[owner, half, :, at : at + step] = (
                        value + relay_in[half, :, at : at + step].astype(jnp.float32)
                    ).astype(jnp.bfloat16)

        @pl.when((owner != plane) & ~ends)
        def _():
            sums_copy(owner, half).start()

        if relayed:

            @pl.when(ends)
            def _():
                relay_copy(owner, half).start()

    def share_expert():
        for load in loads[1:4]:
            load.wait()

        def put(at, step, value):
            total[:, at : at + step] += value

        ffn(normed, common_gate, common_up, common_down, residual, put)

    def step(turn, carry):
        code = pick(plans, (plane + 1) // 2 % 2, turn)
        half, owner, kind = code % halves, code // halves % planes, code // (halves * planes)
        if relayed:
            owner = owner + plane // 2 * (planes - 1 - 2 * owner)

        @pl.when(kind == 0)
        def _():
            dispatch(owner, half)

        @pl.when(kind == 1)
        def _():
            serve(owner)

        @pl.when(kind == 2)
        def _():
            collect(owner, half)

        @pl.when(kind == 3)
        def _():
            share_expert()

        return carry

    for load in loads[4:]:
        load.wait()
    lax.fori_loop(0, len(plans[0]), step, 0)

    for ahead in range(1, tp_count):
        pltpu.make_async_remote_copy(
            src_ref=part_out.at[ahead - 1],
            dst_ref=part_in.at[ahead - 1],
            send_sem=part_send.at[ahead - 1],
            recv_sem=part_recv.at[ahead - 1, 0],
            device_id=(chip, (core + ahead) % tp_count),
            device_id_type=MESH,
        ).wait_send()
    for source, target, send, recv in (go, back):
        pltpu.make_async_remote_copy(
            src_ref=source.at[:, :, pl.ds(0, ring - 1)],
            dst_ref=target.at[:, :, pl.ds(0, ring - 1)],
            send_sem=send.at[0],
            recv_sem=recv.at[0, 0],
            device_id=in_plane((mine + 1) % ring),
            device_id_type=MESH,
        ).wait_send()

    def drain(code, carry):
        owner, half = code // halves, code % halves

        @pl.when((owner <= plane) & (plane < planes - 1))
        def _():
            rows_copy(owner, half, plane + 1, rows_up).wait_send()

        @pl.when((owner >= plane) & (plane > 0))
        def _():
            rows_copy(owner, half, plane - 1, rows_down).wait_send()

        return carry

    lax.fori_loop(0, planes * halves, drain, 0)
    if planes > 1:
        for total_copy in table_totals:
            total_copy.wait_send()
        bytes_of(sums_out, planes - 1, sums_send.at[0], sums_recv.at[0]).wait_send()
        if relayed:
            inside = (plane == 1) | (plane == 2)

            @pl.when(inside)
            def _():
                bytes_of(sums_in, planes - 2, sums_send.at[0], sums_recv.at[0]).wait_recv()

            @pl.when(~inside)
            def _():
                bytes_of(sums_in, planes - 1, sums_send.at[0], sums_recv.at[0]).wait_recv()

        else:
            bytes_of(sums_in, planes - 1, sums_send.at[0], sums_recv.at[0]).wait_recv()

    def last_band(number, carry):
        spot = pl.ds(pl.multiple_of(number * band, band), band)
        for half in range(halves):
            lanes = slice(half * part, (half + 1) * part)
            value = total[spot, lanes] + sums_own[half, spot, :]
            for ahead in range(1, planes):
                value = value + sums_in[(plane + ahead) % planes, half, spot, :].astype(
                    jnp.float32
                )
            out_ref[spot, lanes] = value.astype(jnp.bfloat16)
        return carry

    lax.fori_loop(0, count // band, last_band, 0)


def mixer_stage(
    heads,
    groups,
    owners,
    head_dim,
    gate_ready,
    signal_in,
    write_in,
    read_in,
    gate_in,
    step_in,
    log_in,
    signal_taps,
    write_taps,
    read_taps,
    bias,
    rate,
    direct,
    gain,
    mixed,
    halo_signal,
    halo_write,
    halo_read,
    extended,
    signal,
    write_vec,
    read_vec,
    scaled,
    tailed,
    readout,
    states,
    summed,
    piece_out,
    piece_in,
    decay_out,
    decay_in,
    start_out,
    start_in,
    halo_send,
    halo_recv,
    piece_send,
    piece_recv,
    decay_send,
    decay_recv,
    start_send,
    start_recv,
):
    chip, core = lax.axis_index("sp"), lax.axis_index("tp")
    chips = lax.axis_size("sp")
    length, wide = signal_in.shape
    narrow = write_in.shape[1]
    rim = halo_signal.shape[0]
    taps = signal_taps.shape[0]
    blocks = length // BLK
    per_group = heads // groups
    span = per_group * head_dim
    rows = STATE // owners
    f32, bf16 = jnp.float32, jnp.bfloat16
    exact = lax.Precision.HIGHEST

    def halo_copies(target):
        return [
            pltpu.make_async_remote_copy(
                src_ref=source.at[pl.ds(length - rim, rim), :],
                dst_ref=halo,
                send_sem=halo_send.at[number],
                recv_sem=halo_recv.at[number],
                device_id=(target, core),
                device_id_type=MESH,
            )
            for number, (source, halo) in enumerate(
                [(signal_in, halo_signal), (write_in, halo_write), (read_in, halo_read)]
            )
        ]

    @pl.when(chip < chips - 1)
    def _():
        for copy in halo_copies(chip + 1):
            copy.start()

    timestep = step_in[...].astype(f32).T + bias[...]
    timestep = jnp.maximum(timestep, 0.0) + jnp.log1p(jnp.exp(-jnp.abs(timestep)))
    log_decay = log_in[...].T - rate[...] * timestep
    first = lax.broadcasted_iota(jnp.int32, (BLK, BLK), 0)
    second = lax.broadcasted_iota(jnp.int32, (BLK, BLK), 1)
    causal = first >= second
    lower = jnp.where(causal, 1.0, 0.0)
    cums = [
        jnp.dot(
            lower,
            log_decay[b * BLK : (b + 1) * BLK],
            precision=exact,
            preferred_element_type=f32,
        )
        for b in range(blocks)
    ]
    part = lax.broadcasted_iota(jnp.int32, (heads, wide), 0)
    lane = lax.broadcasted_iota(jnp.int32, (heads, wide), 1) // head_dim
    widen = jnp.where(part == lane, 1.0, 0.0).astype(bf16)

    def expand(value):
        high = value.astype(bf16)
        rest = value - high.astype(f32)
        middle = rest.astype(bf16)
        low = (rest - middle.astype(f32)).astype(bf16)
        return (
            jnp.dot(high, widen, preferred_element_type=f32)
            + jnp.dot(middle, widen, preferred_element_type=f32)
            + jnp.dot(low, widen, preferred_element_type=f32)
        )

    for b in range(blocks):
        readout[b * BLK : (b + 1) * BLK, :] = expand(jnp.exp(cums[b]))
    decay = readout[BLK - 1 : BLK, :]
    for b in range(1, blocks):
        decay = decay * readout[(b + 1) * BLK - 1 : (b + 1) * BLK, :]
    decay_out[...] = decay

    def decay_copy(owner, device):
        return pltpu.make_async_remote_copy(
            src_ref=decay_out,
            dst_ref=decay_in.at[device],
            send_sem=decay_send.at[0],
            recv_sem=decay_recv.at[0],
            device_id=(owner, core),
            device_id_type=MESH,
        )

    def piece_copy(owner, device):
        return pltpu.make_async_remote_copy(
            src_ref=piece_out.at[owner],
            dst_ref=piece_in.at[device],
            send_sem=piece_send.at[0],
            recv_sem=piece_recv.at[device],
            device_id=(owner, core),
            device_id_type=MESH,
        )

    def start_copy(owner, device):
        return pltpu.make_async_remote_copy(
            src_ref=start_out.at[device],
            dst_ref=start_in.at[owner],
            send_sem=start_send.at[0],
            recv_sem=start_recv.at[0],
            device_id=(device, core),
            device_id_type=MESH,
        )

    def others(number, act):
        for at in range(number):

            @pl.when(at != chip)
            def _():
                act(at)

    def with_others(act):
        if owners == chips:
            act(owners - 1)
        else:

            @pl.when(chip < owners)
            def _():
                act(owners - 1)

            @pl.when(chip >= owners)
            def _():
                act(owners)

    others(owners, lambda owner: decay_copy(owner, chip).start())

    @pl.when(chip < owners)
    def _():
        decay_in[chip] = decay_out[...]

    parts = [
        (signal_in, halo_signal, signal_taps, 0, wide),
        (write_in, halo_write, write_taps, wide, narrow),
        (read_in, halo_read, read_taps, wide + narrow, narrow),
    ]
    head_room = 8
    for source, _, _, at, size in parts:
        extended[head_room : head_room + length, at : at + size] = source[...].astype(f32)

    def convolve(b, weights, at, size, put):
        for lanes in range(0, size, 256):
            total = None
            for tap in range(taps):
                begin = head_room - taps + 1 + tap + b * BLK
                term = (
                    weights[tap : tap + 1, lanes : lanes + 256].astype(f32)
                    * extended[begin : begin + BLK, at + lanes : at + lanes + 256]
                )
                total = term if total is None else total + term
            put(b, lanes, jax.nn.silu(total))

    def put_write(b, lanes, value):
        write_vec[b * BLK : (b + 1) * BLK, lanes : lanes + 256] = value.astype(bf16)

    def put_read(b, lanes, value):
        read_vec[b * BLK : (b + 1) * BLK, lanes : lanes + 256] = value.astype(bf16)

    def put_signal(b, lanes, value):
        signal[b * BLK : (b + 1) * BLK, lanes : lanes + 256] = value

    def state_of(b):
        convolve(b, write_taps, wide, narrow, put_write)
        convolve(b, signal_taps, 0, wide, put_signal)
        spot = slice(b * BLK, (b + 1) * BLK)
        step = timestep[spot]
        scaled[spot, :] = (signal[spot, :] * expand(step)).astype(bf16)
        rest = jnp.exp(cums[b][BLK - 1 : BLK, :] - cums[b])
        tailed[spot, :] = (signal[spot, :] * expand(step * rest)).astype(bf16)
        for g in range(groups):
            states[b, :, g * span : (g + 1) * span] = lax.dot_general(
                write_vec[spot, g * STATE : (g + 1) * STATE],
                tailed[spot, g * span : (g + 1) * span],
                (((0,), (0,)), ((), ())),
                preferred_element_type=f32,
            )

    spread_direct = expand(jnp.broadcast_to(direct[...], (8, heads)))[0:1, :]
    low_lanes = lax.broadcasted_iota(jnp.int32, (BLK, 2 * head_dim), 1) < head_dim

    def within(b):
        convolve(b, read_taps, wide + narrow, narrow, put_read)
        spot = slice(b * BLK, (b + 1) * BLK)
        turned = cums[b].T
        for g in range(groups):
            inner = slice(g * STATE, (g + 1) * STATE)
            meeting = lax.dot_general(
                read_vec[spot, inner],
                write_vec[spot, inner],
                (((1,), (1,)), ((), ())),
                preferred_element_type=f32,
            )
            for pair in range(per_group // 2):
                head = g * per_group + 2 * pair
                lanes = slice(head * head_dim, (head + 2) * head_dim)
                weights = []
                for at in (head, head + 1):
                    gap = cums[b][:, at : at + 1] - turned[at : at + 1, :]
                    weights.append(
                        (meeting * jnp.exp(jnp.where(causal, gap, -jnp.inf))).astype(bf16)
                    )
                value = scaled[spot, lanes]
                zero = jnp.zeros_like(value)
                both = jnp.concatenate(
                    [jnp.where(low_lanes, value, zero), jnp.where(low_lanes, zero, value)], axis=0
                )
                summed[spot, lanes] = spread_direct[:, lanes] * signal[spot, lanes] + jnp.dot(
                    jnp.concatenate(weights, axis=1), both, preferred_element_type=f32
                )

    for b in range(1, blocks):
        state_of(b)
        within(b)

    @pl.when(chip > 0)
    def _():
        for copy in halo_copies(chip):
            copy.wait_recv()
        for _, halo, _, at, size in parts:
            extended[0:head_room, at : at + size] = halo[rim - head_room : rim, :].astype(f32)

    @pl.when(chip == 0)
    def _():
        extended[0:head_room, :] = jnp.zeros((head_room, extended.shape[1]), f32)

    state_of(0)
    for owner in range(owners):
        spot = slice(owner * rows, (owner + 1) * rows)
        value = states[0, spot, :]
        for b in range(1, blocks):
            value = value * readout[(b + 1) * BLK - 1 : (b + 1) * BLK, :] + states[b, spot, :]
        piece_out[owner] = value.astype(bf16)
    others(owners, lambda owner: piece_copy(owner, chip).start())

    @pl.when(chip < owners)
    def _():
        piece_in[chip] = piece_out[chip]

    within(0)

    @pl.when(chip < owners)
    def _():
        bytes_of(decay_in, chips - 1, decay_send.at[0], decay_recv.at[0]).wait_recv()

        def scan(device, held):
            @pl.when(device != chip)
            def _():
                piece_copy(chip, device).wait_recv()

            start_out[device] = held.astype(bf16)

            @pl.when(device != chip)
            def _():
                start_copy(chip, device).start()

            return held * decay_in[device] + piece_in[device].astype(f32)

        lax.fori_loop(0, chips, scan, jnp.zeros((rows, wide), f32))
        start_in[chip] = start_out[chip]

    with_others(
        lambda number: bytes_of(start_in, number, start_send.at[0], start_recv.at[0]).wait_recv()
    )
    gate_ready()
    start = jnp.concatenate([start_in[owner].astype(f32) for owner in range(owners)], axis=0)
    for b in range(blocks):
        spot = slice(b * BLK, (b + 1) * BLK)
        if b:
            start = (
                start * readout[b * BLK - 1 : b * BLK, :] + states[b - 1]
            )
        rounded = start.astype(bf16)
        for g in range(groups):
            lanes = slice(g * span, (g + 1) * span)
            near = jnp.dot(
                read_vec[spot, g * STATE : (g + 1) * STATE],
                rounded[:, lanes],
                preferred_element_type=f32,
            )
            value = summed[spot, lanes] + near * readout[spot, lanes]
            value = value * jax.nn.silu(gate_in[spot, lanes].astype(f32))
            scale = lax.rsqrt(jnp.mean(value * value, axis=-1, keepdims=True) + 1e-06)
            mixed[spot, lanes] = (value * scale * gain[:, lanes]).astype(bf16)

    @pl.when(chip < chips - 1)
    def _():
        for copy in halo_copies(chip + 1):
            copy.wait_send()

    with_others(
        lambda number: bytes_of(decay_in, number, decay_send.at[0], decay_recv.at[0]).wait_send()
    )
    with_others(
        lambda number: bytes_of(piece_out, number, piece_send.at[0], piece_recv.at[0]).wait_send()
    )

    @pl.when(chip < owners)
    def _():
        bytes_of(start_out, chips - 1, start_send.at[0], start_recv.at[0]).wait_send()


def mixer_scratch(chips, owners, length, wide, narrow, blocks):
    f32, bf16 = jnp.float32, jnp.bfloat16
    dma = pltpu.SemaphoreType.DMA
    rows = STATE // owners
    rim = 16
    return [
        pltpu.VMEM((rim, wide), bf16),
        pltpu.VMEM((rim, narrow), bf16),
        pltpu.VMEM((rim, narrow), bf16),
        pltpu.VMEM((length + 8, wide + 2 * narrow), f32),
        pltpu.VMEM((length, wide), f32),
        pltpu.VMEM((length, narrow), bf16),
        pltpu.VMEM((length, narrow), bf16),
        pltpu.VMEM((length, wide), bf16),
        pltpu.VMEM((length, wide), bf16),
        pltpu.VMEM((length, wide), f32),
        pltpu.VMEM((blocks, STATE, wide), f32),
        pltpu.VMEM((length, wide), f32),
        pltpu.VMEM((owners, rows, wide), bf16),
        pltpu.VMEM((chips, rows, wide), bf16),
        pltpu.VMEM((1, wide), f32),
        pltpu.VMEM((chips, 1, wide), f32),
        pltpu.VMEM((chips, rows, wide), bf16),
        pltpu.VMEM((owners, rows, wide), bf16),
        dma((3,)),
        dma((3,)),
        dma((1,)),
        dma((chips,)),
        dma((1,)),
        dma((1,)),
        dma((1,)),
        dma((1,)),
    ]


def layer_kernel(tail_sizes, mixer_sizes, mixer_scratch_count, *refs):
    mixer_in, tail_in, out = refs[:13], refs[13:24], refs[24]
    mixed, early_sem = refs[25:27]
    held, refs = refs[27:44], refs[44:]
    mixer_refs, tail_refs = refs[:mixer_scratch_count], refs[mixer_scratch_count:]
    early = [
        pltpu.make_async_copy(source, target, early_sem.at[number])
        for number, (source, target) in enumerate(zip((*mixer_in, *tail_in[:4]), held))
    ]
    late = (3, 13, 14)

    def load_inputs():
        for number in sorted(range(17), key=lambda number: number in late):
            early[number].start()

    def inputs_ready():
        for number in range(17):
            if number not in late:
                early[number].wait()

    def mix():
        mixer_stage(*mixer_sizes, early[3].wait, *held[:13], mixed, *mixer_refs)
        early[13].wait()
        early[14].wait()

    steps = (load_inputs, inputs_ready, mix)
    tail_stage(*tail_sizes, steps, mixed, *held[13:], *tail_in[4:], out, *tail_refs)


def layer(mixer_in, tail_in):
    sp_count, tp_count = lax.axis_size("sp"), lax.axis_size("tp")
    bf16, f32 = jnp.bfloat16, jnp.float32
    dma = pltpu.SemaphoreType.DMA
    vmem, anywhere = pl.BlockSpec(memory_space=pltpu.VMEM), pl.BlockSpec(memory_space=pl.ANY)
    length, wide = mixer_in[0].shape
    narrow = mixer_in[1].shape[1]
    heads = mixer_in[4].shape[0]
    owners = min(sp_count, STATE // 8)
    mixer_sizes = (heads, narrow // STATE, owners, wide // heads)
    mixer_refs = mixer_scratch(sp_count, owners, length, wide, narrow, length // BLK)
    stream, _, index, _, out_weight, gate, up, down, common_gate, common_up, common_down = tail_in
    planes = PLANES if sp_count % PLANES == 0 else 1
    ring = sp_count // planes * tp_count
    count, width = stream.shape
    fanout = index.shape[0]
    experts = sp_count * tp_count
    capacity = max(2, (3 * count * fanout + 2 * experts - 1) // (2 * experts))
    capacity = (capacity + 7) // 8 * 8
    part = width // PARTS
    chunks = len(column_chunks(width))
    slots = (planes, PARTS, ring, capacity, part)
    pieces = (planes, PARTS, count, part)
    return pl.pallas_call(
        functools.partial(
            layer_kernel,
            (planes, ring, tp_count, capacity, fanout),
            mixer_sizes,
            len(mixer_refs),
        ),
        out_shape=pltpu.VMEM((count, width), bf16),
        in_specs=[anywhere] * 24,
        out_specs=vmem,
        scratch_shapes=[
            pltpu.VMEM((length, wide), bf16),
            dma((17,)),
            *[pltpu.VMEM(part.shape, part.dtype) for part in (*mixer_in, *tail_in[:4])],
            *mixer_refs,
            pltpu.VMEM(out_weight.shape, bf16),
            pltpu.VMEM(gate.shape[1:], bf16),
            pltpu.VMEM(up.shape[1:], bf16),
            pltpu.VMEM(down.shape[1:], bf16),
            pltpu.VMEM(common_gate.shape, bf16),
            pltpu.VMEM(common_up.shape, bf16),
            pltpu.VMEM(common_down.shape, bf16),
            pltpu.VMEM((planes, fanout, count), jnp.int32),
            pltpu.VMEM((planes, fanout, count), f32),
            pltpu.VMEM((count, width), f32),
            pltpu.VMEM((count, common_gate.shape[1]), bf16),
            pltpu.VMEM((tp_count - 1, count, width), bf16),
            pltpu.VMEM((tp_count - 1, count, width), bf16),
            pltpu.VMEM((count, width), bf16),
            pltpu.VMEM(pieces, bf16),
            pltpu.VMEM(slots, bf16),
            pltpu.VMEM(slots, bf16),
            pltpu.VMEM((ring * capacity, width), bf16),
            pltpu.VMEM((ring * capacity, gate.shape[2]), bf16),
            pltpu.VMEM(slots, bf16),
            pltpu.VMEM(slots, bf16),
            pltpu.VMEM(pieces[1:], f32),
            pltpu.VMEM(pieces, bf16),
            pltpu.VMEM(pieces, bf16),
            pltpu.VMEM(pieces[1:], bf16),
            dma((7,)),
            dma((tp_count - 1,)),
            dma((tp_count - 1, chunks)),
            dma((2,)),
            dma((2,)),
            *[dma((planes, PARTS))] * 3,
            dma((1,)),
            dma((planes, PARTS)),
            dma((1,)),
            dma((planes, PARTS)),
            dma((1,)),
            dma((1,)),
            dma((PARTS,)),
        ],
        compiler_params=pltpu.CompilerParams(
            collective_id=0, has_side_effects=True, vmem_limit_bytes=62 * 2**20
        ),
    )(*mixer_in, *tail_in)


def on_device(
    stream,
    head_input_signal,
    write_input_vectors,
    read_input_vectors,
    output_gate_input,
    step_size_input,
    position_log_decay,
    signal_filter_taps,
    write_filter_taps,
    read_filter_taps,
    step_size_bias,
    head_decay_rate,
    head_direct_term,
    grouped_norm_gain,
    mixer_output_weight,
    expert_norm_gain,
    chosen_expert_index,
    chosen_expert_weight,
    routed_gate_weight,
    routed_up_weight,
    routed_down_weight,
    common_gate_weight,
    common_up_weight,
    common_down_weight,
):
    row = lambda part: part.reshape(1, -1)
    return layer(
        (
            head_input_signal,
            write_input_vectors,
            read_input_vectors,
            output_gate_input,
            step_size_input.T,
            position_log_decay.T,
            signal_filter_taps,
            write_filter_taps,
            read_filter_taps,
            row(step_size_bias),
            row(head_decay_rate),
            row(head_direct_term),
            row(grouped_norm_gain),
        ),
        (
            stream,
            row(expert_norm_gain),
            chosen_expert_index.T,
            chosen_expert_weight.T,
            mixer_output_weight,
            routed_gate_weight,
            routed_up_weight,
            routed_down_weight,
            common_gate_weight,
            common_up_weight,
            common_down_weight,
        ),
    )


def solution(mesh):
    in_specs = (
        P(("sp", "tp"), None),
        P("sp", "tp"),
        P("sp", "tp"),
        P("sp", "tp"),
        P("sp", "tp"),
        P("sp", "tp"),
        P("sp", "tp"),
        P(None, "tp"),
        P(None, "tp"),
        P(None, "tp"),
        P("tp"),
        P("tp"),
        P("tp"),
        P("tp"),
        P("tp", None),
        P(),
        P(("sp", "tp"), None),
        P(("sp", "tp"), None),
        P(("sp", "tp"), None, None),
        P(("sp", "tp"), None, None),
        P(("sp", "tp"), None, None),
        P(),
        P(),
        P(),
    )
    out_specs = P(("sp", "tp"), None)
    return jax.shard_map(
        on_device, mesh=mesh, in_specs=in_specs, out_specs=out_specs, check_vma=False
    )
```
